128 devices in a mesh: rep: 2 (over z_hi), fs: 32 (over z_lo, y, x), tp: 2 (over core).
Axes of the slice: x: 4, y: 4, z: 4 (z_hi: 2, z_lo: 2; z = z_hi * 2 + z_lo), core: 2. Of those that a mesh axis runs over, the one named last changes fastest.
Arguments:
- tokens: bfloat16 [32768, 2048], P(('rep', 'fs'), 'tp'), may hold values from -6 to 6
- mix_gain: float32 [2048], replicated, may hold values from 0.1 to 1.9
- lru_input: float32 [2048, 2048], P('fs', 'tp'), may hold values from -0.125 to 0.125
- lru_gate: float32 [2048, 2048], P('fs', 'tp'), may hold values from -0.125 to 0.125
- lru_input_scale: float32 [2048], P('tp'), may hold values from 0.5 to 2
- lru_gate_scale: float32 [2048], P('tp'), may hold values from 0.5 to 2
- conv_weight: float32 [4, 2048], P(None, 'tp'), may hold values from -3 to 3
- recur_gate: float32 [32, 64, 64], P('tp'), may hold values from -0.75 to 0.75
- input_gate: float32 [32, 64, 64], P('tp'), may hold values from -0.75 to 0.75
- decay_rate: float32 [2048], P('tp'), may hold values from 3.5 to 9
- extra_decay: float32 [32768], P(('rep', 'fs')), may hold values from 0.0003 to 2.1
- lru_output: float32 [2048, 2048], P('tp', 'fs'), may hold values from -0.125 to 0.125
- lru_output_scale: float32 [2048], replicated, may hold values from 0.5 to 2
- ffn_gain: float32 [2048], replicated, may hold values from 0.1 to 1.9
- ffn_gate: float32 [2048, 2816], P('fs', 'tp'), may hold values from -0.125 to 0.125
- ffn_up: float32 [2048, 2816], P('fs', 'tp'), may hold values from -0.125 to 0.125
- ffn_gate_scale: float32 [2816], P('tp'), may hold values from 0.5 to 2
- ffn_up_scale: float32 [2816], P('tp'), may hold values from 0.5 to 2
- ffn_down: float32 [2816, 2048], P('tp', 'fs'), may hold values from -0.109375 to 0.109375
- ffn_down_scale: float32 [2048], replicated, may hold values from 0.5 to 2
Outputs:
- layer_out: bfloat16 [32768, 2048], P(('rep', 'fs'), 'tp')
The draws below stay inside these ranges and needn't reach their ends.
All inputs are finite; a program needn't handle non-finite values.
Results may differ from the reference program's by a relative error of at most 0.02.
Values may be sent and summed in bfloat16 or wider, within the bound.
No kernel may reach another device: no remote copies, remote signals or barrier semaphores. Data moves between devices by JAX's collectives and lax.ppermute only.
A program may use at most 192 MiB of HBM per device.

```python
import math
import jax
import jax.numpy as jnp
from jax import lax

D = 2048
FF = 2816
BDIM = 64
LRU_BLOCKS = 32
CONV = 4
TOK_DEV = 512
LRU = 2048
SEQS = 64
TOKENS = 32768
N_TP = 2


def draw_decay_rate(key, part):
    first, second, third = jax.random.split(jax.random.fold_in(key, 11), 3)
    share = 0.5
    slow = jax.random.uniform(first, (LRU,), jnp.float32) < share
    slow_value = jax.random.uniform(second, (LRU,), jnp.float32, 8.0, 9.0)
    fast_value = jax.random.uniform(third, (LRU,), jnp.float32, 3.5, 4.5)
    return jnp.where(slow, slow_value, fast_value)


def draw_extra_decay(key, part):
    first, second, third = jax.random.split(jax.random.fold_in(key, 23), 3)
    base = jnp.exp(jax.random.uniform(first, (SEQS, 1), jnp.float32, jnp.log(0.0003), jnp.log(0.0009)))
    spots = jax.random.randint(second, (SEQS, 3), 0, TOK_DEV)
    where = jnp.arange(TOK_DEV, dtype=jnp.int32)
    hits = jnp.sum((where[None, None, :] == spots[:, :, None]).astype(jnp.float32), axis=1)
    sizes = jax.random.uniform(third, (SEQS, TOK_DEV), jnp.float32, 0.22, 0.69)
    return (base + hits * sizes).reshape(TOKENS)


def block_scale(rng, shape, cuts, smallest, top_value):
    def one(position, shards_of):
        draws = jax.random.uniform(jax.random.fold_in(jax.random.fold_in(rng, 6), position), (shards_of,), jnp.float32, smallest / len(cuts), top_value / len(cuts))
        return jnp.repeat(jnp.exp(draws), shape[position] // shards_of).reshape((-1,) + (1,) * (len(shape) - position - 1))

    loudness = one(*cuts[0])
    for cut in cuts[1:]:
        loudness = loudness * one(*cut)
    return loudness


def gaussian(rng, shape, scale, most, cuts=(), kind=jnp.bfloat16):
    entries = jax.random.normal(rng, shape, jnp.float32) * scale
    if len(cuts) > 0:
        entries = block_scale(rng, shape, cuts, -0.22, 0.18) * entries
    return jnp.clip(entries, min=-most, max=most).astype(kind)


def setup_inputs(seed: int = 0) -> dict:
    key_of = jax.random.split(jax.random.key(seed), 21)
    tokens = gaussian(key_of[0], (TOKENS, D), 1.0, 6.0, ((0, 64), (1, 2)))
    mix_gain = jnp.clip(1.0 + 0.18 * jax.random.normal(key_of[1], (D,), jnp.float32), 0.1, 1.9)
    lru_input = gaussian(key_of[2], (D, LRU), D ** -0.5, 0.125, ((0, 32), (1, 2)), jnp.float32)
    lru_gate = gaussian(key_of[3], (D, LRU), D ** -0.5, 0.125, ((0, 32), (1, 2)), jnp.float32)
    lru_input_scale = jnp.clip(jnp.exp(math.log(2.0) - 1.3862944 * jax.random.uniform(key_of[4], (LRU,), jnp.float32) ** block_scale(key_of[4], (LRU,), ((0, 2),), -0.2, 0.2)), 0.5, 2.0)
    lru_gate_scale = jnp.clip(jnp.exp(math.log(2.0) - 1.3862944 * jax.random.uniform(key_of[5], (LRU,), jnp.float32) ** block_scale(key_of[5], (LRU,), ((0, 2),), -0.2, 0.2)), 0.5, 2.0)
    conv_weight = gaussian(key_of[6], (CONV, LRU), 0.5, 3.0, ((1, 2),), jnp.float32)
    recur_gate = gaussian(key_of[7], (LRU_BLOCKS, BDIM, BDIM), BDIM ** -0.5, 0.75, ((0, 2),), jnp.float32)
    input_gate = gaussian(key_of[8], (LRU_BLOCKS, BDIM, BDIM), BDIM ** -0.5, 0.75, ((0, 2),), jnp.float32)
    decay_rate = draw_decay_rate(jax.random.fold_in(key_of[20], 71), 0)
    extra_decay = draw_extra_decay(jax.random.fold_in(key_of[20], 71), 0)
    lru_output = gaussian(key_of[11], (LRU, D), LRU ** -0.5, 0.125, ((0, 2), (1, 32)), jnp.float32)
    lru_output_scale = jnp.clip(jnp.exp(jax.random.uniform(key_of[12], (D,), jnp.float32, math.log(0.5), math.log(2.0))), 0.5, 2.0)
    ffn_gain = jnp.clip(1.0 + 0.18 * jax.random.normal(key_of[13], (D,), jnp.float32), 0.1, 1.9)
    ffn_gate = gaussian(key_of[14], (D, FF), D ** -0.5, 0.125, ((0, 32), (1, 2)), jnp.float32)
    ffn_up = gaussian(key_of[15], (D, FF), D ** -0.5, 0.125, ((0, 32), (1, 2)), jnp.float32)
    ffn_gate_scale = jnp.clip(jnp.exp(math.log(2.0) - 1.3862944 * jax.random.uniform(key_of[16], (FF,), jnp.float32) ** block_scale(key_of[16], (FF,), ((0, 2),), -0.2, 0.2)), 0.5, 2.0)
    ffn_up_scale = jnp.clip(jnp.exp(math.log(2.0) - 1.3862944 * jax.random.uniform(key_of[17], (FF,), jnp.float32) ** block_scale(key_of[17], (FF,), ((0, 2),), -0.2, 0.2)), 0.5, 2.0)
    ffn_down = gaussian(key_of[18], (FF, D), FF ** -0.5, 0.109375, ((0, 2), (1, 32)), jnp.float32)
    ffn_down_scale = jnp.clip(jnp.exp(jax.random.uniform(key_of[19], (D,), jnp.float32, math.log(0.5), math.log(2.0))), 0.5, 2.0)
    return dict(tokens=tokens, mix_gain=mix_gain, lru_input=lru_input, lru_gate=lru_gate, lru_input_scale=lru_input_scale, lru_gate_scale=lru_gate_scale, conv_weight=conv_weight, recur_gate=recur_gate, input_gate=input_gate, decay_rate=decay_rate, extra_decay=extra_decay, lru_output=lru_output, lru_output_scale=lru_output_scale, ffn_gain=ffn_gain, ffn_gate=ffn_gate, ffn_up=ffn_up, ffn_gate_scale=ffn_gate_scale, ffn_up_scale=ffn_up_scale, ffn_down=ffn_down, ffn_down_scale=ffn_down_scale)


EPS = 1e-06
RATE = 8.0

def rms_rows(rows, gain):
    values = rows.astype(jnp.float32)
    scale = lax.rsqrt(lax.optimization_barrier(jnp.mean(values * values, axis=-1, keepdims=True)) + EPS)
    return (values * scale * gain).astype(jnp.bfloat16)

def block_sum(acts, weight, blocks):
    width = acts.shape[1] // blocks
    total = jnp.zeros((acts.shape[0], weight.shape[1]), jnp.float32)
    for block in range(blocks):
        part = jnp.dot(acts[:, block * width:(block + 1) * width], weight[block * width:(block + 1) * width].astype(jnp.bfloat16), preferred_element_type=jnp.float32).astype(jnp.bfloat16)
        part = lax.optimization_barrier(part)
        total = total + part.astype(jnp.float32)
    return total

def combine(left, right):
    return (left[0] * right[0], right[0] * left[1] + right[1])

def recurrence(branch_in, branch_gate, conv_weight, recur_gate, input_gate, decay_rate, extra):
    length = branch_in.shape[0]
    taps = conv_weight.shape[0]
    values = branch_in.astype(jnp.float32)
    padded = jnp.pad(values, ((taps - 1, 0), (0, 0)))
    conv = jnp.zeros_like(values)
    for tap in range(taps):
        conv = conv + conv_weight[tap] * padded[tap:tap + length]
    nblocks, bdim = (recur_gate.shape[0], recur_gate.shape[1])
    grouped = conv.reshape(length, nblocks, bdim)
    recur = jax.nn.sigmoid(jnp.einsum('sni,nij->snj', grouped, recur_gate, precision=lax.Precision.HIGHEST).reshape(length, -1))
    ingate = jax.nn.sigmoid(jnp.einsum('sni,nij->snj', grouped, input_gate, precision=lax.Precision.HIGHEST).reshape(length, -1))
    log_rate = -RATE * jax.nn.softplus(-decay_rate) * recur - extra[:, None]
    factor = jnp.exp(log_rate)
    drive = jnp.sqrt(-jnp.expm1(2.0 * log_rate)) * (ingate * conv)
    state = lax.associative_scan(combine, (factor, drive), axis=0)[1]
    gelu_gate = jax.nn.gelu(branch_gate.astype(jnp.float32), approximate=True)
    return (state * gelu_gate).astype(jnp.bfloat16)

def reference(tokens, mix_gain, lru_input, lru_gate, lru_input_scale, lru_gate_scale, conv_weight, recur_gate, input_gate, decay_rate, extra_decay, lru_output, lru_output_scale, ffn_gain, ffn_gate, ffn_up, ffn_gate_scale, ffn_up_scale, ffn_down, ffn_down_scale):
    normed = rms_rows(tokens, mix_gain)
    branch_in = (jnp.dot(normed, lru_input.astype(jnp.bfloat16), preferred_element_type=jnp.float32) * lru_input_scale).astype(jnp.bfloat16)
    branch_gate = (jnp.dot(normed, lru_gate.astype(jnp.bfloat16), preferred_element_type=jnp.float32) * lru_gate_scale).astype(jnp.bfloat16)
    width = branch_in.shape[1]
    gated = jax.vmap(recurrence, in_axes=(0, 0, None, None, None, None, 0))(branch_in.reshape(SEQS, TOK_DEV, width), branch_gate.reshape(SEQS, TOK_DEV, width), conv_weight, recur_gate, input_gate, decay_rate, extra_decay.reshape(SEQS, TOK_DEV))
    gated = gated.reshape(TOKENS, width)
    mixed = (tokens.astype(jnp.float32) + block_sum(gated, lru_output, N_TP) * lru_output_scale).astype(jnp.bfloat16)
    normed2 = rms_rows(mixed, ffn_gain)
    gate_pre = jnp.dot(normed2, ffn_gate.astype(jnp.bfloat16), preferred_element_type=jnp.float32) * ffn_gate_scale
    up_pre = jnp.dot(normed2, ffn_up.astype(jnp.bfloat16), preferred_element_type=jnp.float32) * ffn_up_scale
    hidden = (jax.nn.silu(gate_pre) * up_pre).astype(jnp.bfloat16)
    total = block_sum(hidden, ffn_down, N_TP)
    return (mixed.astype(jnp.float32) + total * ffn_down_scale).astype(jnp.bfloat16)
```

```python
import jax
import jax.numpy as jnp
from jax import lax
from jax.experimental import pallas as pl
from jax.experimental.pallas import tpu as pltpu
from jax.sharding import Mesh
from jax.sharding import PartitionSpec as P

FS = ("fs_0", "fs_1", "fs_2")
REP_FS = ("rep", "fs_0", "fs_1", "fs_2")

EPS = 1e-06
RATE = 8.0
F32 = jnp.float32
BF16 = jnp.bfloat16
CB = 256
LANES = 128


def sigmoid(v):
    return 0.5 + 0.5 * jnp.tanh(0.5 * v)


def normed_rows(values, gain):
    scale = lax.rsqrt(jnp.mean(values * values, axis=-1, keepdims=True) + EPS)
    return (values * scale * gain).astype(BF16)


def dot(a, b):
    return jnp.dot(a, b, preferred_element_type=F32)


def dot_t(a, b):
    return lax.dot_general(a, b, (((1,), (1,)), ((), ())), preferred_element_type=F32)


def mixer_kernel(
    tok, gain, weights, in_scale, gate_scale, taps, gate_maps, rate, extra,
    partial, win, wgate, wout, xn, xpad, a_s, b_s, gel, gated, sems,
):
    length, width = tok.shape
    chans = in_scale.shape[1]
    half = width
    nblk = chans // CB
    copies = []
    for k in range(nblk):
        cols = pl.ds(k * CB, CB)
        for r, dst in ((0, win), (1, wgate)):
            copy = pltpu.make_async_copy(
                weights.at[pl.ds(r * half, half), cols], dst.at[:, cols], sems.at[r, k]
            )
            copy.start()
            copies.append(copy)
    kout = wout.shape[2]
    out_copies = []
    for r in range(2):
        copy = pltpu.make_async_copy(
            weights.at[pl.ds(r * half, half), pl.ds(chans, kout)], wout.at[r], sems.at[2, r]
        )
        copy.start()
        out_copies.append(copy)

    xn[...] = normed_rows(tok[...].astype(F32), gain[...])
    xpad[0:8, :] = jnp.zeros((8, CB), F32)
    groups = chans // LANES
    for k in range(nblk):
        cols = slice(k * CB, (k + 1) * CB)
        copies[2 * k].wait()
        pre = dot(xn[...], win[:, cols]) * in_scale[:, cols]
        xpad[8 : 8 + length, :] = pre.astype(BF16).astype(F32)
        conv = taps[3:4, cols] * xpad[8 : 8 + length, :]
        for j in range(3):
            conv = conv + taps[j : j + 1, cols] * xpad[5 + j : 5 + j + length, :]
        maps = dot(conv.astype(BF16), gate_maps[k])
        recur = sigmoid(maps[:, :CB])
        ingate = sigmoid(maps[:, CB:])
        factor = jnp.exp(rate[:, cols] * recur - extra[...])
        rest = 1.0 - factor * factor
        drive = rest * lax.rsqrt(rest) * (ingate * conv)
        for g in range(CB // LANES):
            row = k * (CB // LANES) + g
            part = slice(g * LANES, (g + 1) * LANES)
            a_s[pl.ds(row, length, stride=groups), :] = factor[:, part]
            b_s[pl.ds(row, length, stride=groups), :] = drive[:, part]
        copies[2 * k + 1].wait()
        pre_gate = (dot(xn[...], wgate[:, cols]) * gate_scale[:, cols]).astype(BF16)
        gel[:, cols] = jax.nn.gelu(pre_gate.astype(F32), approximate=True)

    step = 16

    def scan(i, h):
        base = pl.multiple_of(i * (step * groups), step * groups)
        for s in range(step):
            rows = pl.ds(base + s * groups, groups)
            h = a_s[rows, :] * h + b_s[rows, :]
            b_s[rows, :] = h
        return h

    lax.fori_loop(0, length // step, scan, jnp.zeros((groups, LANES), F32))
    for g in range(groups):
        cols = slice(g * LANES, (g + 1) * LANES)
        gated[:, cols] = (b_s[pl.ds(g, length, stride=groups), :] * gel[:, cols]).astype(BF16)
    for copy in out_copies:
        copy.wait()
    nout = 512
    for k in range(width // nout):
        rows = slice(k * nout, (k + 1) * nout)
        acc = dot_t(gated[:, :kout], wout[0, rows, :]) + dot_t(gated[:, kout:], wout[1, rows, :])
        partial[:, rows] = acc.astype(BF16)


def ffn_kernel(
    place, tok, mine, other, lru_scale, gain, weights, gate_scale, up_scale,
    own, send, mixed_own, wgate, wup, wdown, xn, hid, sems, *, col0, dcol0,
):
    length, width = tok.shape
    hidden = gate_scale.shape[1]
    kdown = wdown.shape[2]
    blocks = [(s, min(512, hidden - s)) for s in range(0, hidden, 512)]
    copies = []
    for k, (s, n) in enumerate(blocks):
        for r, dst in ((0, wgate), (1, wup)):
            copy = pltpu.make_async_copy(
                weights.at[pl.ds(r * width, width), pl.ds(col0 + s, n)],
                dst.at[:, pl.ds(s, n)],
                sems.at[r, k],
            )
            copy.start()
            copies.append(copy)
    down_copies = []
    for r in range(2):
        copy = pltpu.make_async_copy(
            weights.at[pl.ds(r * width, width), pl.ds(dcol0, kdown)], wdown.at[r], sems.at[2, r]
        )
        copy.start()
        down_copies.append(copy)
    total = mine[...].astype(F32) + other[...].astype(F32)
    mixed = (tok[...].astype(F32) + total * lru_scale[...]).astype(BF16)
    cols = width // 2
    tp = place[0]
    mixed_own[...] = jnp.where(tp == 0, mixed[:, :cols], mixed[:, cols:])
    xn[...] = normed_rows(mixed.astype(F32), gain[...])
    for k, (s, n) in enumerate(blocks):
        part = slice(s, s + n)
        copies[2 * k].wait()
        gate = dot(xn[...], wgate[:, part]) * gate_scale[:, part]
        copies[2 * k + 1].wait()
        up = dot(xn[...], wup[:, part]) * up_scale[:, part]
        hid[:, part] = (gate * sigmoid(gate) * up).astype(BF16)
    for copy in down_copies:
        copy.wait()
    skip = 2 * kdown - hidden
    for dst, which in ((send, 1 - tp), (own, tp)):
        rows = pl.ds(pl.multiple_of(which * cols, cols), cols)
        acc = dot_t(hid[:, :kdown], wdown[0, rows, :])
        acc = acc + dot_t(hid[:, kdown:], wdown[1, rows, skip:])
        dst[...] = acc.astype(BF16)


def local(
    tokens, mix_gain, lru_input, lru_gate, lru_input_scale, lru_gate_scale, conv_weight,
    recur_gate, input_gate, decay_rate, extra_decay, lru_output, lru_output_scale, ffn_gain,
    ffn_gate, ffn_up, ffn_gate_scale, ffn_up_scale, ffn_down, ffn_down_scale,
):
    length, cols = tokens.shape
    width = 2 * cols
    chans = lru_input.shape[1]
    hidden = ffn_gate.shape[1]
    rep = lax.axis_index("rep")
    tp = lax.axis_index("tp")
    swap = [(0, 1), (1, 0)]

    out_t, down_t = lru_output.T, ffn_down.T
    kout = chans // 2
    kdown = -(-hidden // (2 * LANES)) * LANES
    skip = hidden - kdown
    first = jnp.concatenate([lru_input, out_t[:, :kout], ffn_gate, down_t[:, :kdown]], axis=1)
    second = jnp.concatenate([lru_gate, out_t[:, kout:], ffn_up, down_t[:, skip:]], axis=1)
    mine = jnp.where(rep == 0, first, second).astype(BF16)
    weights = lax.all_gather(mine, REP_FS, axis=0, tiled=True)

    other = lax.ppermute(tokens, "tp", swap)
    full = jnp.where(
        tp == 0,
        jnp.concatenate([tokens, other], axis=1),
        jnp.concatenate([other, tokens], axis=1),
    )

    per = CB // recur_gate.shape[1]
    eye = jnp.eye(per, dtype=F32)

    def spread(maps):
        nb, bd, _ = maps.shape
        tiles = maps.reshape(nb // per, per, bd, 1, bd) * eye[None, :, None, :, None]
        return tiles.reshape(nb // per, CB, CB)

    gate_maps = jnp.concatenate([spread(recur_gate), spread(input_gate)], axis=2).astype(BF16)
    rate = -RATE * jax.nn.softplus(-decay_rate)

    vmem = pl.BlockSpec(memory_space=pltpu.VMEM)
    hbm = pl.BlockSpec(memory_space=pl.ANY)
    row = lambda v: v.reshape(1, -1)
    groups = chans // LANES
    partial = pl.pallas_call(
        mixer_kernel,
        out_shape=jax.ShapeDtypeStruct((length, width), BF16),
        in_specs=[vmem, vmem, hbm] + [vmem] * 6,
        out_specs=vmem,
        scratch_shapes=[
            pltpu.VMEM((width, chans), BF16),
            pltpu.VMEM((width, chans), BF16),
            pltpu.VMEM((2, width, kout), BF16),
            pltpu.VMEM((length, width), BF16),
            pltpu.VMEM((length + 8, CB), F32),
            pltpu.VMEM((length * groups, LANES), F32),
            pltpu.VMEM((length * groups, LANES), F32),
            pltpu.VMEM((length, chans), F32),
            pltpu.VMEM((length, chans), BF16),
            pltpu.SemaphoreType.DMA((3, chans // CB)),
        ],
        name="mixer",
    )(
        full, row(mix_gain), weights, row(lru_input_scale), row(lru_gate_scale), conv_weight,
        gate_maps, row(rate), extra_decay.reshape(-1, 1),
    )
    theirs = lax.ppermute(partial, "tp", swap)
    own, send, mixed = pl.pallas_call(
        lambda *refs: ffn_kernel(*refs, col0=chans + kout, dcol0=chans + kout + hidden),
        out_shape=[jax.ShapeDtypeStruct((length, cols), BF16)] * 3,
        in_specs=[pl.BlockSpec(memory_space=pltpu.SMEM)] + [vmem] * 5 + [hbm, vmem, vmem],
        out_specs=[vmem] * 3,
        scratch_shapes=[
            pltpu.VMEM((width, hidden), BF16),
            pltpu.VMEM((width, hidden), BF16),
            pltpu.VMEM((2, width, kdown), BF16),
            pltpu.VMEM((length, width), BF16),
            pltpu.VMEM((length, hidden), BF16),
            pltpu.SemaphoreType.DMA((3, 3)),
        ],
        name="ffn",
    )(
        tp.reshape(1).astype(jnp.int32), full, partial, theirs, row(lru_output_scale),
        row(ffn_gain), weights, row(ffn_gate_scale), row(ffn_up_scale),
    )
    got = lax.ppermute(send, "tp", swap)
    scale = lax.dynamic_slice_in_dim(ffn_down_scale, tp * cols, cols)
    total = own.astype(F32) + got.astype(F32)
    return (mixed.astype(F32) + total * scale).astype(BF16)


def solution(mesh):
    split = Mesh(
        mesh.devices.reshape(mesh.shape["rep"], 2, 4, 4, mesh.shape["tp"]),
        ("rep", "fs_0", "fs_1", "fs_2", "tp"),
    )
    in_specs = (
        P(REP_FS, "tp"),
        P(),
        P(FS, "tp"),
        P(FS, "tp"),
        P("tp"),
        P("tp"),
        P(None, "tp"),
        P("tp", None, None),
        P("tp", None, None),
        P("tp"),
        P(REP_FS),
        P("tp", FS),
        P(),
        P(),
        P(FS, "tp"),
        P(FS, "tp"),
        P("tp"),
        P("tp"),
        P("tp", FS),
        P(),
    )
    out_specs = P(REP_FS, "tp")
    return jax.shard_map(local, mesh=split, in_specs=in_specs, out_specs=out_specs, check_vma=False)
```

```python
import jax
import jax.numpy as jnp
from jax import lax
from jax.experimental import pallas as pl
from jax.experimental.pallas import tpu as pltpu
from jax.sharding import Mesh
from jax.sharding import PartitionSpec as P

FS = ("fs_0", "fs_1", "fs_2")
REP_FS = ("rep", "fs_0", "fs_1", "fs_2")

EPS = 1e-06
RATE = 8.0
F32 = jnp.float32
BF16 = jnp.bfloat16
CB = 256
LANES = 128


def sigmoid(v):
    return 0.5 + 0.5 * jnp.tanh(0.5 * v)


def normed_rows(values, gain):
    scale = lax.rsqrt(jnp.mean(values * values, axis=-1, keepdims=True) + EPS)
    return (values * scale * gain).astype(BF16)


def dot(a, b):
    return jnp.dot(a, b, preferred_element_type=F32)


def dot_t(a, b):
    return lax.dot_general(a, b, (((1,), (1,)), ((), ())), preferred_element_type=F32)


def partner(kind, place):
    z, y, x = place
    if kind == "z":
        return z ^ 1, y, x
    if kind == "ye":
        return z, y ^ 1, x
    if kind == "yo":
        return z, (((y + 1) ^ 1) + 3) % 4, x
    if kind == "xe":
        return z, y, x ^ 1
    return z, y, (((x + 1) ^ 1) + 3) % 4


ODD = [(0, 3), (3, 0), (1, 2), (2, 1)]
EVEN = [(0, 1), (1, 0), (2, 3), (3, 2)]
PAIRS = {
    "z": ("fs_0", [(0, 1), (1, 0)]),
    "ye": ("fs_1", EVEN),
    "yo": ("fs_1", ODD),
    "xe": ("fs_2", EVEN),
    "xo": ("fs_2", ODD),
}
KINDS = ("xe", "ye", "xo", "yo", "z")


def order_of(stream):
    return [KINDS[(stream + s) % len(KINDS)] for s in range(len(KINDS))]


def origin(stream, index, place):
    order = order_of(stream)
    for s in reversed(range(len(order))):
        if (index >> s) & 1:
            place = partner(order[s], place)
    z, y, x = place
    return (z * 4 + y) * 4 + x


def spread_streams(parts):
    held = [p[None] for p in parts]
    got = [None] * len(parts)
    for s in range(len(KINDS)):
        for k in range(len(parts)):
            if s > 0:
                held[k] = jnp.concatenate([held[k], got[k]], axis=0)
        for k in range(len(parts)):
            axis, pairs = PAIRS[order_of(k)[s]]
            got[k] = lax.ppermute(held[k], axis, pairs)
    return [(h, g) for h, g in zip(held, got)]


def place_blocks(stream, halves, segments, place):
    count, rows = halves[0].shape[0], halves[0].shape[1]
    for index in range(2 * count):
        at = pl.multiple_of(origin(stream, index, place) * rows, rows)
        source = halves[index // count].at[index % count]
        for col, wide, target, tcol, sem in segments:
            pltpu.make_async_copy(
                source.at[:, pl.ds(col, wide)], target.at[pl.ds(at, rows), pl.ds(tcol, wide)], sem
            ).start()


def wait_for(target, col, wide, sem):
    ref = target.at[:, pl.ds(col, wide)]
    pltpu.make_async_copy(ref, ref, sem).wait()


def front_kernel(
    place, tok, gain, s0a, s0b, s1a, s1b, s2a, s2b, in_scale, gate_scale, taps, gate_maps, rate,
    extra, gated, win, wgate, xn, xpad, a_s, b_s, gel, sems,
):
    length, width = tok.shape
    chans = in_scale.shape[1]
    wide = s0a.shape[2]
    at = (place[0], place[1], place[2])
    left = chans - wide
    place_blocks(0, (s0a, s0b), [(0, wide, win, 0, sems.at[0])], at)
    place_blocks(
        1,
        (s1a, s1b),
        [(0, left, win, wide, sems.at[1]), (left, wide - left, wgate, 0, sems.at[2])],
        at,
    )
    used = wide - left
    place_blocks(2, (s2a, s2b), [(0, chans - used, wgate, used, sems.at[3])], at)
    waits = {
        (0, 0): (win, 0, wide, 0),
        (0, wide): (win, wide, left, 1),
        (1, 0): (wgate, 0, used, 2),
        (1, used): (wgate, used, chans - used, 3),
    }

    xn[...] = normed_rows(tok[...].astype(F32), gain[...])
    xpad[0:8, :] = jnp.zeros((8, CB), F32)
    groups = chans // LANES
    for k in range(chans // CB):
        cols = slice(k * CB, (k + 1) * CB)
        if (0, k * CB) in waits:
            ref, col, w, sem = waits[(0, k * CB)]
            wait_for(ref, col, w, sems.at[sem])
        pre = dot(xn[...], win[:, cols]) * in_scale[:, cols]
        xpad[8 : 8 + length, :] = pre.astype(BF16).astype(F32)
        conv = taps[3:4, cols] * xpad[8 : 8 + length, :]
        for j in range(3):
            conv = conv + taps[j : j + 1, cols] * xpad[5 + j : 5 + j + length, :]
        maps = dot(conv.astype(BF16), gate_maps[k])
        recur = sigmoid(maps[:, :CB])
        ingate = sigmoid(maps[:, CB:])
        factor = jnp.exp(rate[:, cols] * recur - extra[...])
        rest = 1.0 - factor * factor
        drive = rest * lax.rsqrt(rest) * (ingate * conv)
        for g in range(CB // LANES):
            row = k * (CB // LANES) + g
            part = slice(g * LANES, (g + 1) * LANES)
            a_s[pl.ds(row, length, stride=groups), :] = factor[:, part]
            b_s[pl.ds(row, length, stride=groups), :] = drive[:, part]
        if (1, k * CB) in waits:
            ref, col, w, sem = waits[(1, k * CB)]
            wait_for(ref, col, w, sems.at[sem])
        pre_gate = (dot(xn[...], wgate[:, cols]) * gate_scale[:, cols]).astype(BF16)
        gel[:, cols] = jax.nn.gelu(pre_gate.astype(F32), approximate=True)

    step = 16

    def scan(i, h):
        base = pl.multiple_of(i * (step * groups), step * groups)
        for s in range(step):
            rows = pl.ds(base + s * groups, groups)
            h = a_s[rows, :] * h + b_s[rows, :]
            b_s[rows, :] = h
        return h

    lax.fori_loop(0, length // step, scan, jnp.zeros((groups, LANES), F32))
    for g in range(groups):
        cols = slice(g * LANES, (g + 1) * LANES)
        gated[:, cols] = (b_s[pl.ds(g, length, stride=groups), :] * gel[:, cols]).astype(BF16)


def back_kernel(place, gated, s2a, s2b, s3a, s3b, partial, wout, sems):
    chans = gated.shape[1]
    width = partial.shape[1]
    wide = s3a.shape[2]
    at = (place[0], place[1], place[2])
    left = chans - wide
    place_blocks(2, (s2a, s2b), [(wide - left, left, wout, 0, sems.at[0])], at)
    place_blocks(3, (s3a, s3b), [(0, wide, wout, left, sems.at[1])], at)
    wait_for(wout, 0, left, sems.at[0])
    wait_for(wout, left, wide, sems.at[1])
    nout = 512
    for k in range(width // nout):
        rows = slice(k * nout, (k + 1) * nout)
        partial[:, rows] = dot_t(gated[...], wout[rows, :]).astype(BF16)


def mixed_kernel(place, tok, mine, other, lru_scale, gain, mixed_own, xn):
    width = tok.shape[1]
    total = mine[...].astype(F32) + other[...].astype(F32)
    mixed = (tok[...].astype(F32) + total * lru_scale[...]).astype(BF16)
    cols = width // 2
    mixed_own[...] = jnp.where(place[3] == 0, mixed[:, :cols], mixed[:, cols:])
    xn[...] = normed_rows(mixed.astype(F32), gain[...])


def ffn_kernel(
    place, xn, weights, gate_scale, up_scale, own, send, wgate, wup, wdown, hid, sems
):
    length, width = xn.shape
    hidden = gate_scale.shape[1]
    kdown = wdown.shape[2]
    blocks = [(s, min(512, hidden - s)) for s in range(0, hidden, 512)]
    copies = []
    for k, (s, n) in enumerate(blocks):
        for r, dst in ((0, wgate), (1, wup)):
            copy = pltpu.make_async_copy(
                weights.at[pl.ds(r * width, width), pl.ds(s, n)],
                dst.at[:, pl.ds(s, n)],
                sems.at[r, k],
            )
            copy.start()
            copies.append(copy)
    down_copies = []
    for r in range(2):
        copy = pltpu.make_async_copy(
            weights.at[pl.ds(r * width, width), pl.ds(hidden, kdown)], wdown.at[r], sems.at[2, r]
        )
        copy.start()
        down_copies.append(copy)
    cols = width // 2
    tp = place[3]
    for k, (s, n) in enumerate(blocks):
        part = slice(s, s + n)
        copies[2 * k].wait()
        gate = dot(xn[...], wgate[:, part]) * gate_scale[:, part]
        copies[2 * k + 1].wait()
        up = dot(xn[...], wup[:, part]) * up_scale[:, part]
        hid[:, part] = (gate * sigmoid(gate) * up).astype(BF16)
    for copy in down_copies:
        copy.wait()
    skip = 2 * kdown - hidden
    for dst, which in ((send, 1 - tp), (own, tp)):
        rows = pl.ds(pl.multiple_of(which * cols, cols), cols)
        acc = dot_t(hid[:, :kdown], wdown[0, rows, :])
        acc = acc + dot_t(hid[:, kdown:], wdown[1, rows, skip:])
        dst[...] = acc.astype(BF16)


def local(
    tokens, mix_gain, lru_input, lru_gate, lru_input_scale, lru_gate_scale, conv_weight,
    recur_gate, input_gate, decay_rate, extra_decay, lru_output, lru_output_scale, ffn_gain,
    ffn_gate, ffn_up, ffn_gate_scale, ffn_up_scale, ffn_down, ffn_down_scale,
):
    length, cols = tokens.shape
    width = 2 * cols
    chans = lru_input.shape[1]
    hidden = ffn_gate.shape[1]
    rep = lax.axis_index("rep")
    tp = lax.axis_index("tp")
    swap = [(0, 1), (1, 0)]

    out_t, down_t = lru_output.T, ffn_down.T
    kdown = -(-hidden // (2 * LANES)) * LANES
    skip = hidden - kdown
    first = jnp.concatenate([ffn_gate, down_t[:, :kdown]], axis=1)
    second = jnp.concatenate([ffn_up, down_t[:, skip:]], axis=1)
    mine = jnp.where(rep == 0, first, second).astype(BF16)
    weights = lax.all_gather(mine, REP_FS, axis=0, tiled=True)

    wide = 3 * chans // 4
    lru = jnp.concatenate([lru_input, lru_gate, out_t], axis=1).astype(BF16)
    streams = spread_streams([lru[:, k * wide : (k + 1) * wide] for k in range(4)])
    place = jnp.stack(
        [lax.axis_index(axis) for axis in ("fs_0", "fs_1", "fs_2", "tp")]
    ).astype(jnp.int32)

    other = lax.ppermute(tokens, "tp", swap)
    full = jnp.where(
        tp == 0,
        jnp.concatenate([tokens, other], axis=1),
        jnp.concatenate([other, tokens], axis=1),
    )

    per = CB // recur_gate.shape[1]
    eye = jnp.eye(per, dtype=F32)

    def spread(maps):
        nb, bd, _ = maps.shape
        tiles = maps.reshape(nb // per, per, bd, 1, bd) * eye[None, :, None, :, None]
        return tiles.reshape(nb // per, CB, CB)

    gate_maps = jnp.concatenate([spread(recur_gate), spread(input_gate)], axis=2).astype(BF16)
    rate = -RATE * jax.nn.softplus(-decay_rate)

    vmem = pl.BlockSpec(memory_space=pltpu.VMEM)
    hbm = pl.BlockSpec(memory_space=pl.ANY)
    row = lambda v: v.reshape(1, -1)
    groups = chans // LANES
    smem = pl.BlockSpec(memory_space=pltpu.SMEM)
    dma = pltpu.SemaphoreType.DMA
    gated = pl.pallas_call(
        front_kernel,
        out_shape=jax.ShapeDtypeStruct((length, chans), BF16),
        in_specs=[smem, vmem, vmem] + [hbm] * 6 + [vmem] * 6,
        out_specs=vmem,
        scratch_shapes=[
            pltpu.VMEM((width, chans), BF16),
            pltpu.VMEM((width, chans), BF16),
            pltpu.VMEM((length, width), BF16),
            pltpu.VMEM((length + 8, CB), F32),
            pltpu.VMEM((length * groups, LANES), F32),
            pltpu.VMEM((length * groups, LANES), F32),
            pltpu.VMEM((length, chans), F32),
            dma((4,)),
        ],
        name="front",
    )(
        place, full, row(mix_gain), *streams[0], *streams[1], *streams[2], row(lru_input_scale),
        row(lru_gate_scale), conv_weight, gate_maps, row(rate), extra_decay.reshape(-1, 1),
    )
    partial = pl.pallas_call(
        back_kernel,
        out_shape=jax.ShapeDtypeStruct((length, width), BF16),
        in_specs=[smem, vmem] + [hbm] * 4,
        out_specs=vmem,
        scratch_shapes=[pltpu.VMEM((width, chans), BF16), dma((2,))],
        name="back",
    )(place, gated, *streams[2], *streams[3])
    theirs = lax.ppermute(partial, "tp", swap)
    mixed, normed = pl.pallas_call(
        mixed_kernel,
        out_shape=[
            jax.ShapeDtypeStruct((length, cols), BF16),
            jax.ShapeDtypeStruct((length, width), BF16),
        ],
        in_specs=[smem] + [vmem] * 5,
        out_specs=[vmem] * 2,
        name="mixed",
    )(place, full, partial, theirs, row(lru_output_scale), row(ffn_gain))
    own, send = pl.pallas_call(
        ffn_kernel,
        out_shape=[jax.ShapeDtypeStruct((length, cols), BF16)] * 2,
        in_specs=[smem, vmem, hbm, vmem, vmem],
        out_specs=[vmem] * 2,
        scratch_shapes=[
            pltpu.VMEM((width, hidden), BF16),
            pltpu.VMEM((width, hidden), BF16),
            pltpu.VMEM((2, width, kdown), BF16),
            pltpu.VMEM((length, hidden), BF16),
            dma((3, 3)),
        ],
        name="ffn",
    )(place, normed, weights, row(ffn_gate_scale), row(ffn_up_scale))
    got = lax.ppermute(send, "tp", swap)
    scale = lax.dynamic_slice_in_dim(ffn_down_scale, tp * cols, cols)
    total = own.astype(F32) + got.astype(F32)
    return (mixed.astype(F32) + total * scale).astype(BF16)


def solution(mesh):
    split = Mesh(
        mesh.devices.reshape(mesh.shape["rep"], 2, 4, 4, mesh.shape["tp"]),
        ("rep", "fs_0", "fs_1", "fs_2", "tp"),
    )
    in_specs = (
        P(REP_FS, "tp"),
        P(),
        P(FS, "tp"),
        P(FS, "tp"),
        P("tp"),
        P("tp"),
        P(None, "tp"),
        P("tp", None, None),
        P("tp", None, None),
        P("tp"),
        P(REP_FS),
        P("tp", FS),
        P(),
        P(),
        P(FS, "tp"),
        P(FS, "tp"),
        P("tp"),
        P("tp"),
        P("tp", FS),
        P(),
    )
    out_specs = P(REP_FS, "tp")
    return jax.shard_map(local, mesh=split, in_specs=in_specs, out_specs=out_specs, check_vma=False)
```

```python
import jax
import jax.numpy as jnp
from jax import lax
from jax.experimental import pallas as pl
from jax.experimental.pallas import tpu as pltpu
from jax.sharding import Mesh
from jax.sharding import PartitionSpec as P

FS = ("fs_0", "fs_1", "fs_2")
REP_FS = ("rep", "fs_0", "fs_1", "fs_2")

EPS = 1e-06
RATE = 8.0
F32 = jnp.float32
BF16 = jnp.bfloat16
CB = 256
LANES = 128


def sigmoid(v):
    return 0.5 + 0.5 * jnp.tanh(0.5 * v)


def dot(a, b):
    return jnp.dot(a, b, preferred_element_type=F32)


def dot_t(a, b):
    return lax.dot_general(a, b, (((1,), (1,)), ((), ())), preferred_element_type=F32)


def partner(kind, place):
    z, y, x = place
    if kind == "z":
        return z ^ 1, y, x
    if kind == "ye":
        return z, y ^ 1, x
    if kind == "yo":
        return z, (((y + 1) ^ 1) + 3) % 4, x
    if kind == "xe":
        return z, y, x ^ 1
    return z, y, (((x + 1) ^ 1) + 3) % 4


ODD = [(0, 3), (3, 0), (1, 2), (2, 1)]
EVEN = [(0, 1), (1, 0), (2, 3), (3, 2)]
PAIRS = {
    "z": ("fs_0", [(0, 1), (1, 0)]),
    "ye": ("fs_1", EVEN),
    "yo": ("fs_1", ODD),
    "xe": ("fs_2", EVEN),
    "xo": ("fs_2", ODD),
}
KINDS = ("xe", "ye", "xo", "yo")


def order_of(stream):
    return ["z"] + [KINDS[(stream + s) % len(KINDS)] for s in range(len(KINDS))]


def origin(stream, index, place):
    order = order_of(stream)
    for s in reversed(range(len(order))):
        if (index >> s) & 1:
            place = partner(order[s], place)
    z, y, x = place
    return (z * 4 + y) * 4 + x


def spread_streams(held):
    got = [None] * len(held)
    for s in range(len(KINDS)):
        for k in range(len(held)):
            if s > 0:
                joined = jnp.concatenate([held[k], got[k]], axis=0)
                held[k] = lax.optimization_barrier(joined)
        for k in range(len(held)):
            axis, pairs = PAIRS[order_of(k)[s + 1]]
            got[k] = lax.ppermute(held[k], axis, pairs)
    return [(h, g) for h, g in zip(held, got)]


def place_blocks(stream, halves, target, place, sem):
    count, rows = halves[0].shape[0], halves[0].shape[1]
    for index in range(2 * count):
        at = pl.multiple_of(origin(stream, index, place) * rows, rows)
        source = halves[index // count].at[index % count]
        pltpu.make_async_copy(source, target.at[pl.ds(at, rows)], sem).start()


def wait_for(target, sem):
    pltpu.make_async_copy(target, target, sem).wait()


def put_halves(xn, mine, other, gain, tp):
    cols = mine.shape[1]
    a, b = mine[...].astype(F32), other[...].astype(F32)
    squares = jnp.sum(a * a, axis=-1, keepdims=True) + jnp.sum(b * b, axis=-1, keepdims=True)
    scale = lax.rsqrt(squares * (1.0 / (2 * cols)) + EPS)
    low, high = gain[:, :cols], gain[:, cols:]
    first = tp == 0
    a = (a * scale * jnp.where(first, low, high)).astype(BF16)
    b = (b * scale * jnp.where(first, high, low)).astype(BF16)

    @pl.when(first)
    def _():
        xn[:, :cols] = a
        xn[:, cols:] = b

    @pl.when(jnp.logical_not(first))
    def _():
        xn[:, :cols] = b
        xn[:, cols:] = a


def front_kernel(
    place, mine, other, gain, s0a, s0b, s1a, s1b, in_scale, gate_scale, taps, maps_r, maps_i,
    rate, extra, gated, win, wgate, xn, xpad, a_s, b_s, gel, block_maps, sems,
):
    length = mine.shape[0]
    chans = win.shape[1]
    at = (place[0], place[1], place[2])
    place_blocks(0, (s0a, s0b), win, at, sems.at[0])
    place_blocks(1, (s1a, s1b), wgate, at, sems.at[1])
    low = place[0] == 0

    def half(ref):
        return jnp.where(low, ref[:, :chans], ref[:, chans:])

    bd = maps_r.shape[1]
    per = CB // bd
    block_maps[...] = jnp.zeros(block_maps.shape, BF16)
    for n in range(chans // bd):
        k, i = n // per, n % per
        which = place[0] * (chans // bd) + n
        rows, cols = slice(i * bd, (i + 1) * bd), slice(i * bd, (i + 1) * bd)
        block_maps[k, rows, cols] = maps_r[which].astype(BF16)
        block_maps[k, rows, slice(CB + i * bd, CB + (i + 1) * bd)] = maps_i[which].astype(BF16)

    in_s, gate_s, tap, slope = half(in_scale), half(gate_scale), half(taps), half(rate)
    put_halves(xn, mine, other, gain, place[3])
    xpad[0:8, :] = jnp.zeros((8, CB), F32)
    groups = chans // LANES
    wait_for(win, sems.at[0])
    for k in range(chans // CB):
        cols = slice(k * CB, (k + 1) * CB)
        pre = dot(xn[...], win[:, cols]) * in_s[:, cols]
        xpad[8 : 8 + length, :] = pre.astype(BF16).astype(F32)
        conv = tap[3:4, cols] * xpad[8 : 8 + length, :]
        for j in range(3):
            conv = conv + tap[j : j + 1, cols] * xpad[5 + j : 5 + j + length, :]
        maps = dot(conv.astype(BF16), block_maps[k])
        recur = sigmoid(maps[:, :CB])
        ingate = sigmoid(maps[:, CB:])
        factor = jnp.exp(slope[:, cols] * recur - extra[...])
        rest = 1.0 - factor * factor
        drive = rest * lax.rsqrt(rest) * (ingate * conv)
        for g in range(CB // LANES):
            row = k * (CB // LANES) + g
            part = slice(g * LANES, (g + 1) * LANES)
            a_s[pl.ds(row, length, stride=groups), :] = factor[:, part]
            b_s[pl.ds(row, length, stride=groups), :] = drive[:, part]
    wait_for(wgate, sems.at[1])
    for k in range(chans // CB):
        cols = slice(k * CB, (k + 1) * CB)
        pre_gate = (dot(xn[...], wgate[:, cols]) * gate_s[:, cols]).astype(BF16)
        gel[:, cols] = jax.nn.gelu(pre_gate.astype(F32), approximate=True)

    step = 16

    def scan(i, h):
        base = pl.multiple_of(i * (step * groups), step * groups)
        for s in range(step):
            rows = pl.ds(base + s * groups, groups)
            h = a_s[rows, :] * h + b_s[rows, :]
            b_s[rows, :] = h
        return h

    lax.fori_loop(0, length // step, scan, jnp.zeros((groups, LANES), F32))
    for g in range(groups):
        cols = slice(g * LANES, (g + 1) * LANES)
        gated[:, cols] = (b_s[pl.ds(g, length, stride=groups), :] * gel[:, cols]).astype(BF16)


def back_kernel(place, gated, s2a, s2b, keep, send, wout, sem):
    cols = keep.shape[1]
    place_blocks(2, (s2a, s2b), wout, (place[0], place[1], place[2]), sem.at[0])
    wait_for(wout, sem.at[0])
    tp = place[3]
    for dst, which in ((send, 1 - tp), (keep, tp)):
        rows = pl.ds(pl.multiple_of(which * cols, cols), cols)
        dst[...] = dot_t(gated[...], wout[rows, :]).astype(BF16)


def norm_kernel(place, mine, other, gain, xn):
    put_halves(xn, mine, other, gain, place[3])


def ffn_kernel(
    place, xn, weights, gate_scale, up_scale, own, send, wgate, wup, wdown, hid, sems
):
    length, width = xn.shape
    hidden = gate_scale.shape[1]
    kdown = wdown.shape[2]
    blocks = [(s, min(512, hidden - s)) for s in range(0, hidden, 512)]
    copies = []
    for k, (s, n) in enumerate(blocks):
        for r, dst in ((0, wgate), (1, wup)):
            copy = pltpu.make_async_copy(
                weights.at[pl.ds(r * width, width), pl.ds(s, n)],
                dst.at[:, pl.ds(s, n)],
                sems.at[r, k],
            )
            copy.start()
            copies.append(copy)
    down_copies = []
    for r in range(2):
        copy = pltpu.make_async_copy(
            weights.at[pl.ds(r * width, width), pl.ds(hidden, kdown)], wdown.at[r], sems.at[2, r]
        )
        copy.start()
        down_copies.append(copy)
    cols = width // 2
    tp = place[3]
    for k, (s, n) in enumerate(blocks):
        part = slice(s, s + n)
        copies[2 * k].wait()
        gate = dot(xn[...], wgate[:, part]) * gate_scale[:, part]
        copies[2 * k + 1].wait()
        up = dot(xn[...], wup[:, part]) * up_scale[:, part]
        hid[:, part] = (gate * sigmoid(gate) * up).astype(BF16)
    for copy in down_copies:
        copy.wait()
    skip = 2 * kdown - hidden
    for dst, which in ((send, 1 - tp), (own, tp)):
        rows = pl.ds(pl.multiple_of(which * cols, cols), cols)
        acc = dot_t(hid[:, :kdown], wdown[0, rows, :])
        acc = acc + dot_t(hid[:, kdown:], wdown[1, rows, skip:])
        dst[...] = acc.astype(BF16)


def local(
    tokens, mix_gain, lru_input, lru_gate, lru_input_scale, lru_gate_scale, conv_weight,
    recur_gate, input_gate, decay_rate, extra_decay, lru_output, lru_output_scale, ffn_gain,
    ffn_gate, ffn_up, ffn_gate_scale, ffn_up_scale, ffn_down, ffn_down_scale,
):
    length, cols = tokens.shape
    width = 2 * cols
    chans = lru_input.shape[1] // 2
    hidden = ffn_gate.shape[1]
    rep = lax.axis_index("rep")
    tp = lax.axis_index("tp")
    zed = lax.axis_index("fs_0")
    swap = [(0, 1), (1, 0)]
    place = jnp.stack(
        [lax.axis_index(axis) for axis in ("fs_0", "fs_1", "fs_2", "tp")]
    ).astype(jnp.int32)

    down_t = ffn_down.T
    kdown = -(-hidden // (2 * LANES)) * LANES
    skip = hidden - kdown
    first = jnp.concatenate([ffn_gate, down_t[:, :kdown]], axis=1)
    second = jnp.concatenate([ffn_up, down_t[:, skip:]], axis=1)
    mine = jnp.where(rep == 0, first, second).astype(BF16)
    weights = lax.all_gather(mine, REP_FS, axis=0, tiled=True)

    lru = (lru_input, lru_gate, lru_output.T)
    low = jnp.concatenate([w[:, :chans] for w in lru], axis=1).astype(BF16)
    high = jnp.concatenate([w[:, chans:] for w in lru], axis=1).astype(BF16)
    away = lax.ppermute(jnp.where(zed == 0, high, low), "fs_0", swap)
    home = jnp.where(zed == 0, low, high)
    streams = spread_streams(
        [
            jnp.stack([home[:, k * chans : (k + 1) * chans], away[:, k * chans : (k + 1) * chans]])
            for k in range(3)
        ]
    )

    guest = lax.ppermute(tokens, "fs_0", swap)
    guest_extra = lax.ppermute(extra_decay, "fs_0", swap)
    guest_other = lax.ppermute(guest, "tp", swap)
    tokens_other = lax.ppermute(tokens, "tp", swap)
    rate = -RATE * jax.nn.softplus(-decay_rate)

    vmem = pl.BlockSpec(memory_space=pltpu.VMEM)
    hbm = pl.BlockSpec(memory_space=pl.ANY)
    smem = pl.BlockSpec(memory_space=pltpu.SMEM)
    dma = pltpu.SemaphoreType.DMA
    row = lambda v: v.reshape(1, -1)
    groups = chans // LANES
    half_rows = jax.ShapeDtypeStruct((length, cols), BF16)

    def mix(mine, other, extra):
        gated = pl.pallas_call(
            front_kernel,
            out_shape=jax.ShapeDtypeStruct((length, chans), BF16),
            in_specs=[smem, vmem, vmem, vmem] + [hbm] * 4 + [vmem] * 7,
            out_specs=vmem,
            scratch_shapes=[
                pltpu.VMEM((width, chans), BF16),
                pltpu.VMEM((width, chans), BF16),
                pltpu.VMEM((length, width), BF16),
                pltpu.VMEM((length + 8, CB), F32),
                pltpu.VMEM((length * groups, LANES), F32),
                pltpu.VMEM((length * groups, LANES), F32),
                pltpu.VMEM((length, chans), F32),
                pltpu.VMEM((chans // CB, CB, 2 * CB), BF16),
                dma((2,)),
            ],
            name="front",
        )(
            place, mine, other, row(mix_gain), *streams[0], *streams[1], row(lru_input_scale),
            row(lru_gate_scale), conv_weight, recur_gate, input_gate, row(rate),
            extra.reshape(-1, 1),
        )
        return pl.pallas_call(
            back_kernel,
            out_shape=[half_rows] * 2,
            in_specs=[smem, vmem] + [hbm] * 2,
            out_specs=[vmem] * 2,
            scratch_shapes=[pltpu.VMEM((width, chans), BF16), dma((1,))],
            name="back",
        )(place, gated, *streams[2])

    keep, send = mix(guest, guest_other, guest_extra)
    got = lax.ppermute(send, "tp", swap)
    sums = (keep.astype(F32) + got.astype(F32)).astype(BF16)
    tokens_in, sums = lax.optimization_barrier((tokens, sums))
    away_sums = lax.ppermute(sums, "fs_0", swap)
    own_keep, own_send = mix(tokens_in, tokens_other, extra_decay)
    own_got = lax.ppermute(own_send, "tp", swap)
    total = own_keep.astype(F32) + own_got.astype(F32) + away_sums.astype(F32)
    out_scale = lax.dynamic_slice_in_dim(lru_output_scale, tp * cols, cols)
    mixed = (tokens.astype(F32) + total * out_scale).astype(BF16)
    mixed_other = lax.ppermute(mixed, "tp", swap)
    normed = pl.pallas_call(
        norm_kernel,
        out_shape=jax.ShapeDtypeStruct((length, width), BF16),
        in_specs=[smem] + [vmem] * 3,
        out_specs=vmem,
        name="norm",
    )(place, mixed, mixed_other, row(ffn_gain))
    own, send = pl.pallas_call(
        ffn_kernel,
        out_shape=[half_rows] * 2,
        in_specs=[smem, vmem, hbm, vmem, vmem],
        out_specs=[vmem] * 2,
        scratch_shapes=[
            pltpu.VMEM((width, hidden), BF16),
            pltpu.VMEM((width, hidden), BF16),
            pltpu.VMEM((2, width, kdown), BF16),
            pltpu.VMEM((length, hidden), BF16),
            dma((3, 3)),
        ],
        name="ffn",
    )(place, normed, weights, row(ffn_gate_scale), row(ffn_up_scale))
    got = lax.ppermute(send, "tp", swap)
    scale = lax.dynamic_slice_in_dim(ffn_down_scale, tp * cols, cols)
    total = own.astype(F32) + got.astype(F32)
    return (mixed.astype(F32) + total * scale).astype(BF16)


def solution(mesh):
    split = Mesh(
        mesh.devices.reshape(mesh.shape["rep"], 2, 4, 4, mesh.shape["tp"]),
        ("rep", "fs_0", "fs_1", "fs_2", "tp"),
    )
    in_specs = (
        P(REP_FS, "tp"),
        P(),
        P(FS, "tp"),
        P(FS, "tp"),
        P("tp"),
        P("tp"),
        P(None, "tp"),
        P("tp", None, None),
        P("tp", None, None),
        P("tp"),
        P(REP_FS),
        P("tp", FS),
        P(),
        P(),
        P(FS, "tp"),
        P(FS, "tp"),
        P("tp"),
        P("tp"),
        P("tp", FS),
        P(),
    )
    out_specs = P(REP_FS, "tp")
    return jax.shard_map(local, mesh=split, in_specs=in_specs, out_specs=out_specs, check_vma=False)
```

```python
import jax
import jax.numpy as jnp
from jax import lax
from jax.experimental import pallas as pl
from jax.experimental.pallas import tpu as pltpu
from jax.sharding import Mesh
from jax.sharding import PartitionSpec as P

FS = ("fs_0", "fs_1", "fs_2")
REP_FS = ("rep", "fs_0", "fs_1", "fs_2")

EPS = 1e-06
RATE = 8.0
F32 = jnp.float32
BF16 = jnp.bfloat16
CB = 256
LANES = 128


def sigmoid(v):
    return 0.5 + 0.5 * jnp.tanh(0.5 * v)


def dot(a, b):
    return jnp.dot(a, b, preferred_element_type=F32)


def dot_t(a, b):
    return lax.dot_general(a, b, (((1,), (1,)), ((), ())), preferred_element_type=F32)


def partner(kind, place):
    z, y, x = place
    if kind == "z":
        return z ^ 1, y, x
    if kind == "ye":
        return z, y ^ 1, x
    if kind == "yo":
        return z, (((y + 1) ^ 1) + 3) % 4, x
    if kind == "xe":
        return z, y, x ^ 1
    return z, y, (((x + 1) ^ 1) + 3) % 4


ODD = [(0, 3), (3, 0), (1, 2), (2, 1)]
EVEN = [(0, 1), (1, 0), (2, 3), (3, 2)]
PAIRS = {
    "z": ("fs_0", [(0, 1), (1, 0)]),
    "ye": ("fs_1", EVEN),
    "yo": ("fs_1", ODD),
    "xe": ("fs_2", EVEN),
    "xo": ("fs_2", ODD),
}
KINDS = ("xe", "ye", "xo", "yo")


def order_of(stream):
    return ["z"] + [KINDS[(stream + s) % len(KINDS)] for s in range(len(KINDS))]


def origin(stream, index, place):
    order = order_of(stream)
    for s in reversed(range(len(order))):
        if (index >> s) & 1:
            place = partner(order[s], place)
    z, y, x = place
    return (z * 4 + y) * 4 + x


def spread_streams(held):
    got = [None] * len(held)
    for s in range(len(KINDS)):
        for k in range(len(held)):
            if s > 0:
                joined = jnp.concatenate([held[k], got[k]], axis=0)
                held[k] = lax.optimization_barrier(joined)
        for k in range(len(held)):
            axis, pairs = PAIRS[order_of(k)[s + 1]]
            got[k] = lax.ppermute(held[k], axis, pairs)
    return [(h, g) for h, g in zip(held, got)]


def place_blocks(stream, halves, target, place, sem):
    count, rows = halves[0].shape[0], halves[0].shape[1]
    for index in range(2 * count):
        at = pl.multiple_of(origin(stream, index, place) * rows, rows)
        source = halves[index // count].at[index % count]
        pltpu.make_async_copy(source, target.at[pl.ds(at, rows)], sem).start()


def wait_for(target, sem):
    pltpu.make_async_copy(target, target, sem).wait()


def put_halves(xn, mine, other, gain, tp):
    cols = mine.shape[1]
    a, b = mine[...].astype(F32), other[...].astype(F32)
    squares = jnp.sum(a * a, axis=-1, keepdims=True) + jnp.sum(b * b, axis=-1, keepdims=True)
    scale = lax.rsqrt(squares * (1.0 / (2 * cols)) + EPS)
    low, high = gain[:, :cols], gain[:, cols:]
    first = tp == 0
    a = (a * scale * jnp.where(first, low, high)).astype(BF16)
    b = (b * scale * jnp.where(first, high, low)).astype(BF16)

    @pl.when(first)
    def _():
        xn[:, :cols] = a
        xn[:, cols:] = b

    @pl.when(jnp.logical_not(first))
    def _():
        xn[:, :cols] = b
        xn[:, cols:] = a


def front_kernel(
    place, mine, other, gain, s0a, s0b, s1a, s1b, in_scale, gate_scale, taps, maps_r, maps_i,
    rate, extra, gated, win, wgate, xn, xpad, a_s, b_s, gel, block_maps, sems,
):
    length = mine.shape[0]
    chans = win.shape[1]
    at = (place[0], place[1], place[2])
    place_blocks(0, (s0a, s0b), win, at, sems.at[0])
    place_blocks(1, (s1a, s1b), wgate, at, sems.at[1])
    low = place[0] == 0

    def half(ref):
        return jnp.where(low, ref[:, :chans], ref[:, chans:])

    bd = maps_r.shape[1]
    per = CB // bd
    block_maps[...] = jnp.zeros(block_maps.shape, BF16)
    for n in range(chans // bd):
        k, i = n // per, n % per
        which = place[0] * (chans // bd) + n
        rows, cols = slice(i * bd, (i + 1) * bd), slice(i * bd, (i + 1) * bd)
        block_maps[k, rows, cols] = maps_r[which].astype(BF16)
        block_maps[k, rows, slice(CB + i * bd, CB + (i + 1) * bd)] = maps_i[which].astype(BF16)

    in_s, gate_s, tap, slope = half(in_scale), half(gate_scale), half(taps), half(rate)
    put_halves(xn, mine, other, gain, place[3])
    xpad[0:8, :] = jnp.zeros((8, CB), F32)
    groups = chans // LANES
    wait_for(win, sems.at[0])
    for k in range(chans // CB):
        cols = slice(k * CB, (k + 1) * CB)
        pre = dot(xn[...], win[:, cols]) * in_s[:, cols]
        xpad[8 : 8 + length, :] = pre.astype(BF16).astype(F32)
        conv = tap[3:4, cols] * xpad[8 : 8 + length, :]
        for j in range(3):
            conv = conv + tap[j : j + 1, cols] * xpad[5 + j : 5 + j + length, :]
        maps = dot(conv.astype(BF16), block_maps[k])
        recur = sigmoid(maps[:, :CB])
        ingate = sigmoid(maps[:, CB:])
        factor = jnp.exp(slope[:, cols] * recur - extra[...])
        rest = 1.0 - factor * factor
        drive = rest * lax.rsqrt(rest) * (ingate * conv)
        for g in range(CB // LANES):
            row = k * (CB // LANES) + g
            part = slice(g * LANES, (g + 1) * LANES)
            a_s[pl.ds(row, length, stride=groups), :] = factor[:, part]
            b_s[pl.ds(row, length, stride=groups), :] = drive[:, part]
    wait_for(wgate, sems.at[1])
    for k in range(chans // CB):
        cols = slice(k * CB, (k + 1) * CB)
        pre_gate = (dot(xn[...], wgate[:, cols]) * gate_s[:, cols]).astype(BF16)
        gel[:, cols] = jax.nn.gelu(pre_gate.astype(F32), approximate=True)

    step = 16

    def scan(i, h):
        base = pl.multiple_of(i * (step * groups), step * groups)
        for s in range(step):
            rows = pl.ds(base + s * groups, groups)
            h = a_s[rows, :] * h + b_s[rows, :]
            b_s[rows, :] = h
        return h

    lax.fori_loop(0, length // step, scan, jnp.zeros((groups, LANES), F32))
    for g in range(groups):
        cols = slice(g * LANES, (g + 1) * LANES)
        gated[:, cols] = (b_s[pl.ds(g, length, stride=groups), :] * gel[:, cols]).astype(BF16)


def back_kernel(place, mine, other, s2a, s2b, s3a, s3b, partial, w0, w1, sems):
    at = (place[0], place[1], place[2])
    place_blocks(2, (s2a, s2b), w0, at, sems.at[0])
    place_blocks(3, (s3a, s3b), w1, at, sems.at[1])
    low = place[0] == 0
    g0 = jnp.where(low, mine[...], other[...])
    g1 = jnp.where(low, other[...], mine[...])
    wait_for(w0, sems.at[0])
    wait_for(w1, sems.at[1])
    cols = partial.shape[2]
    for c in range(2):
        rows = slice(c * cols, (c + 1) * cols)
        partial[c] = (dot_t(g0, w0[rows, :]) + dot_t(g1, w1[rows, :])).astype(BF16)


def mixed_kernel(place, tok_mine, tok_other, part, got, out_scale, gain, mixed, xn, hold):
    tp = place[3]

    def mix(tok, which):
        total = part[which].astype(F32) + got[which].astype(F32)
        return (tok[...].astype(F32) + total * out_scale[which]).astype(BF16)

    mixed[...] = mix(tok_mine, tp)
    hold[...] = mix(tok_other, 1 - tp)
    put_halves(xn, mixed, hold, gain, tp)


def ffn_kernel(
    place, xn, weights, gate_scale, up_scale, own, send, wgate, wup, wdown, hid, sems
):
    length, width = xn.shape
    hidden = gate_scale.shape[1]
    kdown = wdown.shape[2]
    blocks = [(s, min(512, hidden - s)) for s in range(0, hidden, 512)]
    copies = []
    for k, (s, n) in enumerate(blocks):
        for r, dst in ((0, wgate), (1, wup)):
            copy = pltpu.make_async_copy(
                weights.at[pl.ds(r * width, width), pl.ds(s, n)],
                dst.at[:, pl.ds(s, n)],
                sems.at[r, k],
            )
            copy.start()
            copies.append(copy)
    down_copies = []
    for r in range(2):
        copy = pltpu.make_async_copy(
            weights.at[pl.ds(r * width, width), pl.ds(hidden, kdown)], wdown.at[r], sems.at[2, r]
        )
        copy.start()
        down_copies.append(copy)
    cols = width // 2
    tp = place[3]
    for k, (s, n) in enumerate(blocks):
        part = slice(s, s + n)
        copies[2 * k].wait()
        gate = dot(xn[...], wgate[:, part]) * gate_scale[:, part]
        copies[2 * k + 1].wait()
        up = dot(xn[...], wup[:, part]) * up_scale[:, part]
        hid[:, part] = (gate * sigmoid(gate) * up).astype(BF16)
    for copy in down_copies:
        copy.wait()
    skip = 2 * kdown - hidden
    for dst, which in ((send, 1 - tp), (own, tp)):
        rows = pl.ds(pl.multiple_of(which * cols, cols), cols)
        acc = dot_t(hid[:, :kdown], wdown[0, rows, :])
        acc = acc + dot_t(hid[:, kdown:], wdown[1, rows, skip:])
        dst[...] = acc.astype(BF16)


def local(
    tokens, mix_gain, lru_input, lru_gate, lru_input_scale, lru_gate_scale, conv_weight,
    recur_gate, input_gate, decay_rate, extra_decay, lru_output, lru_output_scale, ffn_gain,
    ffn_gate, ffn_up, ffn_gate_scale, ffn_up_scale, ffn_down, ffn_down_scale,
):
    length, cols = tokens.shape
    width = 2 * cols
    chans = lru_input.shape[1] // 2
    hidden = ffn_gate.shape[1]
    rep = lax.axis_index("rep")
    tp = lax.axis_index("tp")
    zed = lax.axis_index("fs_0")
    swap = [(0, 1), (1, 0)]
    place = jnp.stack(
        [lax.axis_index(axis) for axis in ("fs_0", "fs_1", "fs_2", "tp")]
    ).astype(jnp.int32)

    down_t = ffn_down.T
    kdown = -(-hidden // (2 * LANES)) * LANES
    skip = hidden - kdown
    first = jnp.concatenate([ffn_gate, down_t[:, :kdown]], axis=1)
    second = jnp.concatenate([ffn_up, down_t[:, skip:]], axis=1)
    mine = jnp.where(rep == 0, first, second).astype(BF16)
    weights = lax.all_gather(mine, REP_FS, axis=0, tiled=True)

    lru = (lru_input, lru_gate)
    low = jnp.concatenate([w[:, :chans] for w in lru], axis=1).astype(BF16)
    high = jnp.concatenate([w[:, chans:] for w in lru], axis=1).astype(BF16)
    out = lru_output.T.astype(BF16)
    away = jnp.concatenate([jnp.where(zed == 0, high, low), out], axis=1)
    away = lax.ppermute(away, "fs_0", swap)
    home = jnp.where(zed == 0, low, high)
    out = jnp.concatenate([home, out], axis=1)
    streams = spread_streams(
        [
            jnp.stack([h[:, k * chans : (k + 1) * chans], a[:, k * chans : (k + 1) * chans]])
            for h, a, k in ((home, away, 0), (home, away, 1), (out, away, 2), (out, away, 3))
        ]
    )

    guest = lax.ppermute(tokens, "fs_0", swap)
    guest_extra = lax.ppermute(extra_decay, "fs_0", swap)
    guest_other = lax.ppermute(guest, "tp", swap)
    tokens_other = lax.ppermute(tokens, "tp", swap)
    rate = -RATE * jax.nn.softplus(-decay_rate)

    vmem = pl.BlockSpec(memory_space=pltpu.VMEM)
    hbm = pl.BlockSpec(memory_space=pl.ANY)
    smem = pl.BlockSpec(memory_space=pltpu.SMEM)
    dma = pltpu.SemaphoreType.DMA
    row = lambda v: v.reshape(1, -1)
    groups = chans // LANES
    half_rows = jax.ShapeDtypeStruct((length, cols), BF16)

    def mix(mine, other, extra):
        return pl.pallas_call(
            front_kernel,
            out_shape=jax.ShapeDtypeStruct((length, chans), BF16),
            in_specs=[smem, vmem, vmem, vmem] + [hbm] * 4 + [vmem] * 7,
            out_specs=vmem,
            scratch_shapes=[
                pltpu.VMEM((width, chans), BF16),
                pltpu.VMEM((width, chans), BF16),
                pltpu.VMEM((length, width), BF16),
                pltpu.VMEM((length + 8, CB), F32),
                pltpu.VMEM((length * groups, LANES), F32),
                pltpu.VMEM((length * groups, LANES), F32),
                pltpu.VMEM((length, chans), F32),
                pltpu.VMEM((chans // CB, CB, 2 * CB), BF16),
                dma((2,)),
            ],
            name="front",
        )(
            place, mine, other, row(mix_gain), *streams[0], *streams[1], row(lru_input_scale),
            row(lru_gate_scale), conv_weight, recur_gate, input_gate, row(rate),
            extra.reshape(-1, 1),
        )

    guest_gated = mix(guest, guest_other, guest_extra)
    tokens_in, guest_gated = lax.optimization_barrier((tokens, guest_gated))
    gated_away = lax.ppermute(guest_gated, "fs_0", swap)
    gated = mix(tokens_in, tokens_other, extra_decay)
    partial = pl.pallas_call(
        back_kernel,
        out_shape=jax.ShapeDtypeStruct((2, length, cols), BF16),
        in_specs=[smem, vmem, vmem] + [hbm] * 4,
        out_specs=vmem,
        scratch_shapes=[
            pltpu.VMEM((width, chans), BF16),
            pltpu.VMEM((width, chans), BF16),
            dma((2,)),
        ],
        name="back",
    )(place, gated, gated_away, *streams[2], *streams[3])
    got = lax.ppermute(partial, "tp", swap)
    mixed, normed = pl.pallas_call(
        mixed_kernel,
        out_shape=[half_rows, jax.ShapeDtypeStruct((length, width), BF16)],
        in_specs=[smem] + [vmem] * 6,
        out_specs=[vmem] * 2,
        scratch_shapes=[pltpu.VMEM((length, cols), BF16)],
        name="mixed",
    )(
        place, tokens, tokens_other, partial, got, lru_output_scale.reshape(2, 1, cols),
        row(ffn_gain),
    )
    own, send = pl.pallas_call(
        ffn_kernel,
        out_shape=[half_rows] * 2,
        in_specs=[smem, vmem, hbm, vmem, vmem],
        out_specs=[vmem] * 2,
        scratch_shapes=[
            pltpu.VMEM((width, hidden), BF16),
            pltpu.VMEM((width, hidden), BF16),
            pltpu.VMEM((2, width, kdown), BF16),
            pltpu.VMEM((length, hidden), BF16),
            dma((3, 3)),
        ],
        name="ffn",
    )(place, normed, weights, row(ffn_gate_scale), row(ffn_up_scale))
    got = lax.ppermute(send, "tp", swap)
    scale = lax.dynamic_slice_in_dim(ffn_down_scale, tp * cols, cols)
    total = own.astype(F32) + got.astype(F32)
    return (mixed.astype(F32) + total * scale).astype(BF16)


def solution(mesh):
    split = Mesh(
        mesh.devices.reshape(mesh.shape["rep"], 2, 4, 4, mesh.shape["tp"]),
        ("rep", "fs_0", "fs_1", "fs_2", "tp"),
    )
    in_specs = (
        P(REP_FS, "tp"),
        P(),
        P(FS, "tp"),
        P(FS, "tp"),
        P("tp"),
        P("tp"),
        P(None, "tp"),
        P("tp", None, None),
        P("tp", None, None),
        P("tp"),
        P(REP_FS),
        P("tp", FS),
        P(),
        P(),
        P(FS, "tp"),
        P(FS, "tp"),
        P("tp"),
        P("tp"),
        P("tp", FS),
        P(),
    )
    out_specs = P(REP_FS, "tp")
    return jax.shard_map(local, mesh=split, in_specs=in_specs, out_specs=out_specs, check_vma=False)
```

```python
import jax
import jax.numpy as jnp
from jax import lax
from jax.experimental import pallas as pl
from jax.experimental.pallas import tpu as pltpu
from jax.sharding import Mesh
from jax.sharding import PartitionSpec as P

FS = ("fs_0", "fs_1", "fs_2")
REP_FS = ("rep", "fs_0", "fs_1", "fs_2")

EPS = 1e-06
RATE = 8.0
F32 = jnp.float32
BF16 = jnp.bfloat16
CB = 256
LANES = 128


def sigmoid(v):
    return 0.5 + 0.5 * jnp.tanh(0.5 * v)


def dot(a, b):
    return jnp.dot(a, b, preferred_element_type=F32)


def dot_t(a, b):
    return lax.dot_general(a, b, (((1,), (1,)), ((), ())), preferred_element_type=F32)


def partner(kind, place):
    z, y, x = place
    if kind == "z":
        return z ^ 1, y, x
    if kind == "ye":
        return z, y ^ 1, x
    if kind == "yo":
        return z, (((y + 1) ^ 1) + 3) % 4, x
    if kind == "xe":
        return z, y, x ^ 1
    return z, y, (((x + 1) ^ 1) + 3) % 4


ODD = [(0, 3), (3, 0), (1, 2), (2, 1)]
EVEN = [(0, 1), (1, 0), (2, 3), (3, 2)]
PAIRS = {
    "z": ("fs_0", [(0, 1), (1, 0)]),
    "ye": ("fs_1", EVEN),
    "yo": ("fs_1", ODD),
    "xe": ("fs_2", EVEN),
    "xo": ("fs_2", ODD),
}
KINDS = ("xe", "ye", "xo", "yo")


def order_of(stream):
    return ["z"] + [KINDS[(stream + s) % len(KINDS)] for s in range(len(KINDS))]


def origin(stream, index, place):
    order = order_of(stream)
    for s in reversed(range(len(order))):
        if (index >> s) & 1:
            place = partner(order[s], place)
    z, y, x = place
    return (z * 4 + y) * 4 + x


def spread_streams(held):
    got = [None] * len(held)
    ticks = []
    for s in range(len(KINDS)):
        for k in range(len(held)):
            if s > 0:
                joined = jnp.concatenate([held[k], got[k]], axis=0)
                held[k] = lax.optimization_barrier(joined)
        for k in range(len(held)):
            axis, pairs = PAIRS[order_of(k)[s + 1]]
            got[k] = lax.ppermute(held[k], axis, pairs)
        ticks.append(list(got))
    return [(h, g) for h, g in zip(held, got)], ticks


def place_blocks(stream, halves, target, place, sem):
    count, rows = halves[0].shape[0], halves[0].shape[1]
    for index in range(2 * count):
        at = pl.multiple_of(origin(stream, index, place) * rows, rows)
        source = halves[index // count].at[index % count]
        pltpu.make_async_copy(source, target.at[pl.ds(at, rows)], sem).start()


def wait_for(target, sem):
    pltpu.make_async_copy(target, target, sem).wait()


def put_halves(xn, mine, other, gain, tp):
    cols = mine.shape[1]
    a, b = mine[...].astype(F32), other[...].astype(F32)
    squares = jnp.sum(a * a, axis=-1, keepdims=True) + jnp.sum(b * b, axis=-1, keepdims=True)
    scale = lax.rsqrt(squares * (1.0 / (2 * cols)) + EPS)
    low, high = gain[:, :cols], gain[:, cols:]
    first = tp == 0
    a = (a * scale * jnp.where(first, low, high)).astype(BF16)
    b = (b * scale * jnp.where(first, high, low)).astype(BF16)

    @pl.when(first)
    def _():
        xn[:, :cols] = a
        xn[:, cols:] = b

    @pl.when(jnp.logical_not(first))
    def _():
        xn[:, :cols] = b
        xn[:, cols:] = a


def front_kernel(
    place, xn, s0a, s0b, s1a, s1b, in_scale, gate_scale, taps, maps_r, maps_i,
    rate, extra, gated, win, wgate, xpad, a_s, b_s, gel, block_maps, sems,
):
    length = xn.shape[0]
    chans = win.shape[1]
    at = (place[0], place[1], place[2])
    place_blocks(0, (s0a, s0b), win, at, sems.at[0])
    place_blocks(1, (s1a, s1b), wgate, at, sems.at[1])
    low = place[0] == 0

    def half(ref):
        return jnp.where(low, ref[:, :chans], ref[:, chans:])

    bd = maps_r.shape[1]
    per = CB // bd
    block_maps[...] = jnp.zeros(block_maps.shape, BF16)
    for n in range(chans // bd):
        k, i = n // per, n % per
        which = place[0] * (chans // bd) + n
        rows, cols = slice(i * bd, (i + 1) * bd), slice(i * bd, (i + 1) * bd)
        block_maps[k, rows, cols] = maps_r[which].astype(BF16)
        block_maps[k, rows, slice(CB + i * bd, CB + (i + 1) * bd)] = maps_i[which].astype(BF16)

    in_s, gate_s, tap, slope = half(in_scale), half(gate_scale), half(taps), half(rate)
    xpad[0:8, :] = jnp.zeros((8, CB), F32)
    groups = chans // LANES
    wait_for(win, sems.at[0])
    wait_for(wgate, sems.at[1])
    for k in range(chans // CB):
        cols = slice(k * CB, (k + 1) * CB)
        pre = dot(xn[...], win[:, cols]) * in_s[:, cols]
        xpad[8 : 8 + length, :] = pre.astype(BF16).astype(F32)
        conv = tap[3:4, cols] * xpad[8 : 8 + length, :]
        for j in range(3):
            conv = conv + tap[j : j + 1, cols] * xpad[5 + j : 5 + j + length, :]
        maps = dot(conv.astype(BF16), block_maps[k])
        recur = sigmoid(maps[:, :CB])
        ingate = sigmoid(maps[:, CB:])
        factor = jnp.exp(slope[:, cols] * recur - extra[...])
        rest = 1.0 - factor * factor
        drive = rest * lax.rsqrt(rest) * (ingate * conv)
        for g in range(CB // LANES):
            row = k * (CB // LANES) + g
            part = slice(g * LANES, (g + 1) * LANES)
            a_s[pl.ds(row, length, stride=groups), :] = factor[:, part]
            b_s[pl.ds(row, length, stride=groups), :] = drive[:, part]
    for k in range(chans // CB):
        cols = slice(k * CB, (k + 1) * CB)
        pre_gate = (dot(xn[...], wgate[:, cols]) * gate_s[:, cols]).astype(BF16)
        gel[:, cols] = jax.nn.gelu(pre_gate.astype(F32), approximate=True)
    h = jnp.zeros((groups, LANES), F32)
    for t in range(length):
        rows = slice(t * groups, (t + 1) * groups)
        h = a_s[rows, :] * h + b_s[rows, :]
        b_s[rows, :] = h
    for g in range(groups):
        cols = slice(g * LANES, (g + 1) * LANES)
        gated[:, cols] = (b_s[pl.ds(g, length, stride=groups), :] * gel[:, cols]).astype(BF16)


def back_kernel(place, mine, other, s2a, s2b, s3a, s3b, partial, w0, w1, sems):
    at = (place[0], place[1], place[2])
    place_blocks(2, (s2a, s2b), w0, at, sems.at[0])
    place_blocks(3, (s3a, s3b), w1, at, sems.at[1])
    low = place[0] == 0
    g0 = jnp.where(low, mine[...], other[...])
    g1 = jnp.where(low, other[...], mine[...])
    wait_for(w0, sems.at[0])
    wait_for(w1, sems.at[1])
    cols = partial.shape[2]
    for c in range(2):
        rows = slice(c * cols, (c + 1) * cols)
        partial[c] = (dot_t(g0, w0[rows, :]) + dot_t(g1, w1[rows, :])).astype(BF16)


def norm_kernel(place, mine, other, gain, xn):
    put_halves(xn, mine, other, gain, place[3])


def mixed_kernel(place, tok_mine, tok_other, part, got, out_scale, gain, mixed, xn, hold):
    tp = place[3]

    def mix(tok, which):
        total = part[which].astype(F32) + got[which].astype(F32)
        return (tok[...].astype(F32) + total * out_scale[which]).astype(BF16)

    mixed[...] = mix(tok_mine, tp)
    hold[...] = mix(tok_other, 1 - tp)
    put_halves(xn, mixed, hold, gain, tp)


def ffn_kernel(
    place, xn, weights, gate_scale, up_scale, own, send, wgate, wup, wdown, hid, sems
):
    length, width = xn.shape
    hidden = gate_scale.shape[1]
    kdown = wdown.shape[2]
    blocks = [(s, min(512, hidden - s)) for s in range(0, hidden, 512)]
    copies = []
    for k, (s, n) in enumerate(blocks):
        for r, dst in ((0, wgate), (1, wup)):
            copy = pltpu.make_async_copy(
                weights.at[pl.ds(r * width, width), pl.ds(s, n)],
                dst.at[:, pl.ds(s, n)],
                sems.at[r, k],
            )
            copy.start()
            copies.append(copy)
    down_copies = []
    for r in range(2):
        copy = pltpu.make_async_copy(
            weights.at[pl.ds(r * width, width), pl.ds(hidden, kdown)], wdown.at[r], sems.at[2, r]
        )
        copy.start()
        down_copies.append(copy)
    cols = width // 2
    tp = place[3]
    for k, (s, n) in enumerate(blocks):
        part = slice(s, s + n)
        copies[2 * k].wait()
        gate = dot(xn[...], wgate[:, part]) * gate_scale[:, part]
        copies[2 * k + 1].wait()
        up = dot(xn[...], wup[:, part]) * up_scale[:, part]
        hid[:, part] = (gate * sigmoid(gate) * up).astype(BF16)
    for copy in down_copies:
        copy.wait()
    skip = 2 * kdown - hidden
    for dst, which in ((send, 1 - tp), (own, tp)):
        rows = pl.ds(pl.multiple_of(which * cols, cols), cols)
        acc = dot_t(hid[:, :kdown], wdown[0, rows, :])
        acc = acc + dot_t(hid[:, kdown:], wdown[1, rows, skip:])
        dst[...] = acc.astype(BF16)


def local(
    tokens, mix_gain, lru_input, lru_gate, lru_input_scale, lru_gate_scale, conv_weight,
    recur_gate, input_gate, decay_rate, extra_decay, lru_output, lru_output_scale, ffn_gain,
    ffn_gate, ffn_up, ffn_gate_scale, ffn_up_scale, ffn_down, ffn_down_scale,
):
    length, cols = tokens.shape
    width = 2 * cols
    chans = lru_input.shape[1] // 2
    hidden = ffn_gate.shape[1]
    rep = lax.axis_index("rep")
    tp = lax.axis_index("tp")
    zed = lax.axis_index("fs_0")
    swap = [(0, 1), (1, 0)]
    place = jnp.stack(
        [lax.axis_index(axis) for axis in ("fs_0", "fs_1", "fs_2", "tp")]
    ).astype(jnp.int32)

    down_t = ffn_down.T
    kdown = -(-hidden // (2 * LANES)) * LANES
    skip = hidden - kdown
    first = jnp.concatenate([ffn_gate, down_t[:, :kdown]], axis=1)
    second = jnp.concatenate([ffn_up, down_t[:, skip:]], axis=1)
    mine = jnp.where(rep == 0, first, second).astype(BF16)

    lru = (lru_input, lru_gate)
    low = jnp.concatenate([w[:, :chans] for w in lru], axis=1).astype(BF16)
    high = jnp.concatenate([w[:, chans:] for w in lru], axis=1).astype(BF16)
    out = lru_output.T.astype(BF16)
    away = jnp.concatenate([jnp.where(zed == 0, high, low), out], axis=1)
    away = lax.ppermute(away, "fs_0", swap)
    home = jnp.where(zed == 0, low, high)
    out = jnp.concatenate([home, out], axis=1)
    streams, ticks = spread_streams(
        [
            jnp.stack([h[:, k * chans : (k + 1) * chans], a[:, k * chans : (k + 1) * chans]])
            for h, a, k in ((home, away, 0), (home, away, 1), (out, away, 2), (out, away, 3))
        ]
    )

    mine, _ = lax.optimization_barrier((mine, ticks[0][0]))
    weights = lax.all_gather(mine, REP_FS, axis=0, tiled=True)

    guest = lax.ppermute(tokens, "fs_0", swap)
    guest_extra = lax.ppermute(extra_decay, "fs_0", swap)
    guest_other = lax.ppermute(guest, "tp", swap)
    tokens_other = lax.ppermute(tokens, "tp", swap)
    rate = -RATE * jax.nn.softplus(-decay_rate)

    vmem = pl.BlockSpec(memory_space=pltpu.VMEM)
    hbm = pl.BlockSpec(memory_space=pl.ANY)
    smem = pl.BlockSpec(memory_space=pltpu.SMEM)
    dma = pltpu.SemaphoreType.DMA
    row = lambda v: v.reshape(1, -1)
    groups = chans // LANES
    half_rows = jax.ShapeDtypeStruct((length, cols), BF16)

    blk = 128
    grid = (length // blk,)
    whole = lambda *dims: pl.BlockSpec(dims, lambda i: (0,) * len(dims))
    rows_of = lambda n: pl.BlockSpec((blk, n), lambda i: (i, 0))

    def norm(mine, other):
        return pl.pallas_call(
            norm_kernel,
            grid=grid,
            out_shape=jax.ShapeDtypeStruct((length, width), BF16),
            in_specs=[smem, rows_of(cols), rows_of(cols), whole(1, width)],
            out_specs=rows_of(width),
            name="norm",
        )(place, mine, other, row(mix_gain))

    def mix(normed, extra):
        return pl.pallas_call(
            front_kernel,
            out_shape=jax.ShapeDtypeStruct((length, chans), BF16),
            in_specs=[smem, vmem] + [hbm] * 4 + [vmem] * 7,
            out_specs=vmem,
            scratch_shapes=[
                pltpu.VMEM((width, chans), BF16),
                pltpu.VMEM((width, chans), BF16),
                pltpu.VMEM((length + 8, CB), F32),
                pltpu.VMEM((length * groups, LANES), F32),
                pltpu.VMEM((length * groups, LANES), F32),
                pltpu.VMEM((length, chans), F32),
                pltpu.VMEM((chans // CB, CB, 2 * CB), BF16),
                dma((2,)),
            ],
            name="front",
        )(
            place, normed, *streams[0], *streams[1], row(lru_input_scale),
            row(lru_gate_scale), conv_weight, recur_gate, input_gate, row(rate),
            extra.reshape(-1, 1),
        )

    normed = norm(tokens, tokens_other)
    guest_gated = mix(norm(guest, guest_other), guest_extra)
    normed, guest_gated = lax.optimization_barrier((normed, guest_gated))
    gated_away = lax.ppermute(guest_gated, "fs_0", swap)
    gated = mix(normed, extra_decay)
    partial = pl.pallas_call(
        back_kernel,
        out_shape=jax.ShapeDtypeStruct((2, length, cols), BF16),
        in_specs=[smem, vmem, vmem] + [hbm] * 4,
        out_specs=vmem,
        scratch_shapes=[
            pltpu.VMEM((width, chans), BF16),
            pltpu.VMEM((width, chans), BF16),
            dma((2,)),
        ],
        name="back",
    )(place, gated, gated_away, *streams[2], *streams[3])
    got = lax.ppermute(partial, "tp", swap)
    mixed, normed = pl.pallas_call(
        mixed_kernel,
        grid=grid,
        out_shape=[half_rows, jax.ShapeDtypeStruct((length, width), BF16)],
        in_specs=[smem, rows_of(cols), rows_of(cols)]
        + [pl.BlockSpec((2, blk, cols), lambda i: (0, i, 0))] * 2
        + [whole(2, 1, cols), whole(1, width)],
        out_specs=[rows_of(cols), rows_of(width)],
        scratch_shapes=[pltpu.VMEM((blk, cols), BF16)],
        name="mixed",
    )(
        place, tokens, tokens_other, partial, got, lru_output_scale.reshape(2, 1, cols),
        row(ffn_gain),
    )
    own, send = pl.pallas_call(
        ffn_kernel,
        out_shape=[half_rows] * 2,
        in_specs=[smem, vmem, hbm, vmem, vmem],
        out_specs=[vmem] * 2,
        scratch_shapes=[
            pltpu.VMEM((width, hidden), BF16),
            pltpu.VMEM((width, hidden), BF16),
            pltpu.VMEM((2, width, kdown), BF16),
            pltpu.VMEM((length, hidden), BF16),
            dma((3, 3)),
        ],
        name="ffn",
    )(place, normed, weights, row(ffn_gate_scale), row(ffn_up_scale))
    got = lax.ppermute(send, "tp", swap)
    scale = lax.dynamic_slice_in_dim(ffn_down_scale, tp * cols, cols)
    total = own.astype(F32) + got.astype(F32)
    return (mixed.astype(F32) + total * scale).astype(BF16)


def solution(mesh):
    split = Mesh(
        mesh.devices.reshape(mesh.shape["rep"], 2, 4, 4, mesh.shape["tp"]),
        ("rep", "fs_0", "fs_1", "fs_2", "tp"),
    )
    in_specs = (
        P(REP_FS, "tp"),
        P(),
        P(FS, "tp"),
        P(FS, "tp"),
        P("tp"),
        P("tp"),
        P(None, "tp"),
        P("tp", None, None),
        P("tp", None, None),
        P("tp"),
        P(REP_FS),
        P("tp", FS),
        P(),
        P(),
        P(FS, "tp"),
        P(FS, "tp"),
        P("tp"),
        P("tp"),
        P("tp", FS),
        P(),
    )
    out_specs = P(REP_FS, "tp")
    return jax.shard_map(local, mesh=split, in_specs=in_specs, out_specs=out_specs, check_vma=False)
```

```python
import jax
import jax.numpy as jnp
from jax import lax
from jax.experimental import pallas as pl
from jax.experimental.pallas import tpu as pltpu
from jax.sharding import Mesh
from jax.sharding import PartitionSpec as P

FS = ("fs_0", "fs_1", "fs_2")
REP_FS = ("rep", "fs_0", "fs_1", "fs_2")

EPS = 1e-06
RATE = 8.0
F32 = jnp.float32
BF16 = jnp.bfloat16
CB = 256
LANES = 128
FFN_BLOCKS = (0, 256, 512, 1024)


def sigmoid(v):
    return 0.5 + 0.5 * jnp.tanh(0.5 * v)


def dot(a, b):
    return jnp.dot(a, b, preferred_element_type=F32)


def dot_t(a, b):
    return lax.dot_general(a, b, (((1,), (1,)), ((), ())), preferred_element_type=F32)


def partner(kind, place):
    z, y, x = place
    if kind == "z":
        return z ^ 1, y, x
    if kind == "ye":
        return z, y ^ 1, x
    if kind == "yo":
        return z, (((y + 1) ^ 1) + 3) % 4, x
    if kind == "xe":
        return z, y, x ^ 1
    return z, y, (((x + 1) ^ 1) + 3) % 4


ODD = [(0, 3), (3, 0), (1, 2), (2, 1)]
EVEN = [(0, 1), (1, 0), (2, 3), (3, 2)]
PAIRS = {
    "z": ("fs_0", [(0, 1), (1, 0)]),
    "ye": ("fs_1", EVEN),
    "yo": ("fs_1", ODD),
    "xe": ("fs_2", EVEN),
    "xo": ("fs_2", ODD),
}
KINDS = ("xe", "ye", "xo", "yo")
OUT_TURNS = (0, 2)


def order_of(stream):
    return ["z"] + [KINDS[(stream + s) % len(KINDS)] for s in range(len(KINDS))]


def origin(stream, index, place):
    order = order_of(stream)
    for s in reversed(range(len(order))):
        if (index >> s) & 1:
            place = partner(order[s], place)
    z, y, x = place
    return (z * 4 + y) * 4 + x


def spread_streams(held, turns):
    got = [None] * len(held)
    ticks = []
    for s in range(len(KINDS)):
        for k in range(len(held)):
            if s > 0:
                joined = jnp.concatenate([held[k], got[k]], axis=0)
                held[k] = lax.optimization_barrier(joined)
        for k in range(len(held)):
            axis, pairs = PAIRS[order_of(turns[k])[s + 1]]
            got[k] = lax.ppermute(held[k], axis, pairs)
        ticks.append(list(got))
    return [(h, g) for h, g in zip(held, got)], ticks


def place_blocks(turn, halves, target, place, sem):
    count, rows = halves[0].shape[0], halves[0].shape[1]
    for index in range(2 * count):
        at = pl.multiple_of(origin(turn, index, place) * rows, rows)
        source = halves[index // count].at[index % count]
        pltpu.make_async_copy(source, target.at[pl.ds(at, rows)], sem).start()


def wait_for(target, sem):
    pltpu.make_async_copy(target, target, sem).wait()


def put_halves(xn, halves, gain, tp):
    length, width = xn.shape
    cols = width // 2
    low, high = gain[:, :cols], gain[:, cols:]
    first = tp == 0
    gain_a, gain_b = jnp.where(first, low, high), jnp.where(first, high, low)
    step = 16
    for r in range(0, length, step):
        rows = slice(r, r + step)
        a, b = halves(rows)
        squares = jnp.sum(a * a + b * b, axis=-1, keepdims=True)
        scale = lax.rsqrt(squares * (1.0 / width) + EPS)
        a = a * scale * gain_a
        b = b * scale * gain_b
        xn[rows, :cols] = jnp.where(first, a, b).astype(BF16)
        xn[rows, cols:] = jnp.where(first, b, a).astype(BF16)


def front_kernel(
    place, normed, s0a, s0b, s1a, s1b, s2a, s2b, s3a, s3b, in_scale, gate_scale, taps, maps_r, maps_i,
    rate, extra, gated, xn, win, wgate, xpad, a_s, b_s, gel, block_maps, sems,
):
    length = xn.shape[0]
    chans = gated.shape[1]
    at = (place[0], place[1], place[2])
    loaded = pltpu.make_async_copy(normed, xn, sems.at[2])
    loaded.start()
    place_blocks(0, (s0a, s0b), win.at[0], at, sems.at[0])
    place_blocks(1, (s1a, s1b), win.at[1], at, sems.at[1])
    place_blocks(2, (s2a, s2b), wgate.at[0], at, sems.at[3])
    place_blocks(3, (s3a, s3b), wgate.at[1], at, sems.at[4])
    low = place[0] == 0

    def half(ref):
        return jnp.where(low, ref[:, :chans], ref[:, chans:])

    bd = maps_r.shape[1]
    per = CB // bd
    block_maps[...] = jnp.zeros(block_maps.shape, BF16)
    for n in range(chans // bd):
        k, i = n // per, n % per
        which = place[0] * (chans // bd) + n
        rows, cols = slice(i * bd, (i + 1) * bd), slice(i * bd, (i + 1) * bd)
        block_maps[k, rows, cols] = maps_r[which].astype(BF16)
        block_maps[k, rows, slice(CB + i * bd, CB + (i + 1) * bd)] = maps_i[which].astype(BF16)

    in_s, gate_s, tap, slope = half(in_scale), half(gate_scale), half(taps), half(rate)
    xpad[0:8, :] = jnp.zeros((8, CB), F32)
    groups = chans // LANES
    loaded.wait()
    wait_for(win.at[0], sems.at[0])
    wait_for(win.at[1], sems.at[1])
    wait_for(wgate.at[0], sems.at[3])
    wait_for(wgate.at[1], sems.at[4])
    for k in range(chans // CB):
        cols = slice(k * CB, (k + 1) * CB)
        pre = dot(xn[...], win[k]) * in_s[:, cols]
        xpad[8 : 8 + length, :] = pre.astype(BF16).astype(F32)
        conv = tap[3:4, cols] * xpad[8 : 8 + length, :]
        for j in range(3):
            conv = conv + tap[j : j + 1, cols] * xpad[5 + j : 5 + j + length, :]
        maps = dot(conv.astype(BF16), block_maps[k])
        recur = sigmoid(maps[:, :CB])
        ingate = sigmoid(maps[:, CB:])
        factor = jnp.exp(slope[:, cols] * recur - extra[...])
        rest = 1.0 - factor * factor
        drive = rest * lax.rsqrt(rest) * (ingate * conv)
        for g in range(CB // LANES):
            row = k * (CB // LANES) + g
            part = slice(g * LANES, (g + 1) * LANES)
            a_s[pl.ds(row, length, stride=groups), :] = factor[:, part]
            b_s[pl.ds(row, length, stride=groups), :] = drive[:, part]
    for k in range(chans // CB):
        cols = slice(k * CB, (k + 1) * CB)
        pre_gate = (dot(xn[...], wgate[k]) * gate_s[:, cols]).astype(BF16)
        gel[:, cols] = jax.nn.gelu(pre_gate.astype(F32), approximate=True)
    h = jnp.zeros((groups, LANES), F32)
    for t in range(length):
        rows = slice(t * groups, (t + 1) * groups)
        h = a_s[rows, :] * h + b_s[rows, :]
        b_s[rows, :] = h
    for g in range(groups):
        cols = slice(g * LANES, (g + 1) * LANES)
        gated[:, cols] = (b_s[pl.ds(g, length, stride=groups), :] * gel[:, cols]).astype(BF16)


def back_kernel(place, mine, other, s2a, s2b, s3a, s3b, partial, g, w0, w1, acc, outs, sems):
    at = (place[0], place[1], place[2])
    low = place[0]
    loads = [
        pltpu.make_async_copy(mine, g.at[low], sems.at[2]),
        pltpu.make_async_copy(other, g.at[1 - low], sems.at[3]),
    ]
    place_blocks(OUT_TURNS[0], (s2a, s2b), w0, at, sems.at[0])
    for copy in loads:
        copy.start()
    place_blocks(OUT_TURNS[1], (s3a, s3b), w1, at, sems.at[1])
    for copy in loads:
        copy.wait()
    wait_for(w0, sems.at[0])
    width = w0.shape[0]
    cols = partial.shape[2]
    piece = cols // 2
    for c in range(width // piece):
        rows = slice(c * piece, (c + 1) * piece)
        acc[:, rows] = dot_t(g[0], w0[rows, :])
    wait_for(w1, sems.at[1])
    sent = []
    for c in range(width // piece):
        rows = slice(c * piece, (c + 1) * piece)
        outs[c] = (acc[:, rows] + dot_t(g[1], w1[rows, :])).astype(BF16)
        copy = pltpu.make_async_copy(
            outs.at[c],
            partial.at[c // 2, :, pl.ds((c % 2) * piece, piece)],
            sems.at[4 + c],
        )
        copy.start()
        sent.append(copy)
    for copy in sent:
        copy.wait()


def norm_kernel(place, mine, other, gain, xn):
    put_halves(
        xn, lambda rows: (mine[rows, :].astype(F32), other[rows, :].astype(F32)), gain, place[3]
    )


def mixed_kernel(place, tok_mine, tok_other, part, got, out_scale, gain, mixed, xn):
    tp = place[3]

    def mix(tok, which, rows):
        total = part[which, rows, :].astype(F32) + got[which, rows, :].astype(F32)
        return (tok[rows, :].astype(F32) + total * out_scale[which]).astype(BF16)

    def halves(rows):
        a = mix(tok_mine, tp, rows)
        mixed[rows, :] = a
        return a.astype(F32), mix(tok_other, 1 - tp, rows).astype(F32)

    put_halves(xn, halves, gain, tp)


def ffn_kernel(
    place, normed, weights, gate_scale, up_scale, own, send, xn, wgate, wup, wdown, hid, outs, sems
):
    length, width = xn.shape
    hidden = gate_scale.shape[1]
    kdown = wdown.shape[2]
    starts = list(FFN_BLOCKS) + [hidden]
    blocks = [(s, e - s) for s, e in zip(starts[:-1], starts[1:])]
    copies = []

    def begin(source, target, sem):
        copy = pltpu.make_async_copy(source, target, sem)
        copy.start()
        return copy

    loaded = begin(normed, xn, sems.at[3, 0])
    for k, (s, n) in enumerate(blocks):
        for r, dst in ((0, wgate), (1, wup)):
            copies.append(
                begin(
                    weights.at[pl.ds(r * width, width), pl.ds(s, n)],
                    dst.at[:, pl.ds(s, n)],
                    sems.at[r, k],
                )
            )
    down_copies = [
        begin(
            weights.at[pl.ds(r * width, width), pl.ds(hidden, kdown)], wdown.at[r], sems.at[2, r]
        )
        for r in range(2)
    ]
    cols = width // 2
    tp = place[3]
    loaded.wait()
    for k, (s, n) in enumerate(blocks):
        part = slice(s, s + n)
        copies[2 * k].wait()
        copies[2 * k + 1].wait()
        gate = dot(xn[...], wgate[:, part]) * gate_scale[:, part]
        up = dot(xn[...], wup[:, part]) * up_scale[:, part]
        hid[:, part] = (gate * sigmoid(gate) * up).astype(BF16)
    for copy in down_copies:
        copy.wait()
    skip = 2 * kdown - hidden
    sent = []
    piece = cols // 2
    for i, (dst, which) in enumerate(((send, 1 - tp), (own, tp))):
        for j in range(2):
            rows = pl.ds(pl.multiple_of(which * cols + j * piece, piece), piece)
            acc = dot_t(hid[:, :kdown], wdown[0, rows, :])
            acc = acc + dot_t(hid[:, kdown:], wdown[1, rows, skip:])
            span = slice(j * piece, (j + 1) * piece)
            outs[i, :, span] = acc.astype(BF16)
            sent.append(begin(outs.at[i, :, span], dst.at[:, span], sems.at[4, 2 * i + j]))
    for copy in sent:
        copy.wait()


def local(
    tokens, mix_gain, lru_input, lru_gate, lru_input_scale, lru_gate_scale, conv_weight,
    recur_gate, input_gate, decay_rate, extra_decay, lru_output, lru_output_scale, ffn_gain,
    ffn_gate, ffn_up, ffn_gate_scale, ffn_up_scale, ffn_down, ffn_down_scale,
):
    length, cols = tokens.shape
    width = 2 * cols
    chans = lru_input.shape[1] // 2
    hidden = ffn_gate.shape[1]
    rep = lax.axis_index("rep")
    tp = lax.axis_index("tp")
    zed = lax.axis_index("fs_0")
    swap = [(0, 1), (1, 0)]
    place = jnp.stack(
        [lax.axis_index(axis) for axis in ("fs_0", "fs_1", "fs_2", "tp")]
    ).astype(jnp.int32)

    down_t = ffn_down.T
    kdown = -(-hidden // (2 * LANES)) * LANES
    skip = hidden - kdown
    first = jnp.concatenate([ffn_gate, down_t[:, :kdown]], axis=1)
    second = jnp.concatenate([ffn_up, down_t[:, skip:]], axis=1)
    mine = jnp.where(rep == 0, first, second).astype(BF16)

    lru = (lru_input, lru_gate)
    low = jnp.concatenate([w[:, :chans] for w in lru], axis=1).astype(BF16)
    high = jnp.concatenate([w[:, chans:] for w in lru], axis=1).astype(BF16)
    home = jnp.where(zed == 0, low, high)
    away = lax.ppermute(jnp.where(zed == 0, high, low), "fs_0", swap)
    out = lru_output.T.astype(BF16)
    away_out = lax.ppermute(out, "fs_0", swap)
    blocks = lambda h, a, k, n: jnp.stack([h[:, k * n : (k + 1) * n], a[:, k * n : (k + 1) * n]])
    streams, ticks = spread_streams([blocks(home, away, k, CB) for k in range(4)], range(4))
    late = [blocks(out, away_out, k, chans) for k in range(2)]
    late = list(lax.optimization_barrier((*late, ticks[1][0]))[:2])
    outs, _ = spread_streams(late, OUT_TURNS)

    weights = lax.all_gather(mine, REP_FS, axis=0, tiled=True)

    guest = lax.ppermute(tokens, "fs_0", swap)
    guest_extra = lax.ppermute(extra_decay, "fs_0", swap)
    guest_other = lax.ppermute(guest, "tp", swap)
    tokens_other = lax.ppermute(tokens, "tp", swap)
    rate = -RATE * jax.nn.softplus(-decay_rate)

    vmem = pl.BlockSpec(memory_space=pltpu.VMEM)
    hbm = pl.BlockSpec(memory_space=pl.ANY)
    smem = pl.BlockSpec(memory_space=pltpu.SMEM)
    dma = pltpu.SemaphoreType.DMA
    row = lambda v: v.reshape(1, -1)
    groups = chans // LANES
    half_rows = jax.ShapeDtypeStruct((length, cols), BF16)

    blk = 128
    grid = (length // blk,)
    whole = lambda *dims: pl.BlockSpec(dims, lambda i: (0,) * len(dims))
    rows_of = lambda n: pl.BlockSpec((blk, n), lambda i: (i, 0))

    def norm(mine, other):
        return pl.pallas_call(
            norm_kernel,
            grid=grid,
            out_shape=jax.ShapeDtypeStruct((length, width), BF16),
            in_specs=[smem, rows_of(cols), rows_of(cols), whole(1, width)],
            out_specs=rows_of(width),
            name="norm",
        )(place, mine, other, row(mix_gain))

    def mix(normed, extra):
        return pl.pallas_call(
            front_kernel,
            out_shape=jax.ShapeDtypeStruct((length, chans), BF16),
            in_specs=[smem, hbm] + [hbm] * 8 + [vmem] * 7,
            out_specs=vmem,
            scratch_shapes=[
                pltpu.VMEM((length, width), BF16),
                pltpu.VMEM((chans // CB, width, CB), BF16),
                pltpu.VMEM((chans // CB, width, CB), BF16),
                pltpu.VMEM((length + 8, CB), F32),
                pltpu.VMEM((length * groups, LANES), F32),
                pltpu.VMEM((length * groups, LANES), F32),
                pltpu.VMEM((length, chans), F32),
                pltpu.VMEM((chans // CB, CB, 2 * CB), BF16),
                dma((5,)),
            ],
            name="front",
        )(
            place, normed, *streams[0], *streams[1], *streams[2], *streams[3],
            row(lru_input_scale),
            row(lru_gate_scale), conv_weight, recur_gate, input_gate, row(rate),
            extra.reshape(-1, 1),
        )

    normed = norm(tokens, tokens_other)
    guest_gated = mix(norm(guest, guest_other), guest_extra)
    normed, guest_gated = lax.optimization_barrier((normed, guest_gated))
    gated_away = lax.ppermute(guest_gated, "fs_0", swap)
    gated = mix(normed, extra_decay)
    partial = pl.pallas_call(
        back_kernel,
        out_shape=jax.ShapeDtypeStruct((2, length, cols), BF16),
        in_specs=[smem] + [hbm] * 6,
        out_specs=hbm,
        scratch_shapes=[
            pltpu.VMEM((2, length, chans), BF16),
            pltpu.VMEM((width, chans), BF16),
            pltpu.VMEM((width, chans), BF16),
            pltpu.VMEM((length, width), F32),
            pltpu.VMEM((4, length, width // 4), BF16),
            dma((8,)),
        ],
        name="back",
    )(place, gated, gated_away, *outs[0], *outs[1])
    got = lax.ppermute(partial, "tp", swap)
    mixed, normed = pl.pallas_call(
        mixed_kernel,
        grid=grid,
        out_shape=[half_rows, jax.ShapeDtypeStruct((length, width), BF16)],
        in_specs=[smem, rows_of(cols), rows_of(cols)]
        + [pl.BlockSpec((2, blk, cols), lambda i: (0, i, 0))] * 2
        + [whole(2, 1, cols), whole(1, width)],
        out_specs=[rows_of(cols), rows_of(width)],
        name="mixed",
    )(
        place, tokens, tokens_other, partial, got, lru_output_scale.reshape(2, 1, cols),
        row(ffn_gain),
    )
    own, send = pl.pallas_call(
        ffn_kernel,
        out_shape=[half_rows] * 2,
        in_specs=[smem, hbm, hbm, vmem, vmem],
        out_specs=[hbm] * 2,
        scratch_shapes=[
            pltpu.VMEM((length, width), BF16),
            pltpu.VMEM((width, hidden), BF16),
            pltpu.VMEM((width, hidden), BF16),
            pltpu.VMEM((2, width, kdown), BF16),
            pltpu.VMEM((length, hidden), BF16),
            pltpu.VMEM((2, length, cols), BF16),
            dma((5, 4)),
        ],
        name="ffn",
    )(place, normed, weights, row(ffn_gate_scale), row(ffn_up_scale))
    got = lax.ppermute(send, "tp", swap)
    scale = lax.dynamic_slice_in_dim(ffn_down_scale, tp * cols, cols)
    total = own.astype(F32) + got.astype(F32)
    return (mixed.astype(F32) + total * scale).astype(BF16)


def solution(mesh):
    split = Mesh(
        mesh.devices.reshape(mesh.shape["rep"], 2, 4, 4, mesh.shape["tp"]),
        ("rep", "fs_0", "fs_1", "fs_2", "tp"),
    )
    in_specs = (
        P(REP_FS, "tp"),
        P(),
        P(FS, "tp"),
        P(FS, "tp"),
        P("tp"),
        P("tp"),
        P(None, "tp"),
        P("tp", None, None),
        P("tp", None, None),
        P("tp"),
        P(REP_FS),
        P("tp", FS),
        P(),
        P(),
        P(FS, "tp"),
        P(FS, "tp"),
        P("tp"),
        P("tp"),
        P("tp", FS),
        P(),
    )
    out_specs = P(REP_FS, "tp")
    return jax.shard_map(local, mesh=split, in_specs=in_specs, out_specs=out_specs, check_vma=False)
```

```python
import jax
import jax.numpy as jnp
from jax import lax
from jax.experimental import pallas as pl
from jax.experimental.pallas import tpu as pltpu
from jax.sharding import Mesh
from jax.sharding import PartitionSpec as P

FS = ("fs_0", "fs_1", "fs_2")
REP_FS = ("rep", "fs_0", "fs_1", "fs_2")

EPS = 1e-06
RATE = 8.0
F32 = jnp.float32
BF16 = jnp.bfloat16
CB = 256
LANES = 128
FFN_BLOCKS = (0, 256, 512, 1024)


def sigmoid(v):
    return 0.5 + 0.5 * jnp.tanh(0.5 * v)


def dot(a, b):
    return jnp.dot(a, b, preferred_element_type=F32)


def dot_t(a, b):
    return lax.dot_general(a, b, (((1,), (1,)), ((), ())), preferred_element_type=F32)


def partner(kind, place):
    z, y, x = place
    if kind == "z":
        return z ^ 1, y, x
    if kind == "ye":
        return z, y ^ 1, x
    if kind == "yo":
        return z, (((y + 1) ^ 1) + 3) % 4, x
    if kind == "xe":
        return z, y, x ^ 1
    return z, y, (((x + 1) ^ 1) + 3) % 4


ODD = [(0, 3), (3, 0), (1, 2), (2, 1)]
EVEN = [(0, 1), (1, 0), (2, 3), (3, 2)]
PAIRS = {
    "z": ("fs_0", [(0, 1), (1, 0)]),
    "ye": ("fs_1", EVEN),
    "yo": ("fs_1", ODD),
    "xe": ("fs_2", EVEN),
    "xo": ("fs_2", ODD),
}
KINDS = ("xe", "ye", "xo", "yo")
OUT_TURNS = (0, 2)


def order_of(stream):
    return ["z"] + [KINDS[(stream + s) % len(KINDS)] for s in range(len(KINDS))]


def origin(stream, index, place):
    order = order_of(stream)
    for s in reversed(range(len(order))):
        if (index >> s) & 1:
            place = partner(order[s], place)
    z, y, x = place
    return (z * 4 + y) * 4 + x


def spread_streams(held, turns, after=()):
    got = [None] * len(held)
    ticks = []
    for s in range(len(KINDS)):
        for k in range(len(held)):
            if s > 0:
                joined = jnp.concatenate([held[k], got[k]], axis=0)
                ready = after[s] if s < len(after) and after[s] is not None else ()
                held[k] = lax.optimization_barrier((joined, *ready))[0]
        for k in range(len(held)):
            axis, pairs = PAIRS[order_of(turns[k])[s + 1]]
            got[k] = lax.ppermute(held[k], axis, pairs)
        ticks.append(list(got))
    return [(h, g) for h, g in zip(held, got)], ticks


def place_blocks(turn, halves, target, place, sem):
    count, rows = halves[0].shape[0], halves[0].shape[1]
    for index in range(2 * count):
        at = pl.multiple_of(origin(turn, index, place) * rows, rows)
        source = halves[index // count].at[index % count]
        pltpu.make_async_copy(source, target.at[pl.ds(at, rows)], sem).start()


def wait_for(target, sem):
    pltpu.make_async_copy(target, target, sem).wait()


def put_halves(xn, halves, gain, tp):
    length, width = xn.shape
    cols = width // 2
    low, high = gain[:, :cols], gain[:, cols:]
    first = tp == 0
    gain_a, gain_b = jnp.where(first, low, high), jnp.where(first, high, low)
    step = 16
    for r in range(0, length, step):
        rows = slice(r, r + step)
        a, b = halves(rows)
        squares = jnp.sum(a * a + b * b, axis=-1, keepdims=True)
        scale = lax.rsqrt(squares * (1.0 / width) + EPS)
        a = a * scale * gain_a
        b = b * scale * gain_b
        xn[rows, :cols] = jnp.where(first, a, b).astype(BF16)
        xn[rows, cols:] = jnp.where(first, b, a).astype(BF16)


def front_kernel(
    place, normed, s0a, s0b, s1a, s1b, s2a, s2b, s3a, s3b, in_scale, gate_scale, taps, maps_r, maps_i,
    rate, extra, gated, xn, win, wgate, xpad, a_s, b_s, gel, block_maps, sems,
):
    length = xn.shape[0]
    chans = gated.shape[1]
    at = (place[0], place[1], place[2])
    loaded = pltpu.make_async_copy(normed, xn, sems.at[2])
    loaded.start()
    place_blocks(0, (s0a, s0b), win.at[0], at, sems.at[0])
    place_blocks(1, (s1a, s1b), win.at[1], at, sems.at[1])
    place_blocks(2, (s2a, s2b), wgate.at[0], at, sems.at[3])
    place_blocks(3, (s3a, s3b), wgate.at[1], at, sems.at[4])
    low = place[0] == 0

    def half(ref):
        return jnp.where(low, ref[:, :chans], ref[:, chans:])

    bd = maps_r.shape[1]
    per = CB // bd
    block_maps[...] = jnp.zeros(block_maps.shape, BF16)
    for n in range(chans // bd):
        k, i = n // per, n % per
        which = place[0] * (chans // bd) + n
        rows, cols = slice(i * bd, (i + 1) * bd), slice(i * bd, (i + 1) * bd)
        block_maps[k, rows, cols] = maps_r[which].astype(BF16)
        block_maps[k, rows, slice(CB + i * bd, CB + (i + 1) * bd)] = maps_i[which].astype(BF16)

    in_s, gate_s, tap, slope = half(in_scale), half(gate_scale), half(taps), half(rate)
    xpad[0:8, :] = jnp.zeros((8, CB), F32)
    groups = chans // LANES
    loaded.wait()
    wait_for(win.at[0], sems.at[0])
    wait_for(win.at[1], sems.at[1])
    wait_for(wgate.at[0], sems.at[3])
    wait_for(wgate.at[1], sems.at[4])
    for k in range(chans // CB):
        cols = slice(k * CB, (k + 1) * CB)
        pre = dot(xn[...], win[k]) * in_s[:, cols]
        xpad[8 : 8 + length, :] = pre.astype(BF16).astype(F32)
        conv = tap[3:4, cols] * xpad[8 : 8 + length, :]
        for j in range(3):
            conv = conv + tap[j : j + 1, cols] * xpad[5 + j : 5 + j + length, :]
        maps = dot(conv.astype(BF16), block_maps[k])
        recur = sigmoid(maps[:, :CB])
        ingate = sigmoid(maps[:, CB:])
        factor = jnp.exp(slope[:, cols] * recur - extra[...])
        rest = 1.0 - factor * factor
        drive = rest * lax.rsqrt(rest) * (ingate * conv)
        for g in range(CB // LANES):
            row = k * (CB // LANES) + g
            part = slice(g * LANES, (g + 1) * LANES)
            a_s[pl.ds(row, length, stride=groups), :] = factor[:, part]
            b_s[pl.ds(row, length, stride=groups), :] = drive[:, part]
    for k in range(chans // CB):
        cols = slice(k * CB, (k + 1) * CB)
        pre_gate = (dot(xn[...], wgate[k]) * gate_s[:, cols]).astype(BF16)
        gel[:, cols] = jax.nn.gelu(pre_gate.astype(F32), approximate=True)
    h = jnp.zeros((groups, LANES), F32)
    for t in range(length):
        rows = slice(t * groups, (t + 1) * groups)
        h = a_s[rows, :] * h + b_s[rows, :]
        b_s[rows, :] = h
    for g in range(groups):
        cols = slice(g * LANES, (g + 1) * LANES)
        gated[:, cols] = (b_s[pl.ds(g, length, stride=groups), :] * gel[:, cols]).astype(BF16)


def back_kernel(place, mine, other, s2a, s2b, s3a, s3b, partial, g, w0, w1, acc, outs, sems):
    at = (place[0], place[1], place[2])
    low = place[0]
    loads = [
        pltpu.make_async_copy(mine, g.at[low], sems.at[2]),
        pltpu.make_async_copy(other, g.at[1 - low], sems.at[3]),
    ]
    place_blocks(OUT_TURNS[0], (s2a, s2b), w0, at, sems.at[0])
    for copy in loads:
        copy.start()
    place_blocks(OUT_TURNS[1], (s3a, s3b), w1, at, sems.at[1])
    for copy in loads:
        copy.wait()
    wait_for(w0, sems.at[0])
    width = w0.shape[0]
    cols = partial.shape[2]
    piece = cols // 2
    for c in range(width // piece):
        rows = slice(c * piece, (c + 1) * piece)
        acc[:, rows] = dot_t(g[0], w0[rows, :])
    wait_for(w1, sems.at[1])
    sent = []
    for c in range(width // piece):
        rows = slice(c * piece, (c + 1) * piece)
        outs[c] = (acc[:, rows] + dot_t(g[1], w1[rows, :])).astype(BF16)
        copy = pltpu.make_async_copy(
            outs.at[c],
            partial.at[c // 2, :, pl.ds((c % 2) * piece, piece)],
            sems.at[4 + c],
        )
        copy.start()
        sent.append(copy)
    for copy in sent:
        copy.wait()


def norm_kernel(place, mine, other, gain, xn):
    put_halves(
        xn, lambda rows: (mine[rows, :].astype(F32), other[rows, :].astype(F32)), gain, place[3]
    )


def mixed_kernel(place, tok_mine, tok_other, part, got, out_scale, gain, mixed, xn):
    tp = place[3]

    def mix(tok, which, rows):
        total = part[which, rows, :].astype(F32) + got[which, rows, :].astype(F32)
        return (tok[rows, :].astype(F32) + total * out_scale[which]).astype(BF16)

    def halves(rows):
        a = mix(tok_mine, tp, rows)
        mixed[rows, :] = a
        return a.astype(F32), mix(tok_other, 1 - tp, rows).astype(F32)

    put_halves(xn, halves, gain, tp)


def ffn_kernel(
    place, normed, weights, gate_scale, up_scale, own, send, xn, wgate, wup, wdown, hid, outs, sems
):
    length, width = xn.shape
    hidden = gate_scale.shape[1]
    kdown = wdown.shape[2]
    starts = list(FFN_BLOCKS) + [hidden]
    blocks = [(s, e - s) for s, e in zip(starts[:-1], starts[1:])]
    copies = []

    def begin(source, target, sem):
        copy = pltpu.make_async_copy(source, target, sem)
        copy.start()
        return copy

    loaded = begin(normed, xn, sems.at[3, 0])
    for k, (s, n) in enumerate(blocks):
        for r, dst in ((0, wgate), (1, wup)):
            copies.append(
                begin(
                    weights.at[pl.ds(r * width, width), pl.ds(s, n)],
                    dst.at[:, pl.ds(s, n)],
                    sems.at[r, k],
                )
            )
    down_copies = [
        begin(
            weights.at[pl.ds(r * width, width), pl.ds(hidden, kdown)], wdown.at[r], sems.at[2, r]
        )
        for r in range(2)
    ]
    cols = width // 2
    tp = place[3]
    loaded.wait()
    for k, (s, n) in enumerate(blocks):
        part = slice(s, s + n)
        copies[2 * k].wait()
        copies[2 * k + 1].wait()
        gate = dot(xn[...], wgate[:, part]) * gate_scale[:, part]
        up = dot(xn[...], wup[:, part]) * up_scale[:, part]
        hid[:, part] = (gate * sigmoid(gate) * up).astype(BF16)
    for copy in down_copies:
        copy.wait()
    skip = 2 * kdown - hidden
    sent = []
    piece = cols // 2
    for i, (dst, which) in enumerate(((send, 1 - tp), (own, tp))):
        for j in range(2):
            rows = pl.ds(pl.multiple_of(which * cols + j * piece, piece), piece)
            acc = dot_t(hid[:, :kdown], wdown[0, rows, :])
            acc = acc + dot_t(hid[:, kdown:], wdown[1, rows, skip:])
            span = slice(j * piece, (j + 1) * piece)
            outs[i, :, span] = acc.astype(BF16)
            sent.append(begin(outs.at[i, :, span], dst.at[:, span], sems.at[4, 2 * i + j]))
    for copy in sent:
        copy.wait()


def local(
    tokens, mix_gain, lru_input, lru_gate, lru_input_scale, lru_gate_scale, conv_weight,
    recur_gate, input_gate, decay_rate, extra_decay, lru_output, lru_output_scale, ffn_gain,
    ffn_gate, ffn_up, ffn_gate_scale, ffn_up_scale, ffn_down, ffn_down_scale,
):
    length, cols = tokens.shape
    width = 2 * cols
    chans = lru_input.shape[1] // 2
    hidden = ffn_gate.shape[1]
    rep = lax.axis_index("rep")
    tp = lax.axis_index("tp")
    zed = lax.axis_index("fs_0")
    swap = [(0, 1), (1, 0)]
    place = jnp.stack(
        [lax.axis_index(axis) for axis in ("fs_0", "fs_1", "fs_2", "tp")]
    ).astype(jnp.int32)

    down_t = ffn_down.T
    kdown = -(-hidden // (2 * LANES)) * LANES
    skip = hidden - kdown
    first = jnp.concatenate([ffn_gate, down_t[:, :kdown]], axis=1)
    second = jnp.concatenate([ffn_up, down_t[:, skip:]], axis=1)
    mine = jnp.where(rep == 0, first, second).astype(BF16)

    lru = (lru_input, lru_gate)
    low = jnp.concatenate([w[:, :chans] for w in lru], axis=1).astype(BF16)
    high = jnp.concatenate([w[:, chans:] for w in lru], axis=1).astype(BF16)
    home = jnp.where(zed == 0, low, high)
    away = lax.ppermute(jnp.where(zed == 0, high, low), "fs_0", swap)
    out = lru_output.T.astype(BF16)
    away_out = lax.ppermute(out, "fs_0", swap)
    blocks = lambda h, a, k, n: jnp.stack([h[:, k * n : (k + 1) * n], a[:, k * n : (k + 1) * n]])
    streams, ticks = spread_streams([blocks(home, away, k, CB) for k in range(4)], range(4))
    late = [blocks(out, away_out, k, chans) for k in range(2)]
    late = list(lax.optimization_barrier((*late, ticks[1][0]))[:2])

    weights = lax.all_gather(mine, REP_FS, axis=0, tiled=True)

    behind, behind_extra, _ = lax.optimization_barrier((tokens, extra_decay, away))
    guest = lax.ppermute(behind, "fs_0", swap)
    guest_extra = lax.ppermute(behind_extra, "fs_0", swap)
    guest_other = lax.ppermute(guest, "tp", swap)
    tokens_other = lax.ppermute(tokens, "tp", swap)
    rate = -RATE * jax.nn.softplus(-decay_rate)

    vmem = pl.BlockSpec(memory_space=pltpu.VMEM)
    hbm = pl.BlockSpec(memory_space=pl.ANY)
    smem = pl.BlockSpec(memory_space=pltpu.SMEM)
    dma = pltpu.SemaphoreType.DMA
    row = lambda v: v.reshape(1, -1)
    groups = chans // LANES
    half_rows = jax.ShapeDtypeStruct((length, cols), BF16)

    blk = 128
    grid = (length // blk,)
    whole = lambda *dims: pl.BlockSpec(dims, lambda i: (0,) * len(dims))
    rows_of = lambda n: pl.BlockSpec((blk, n), lambda i: (i, 0))

    def norm(mine, other):
        return pl.pallas_call(
            norm_kernel,
            grid=grid,
            out_shape=jax.ShapeDtypeStruct((length, width), BF16),
            in_specs=[smem, rows_of(cols), rows_of(cols), whole(1, width)],
            out_specs=rows_of(width),
            name="norm",
        )(place, mine, other, row(mix_gain))

    def mix(normed, extra):
        return pl.pallas_call(
            front_kernel,
            out_shape=jax.ShapeDtypeStruct((length, chans), BF16),
            in_specs=[smem, hbm] + [hbm] * 8 + [vmem] * 7,
            out_specs=vmem,
            scratch_shapes=[
                pltpu.VMEM((length, width), BF16),
                pltpu.VMEM((chans // CB, width, CB), BF16),
                pltpu.VMEM((chans // CB, width, CB), BF16),
                pltpu.VMEM((length + 8, CB), F32),
                pltpu.VMEM((length * groups, LANES), F32),
                pltpu.VMEM((length * groups, LANES), F32),
                pltpu.VMEM((length, chans), F32),
                pltpu.VMEM((chans // CB, CB, 2 * CB), BF16),
                dma((5,)),
            ],
            name="front",
        )(
            place, normed, *streams[0], *streams[1], *streams[2], *streams[3],
            row(lru_input_scale),
            row(lru_gate_scale), conv_weight, recur_gate, input_gate, row(rate),
            extra.reshape(-1, 1),
        )

    normed = norm(tokens, tokens_other)
    guest_normed = norm(guest, guest_other)
    outs, _ = spread_streams(late, OUT_TURNS, (None, None, (normed,), (guest_normed,)))
    guest_gated = mix(guest_normed, guest_extra)
    normed, guest_gated = lax.optimization_barrier((normed, guest_gated))
    gated_away = lax.ppermute(guest_gated, "fs_0", swap)
    gated = mix(normed, extra_decay)
    partial = pl.pallas_call(
        back_kernel,
        out_shape=jax.ShapeDtypeStruct((2, length, cols), BF16),
        in_specs=[smem] + [hbm] * 6,
        out_specs=hbm,
        scratch_shapes=[
            pltpu.VMEM((2, length, chans), BF16),
            pltpu.VMEM((width, chans), BF16),
            pltpu.VMEM((width, chans), BF16),
            pltpu.VMEM((length, width), F32),
            pltpu.VMEM((4, length, width // 4), BF16),
            dma((8,)),
        ],
        name="back",
    )(place, gated, gated_away, *outs[0], *outs[1])
    got = lax.ppermute(partial, "tp", swap)
    mixed, normed = pl.pallas_call(
        mixed_kernel,
        grid=grid,
        out_shape=[half_rows, jax.ShapeDtypeStruct((length, width), BF16)],
        in_specs=[smem, rows_of(cols), rows_of(cols)]
        + [pl.BlockSpec((2, blk, cols), lambda i: (0, i, 0))] * 2
        + [whole(2, 1, cols), whole(1, width)],
        out_specs=[rows_of(cols), rows_of(width)],
        name="mixed",
    )(
        place, tokens, tokens_other, partial, got, lru_output_scale.reshape(2, 1, cols),
        row(ffn_gain),
    )
    own, send = pl.pallas_call(
        ffn_kernel,
        out_shape=[half_rows] * 2,
        in_specs=[smem, hbm, hbm, vmem, vmem],
        out_specs=[hbm] * 2,
        scratch_shapes=[
            pltpu.VMEM((length, width), BF16),
            pltpu.VMEM((width, hidden), BF16),
            pltpu.VMEM((width, hidden), BF16),
            pltpu.VMEM((2, width, kdown), BF16),
            pltpu.VMEM((length, hidden), BF16),
            pltpu.VMEM((2, length, cols), BF16),
            dma((5, 4)),
        ],
        name="ffn",
    )(place, normed, weights, row(ffn_gate_scale), row(ffn_up_scale))
    got = lax.ppermute(send, "tp", swap)
    scale = lax.dynamic_slice_in_dim(ffn_down_scale, tp * cols, cols)
    total = own.astype(F32) + got.astype(F32)
    return (mixed.astype(F32) + total * scale).astype(BF16)


def solution(mesh):
    split = Mesh(
        mesh.devices.reshape(mesh.shape["rep"], 2, 4, 4, mesh.shape["tp"]),
        ("rep", "fs_0", "fs_1", "fs_2", "tp"),
    )
    in_specs = (
        P(REP_FS, "tp"),
        P(),
        P(FS, "tp"),
        P(FS, "tp"),
        P("tp"),
        P("tp"),
        P(None, "tp"),
        P("tp", None, None),
        P("tp", None, None),
        P("tp"),
        P(REP_FS),
        P("tp", FS),
        P(),
        P(),
        P(FS, "tp"),
        P(FS, "tp"),
        P("tp"),
        P("tp"),
        P("tp", FS),
        P(),
    )
    out_specs = P(REP_FS, "tp")
    return jax.shard_map(local, mesh=split, in_specs=in_specs, out_specs=out_specs, check_vma=False)
```

```python
import jax
import jax.numpy as jnp
from jax import lax
from jax.experimental import pallas as pl
from jax.experimental.pallas import tpu as pltpu
from jax.sharding import Mesh
from jax.sharding import PartitionSpec as P

FS = ("fs_0", "fs_1", "fs_2")
REP_FS = ("rep", "fs_0", "fs_1", "fs_2")

EPS = 1e-06
RATE = 8.0
F32 = jnp.float32
BF16 = jnp.bfloat16
CB = 256
LANES = 128
FFN_BLOCKS = (0, 256, 512, 1024)


def sigmoid(v):
    return 0.5 + 0.5 * jnp.tanh(0.5 * v)


def dot(a, b):
    return jnp.dot(a, b, preferred_element_type=F32)


def dot_t(a, b):
    return lax.dot_general(a, b, (((1,), (1,)), ((), ())), preferred_element_type=F32)


def partner(kind, place):
    z, y, x = place
    if kind == "z":
        return z ^ 1, y, x
    if kind == "ye":
        return z, y ^ 1, x
    if kind == "yo":
        return z, (((y + 1) ^ 1) + 3) % 4, x
    if kind == "xe":
        return z, y, x ^ 1
    return z, y, (((x + 1) ^ 1) + 3) % 4


ODD = [(0, 3), (3, 0), (1, 2), (2, 1)]
EVEN = [(0, 1), (1, 0), (2, 3), (3, 2)]
PAIRS = {
    "z": ("fs_0", [(0, 1), (1, 0)]),
    "ye": ("fs_1", EVEN),
    "yo": ("fs_1", ODD),
    "xe": ("fs_2", EVEN),
    "xo": ("fs_2", ODD),
}
KINDS = ("xe", "ye", "xo", "yo")
OUT_ORDERS = (("xe", "ye", "xo", "yo"), ("yo", "xo", "ye", "xe"))


IN_ORDERS = tuple(KINDS[k:] + KINDS[:k] for k in range(len(KINDS)))


def origin(order, index, place):
    order = ("z",) + order
    for s in reversed(range(len(order))):
        if (index >> s) & 1:
            place = partner(order[s], place)
    z, y, x = place
    return (z * 4 + y) * 4 + x


def spread_streams(held, orders, after=()):
    got = [None] * len(held)
    ticks = []
    for s in range(len(KINDS)):
        for k in range(len(held)):
            if s > 0:
                joined = jnp.concatenate([held[k], got[k]], axis=0)
                ready = after[s] if s < len(after) and after[s] is not None else ()
                held[k] = lax.optimization_barrier((joined, *ready))[0]
        for k in range(len(held)):
            axis, pairs = PAIRS[orders[k][s]]
            got[k] = lax.ppermute(held[k], axis, pairs)
        ticks.append(list(got))
    return [(h, g) for h, g in zip(held, got)], ticks


def place_blocks(order, halves, target, place, sem):
    count, rows = halves[0].shape[0], halves[0].shape[1]
    for index in range(2 * count):
        at = pl.multiple_of(origin(order, index, place) * rows, rows)
        source = halves[index // count].at[index % count]
        pltpu.make_async_copy(source, target.at[pl.ds(at, rows)], sem).start()


def wait_for(target, sem):
    pltpu.make_async_copy(target, target, sem).wait()


def put_halves(xn, halves, gain, tp):
    length, width = xn.shape
    cols = width // 2
    low, high = gain[:, :cols], gain[:, cols:]
    first = tp == 0
    gain_a, gain_b = jnp.where(first, low, high), jnp.where(first, high, low)
    step = 16
    for r in range(0, length, step):
        rows = slice(r, r + step)
        a, b = halves(rows)
        squares = jnp.sum(a * a + b * b, axis=-1, keepdims=True)
        scale = lax.rsqrt(squares * (1.0 / width) + EPS)
        a = a * scale * gain_a
        b = b * scale * gain_b
        xn[rows, :cols] = jnp.where(first, a, b).astype(BF16)
        xn[rows, cols:] = jnp.where(first, b, a).astype(BF16)


def front_kernel(
    place, normed, s0a, s0b, s1a, s1b, s2a, s2b, s3a, s3b, in_scale, gate_scale, taps, maps_r, maps_i,
    rate, extra, gated, xn, win, wgate, xpad, a_s, b_s, gel, block_maps, sems,
):
    length = xn.shape[0]
    chans = gated.shape[1]
    at = (place[0], place[1], place[2])
    loaded = pltpu.make_async_copy(normed, xn, sems.at[2])
    loaded.start()
    place_blocks(IN_ORDERS[0], (s0a, s0b), win.at[0], at, sems.at[0])
    place_blocks(IN_ORDERS[1], (s1a, s1b), win.at[1], at, sems.at[1])
    place_blocks(IN_ORDERS[2], (s2a, s2b), wgate.at[0], at, sems.at[3])
    place_blocks(IN_ORDERS[3], (s3a, s3b), wgate.at[1], at, sems.at[4])
    low = place[0] == 0

    def half(ref):
        return jnp.where(low, ref[:, :chans], ref[:, chans:])

    bd = maps_r.shape[1]
    per = CB // bd
    block_maps[...] = jnp.zeros(block_maps.shape, BF16)
    for n in range(chans // bd):
        k, i = n // per, n % per
        which = place[0] * (chans // bd) + n
        rows, cols = slice(i * bd, (i + 1) * bd), slice(i * bd, (i + 1) * bd)
        block_maps[k, rows, cols] = maps_r[which].astype(BF16)
        block_maps[k, rows, slice(CB + i * bd, CB + (i + 1) * bd)] = maps_i[which].astype(BF16)

    in_s, gate_s, tap, slope = half(in_scale), half(gate_scale), half(taps), half(rate)
    xpad[0:8, :] = jnp.zeros((8, CB), F32)
    groups = chans // LANES
    loaded.wait()
    wait_for(win.at[0], sems.at[0])
    wait_for(win.at[1], sems.at[1])
    wait_for(wgate.at[0], sems.at[3])
    wait_for(wgate.at[1], sems.at[4])
    for k in range(chans // CB):
        cols = slice(k * CB, (k + 1) * CB)
        pre = dot(xn[...], win[k]) * in_s[:, cols]
        xpad[8 : 8 + length, :] = pre.astype(BF16).astype(F32)
        conv = tap[3:4, cols] * xpad[8 : 8 + length, :]
        for j in range(3):
            conv = conv + tap[j : j + 1, cols] * xpad[5 + j : 5 + j + length, :]
        maps = dot(conv.astype(BF16), block_maps[k])
        recur = sigmoid(maps[:, :CB])
        ingate = sigmoid(maps[:, CB:])
        factor = jnp.exp(slope[:, cols] * recur - extra[...])
        rest = 1.0 - factor * factor
        drive = rest * lax.rsqrt(rest) * (ingate * conv)
        for g in range(CB // LANES):
            row = k * (CB // LANES) + g
            part = slice(g * LANES, (g + 1) * LANES)
            a_s[pl.ds(row, length, stride=groups), :] = factor[:, part]
            b_s[pl.ds(row, length, stride=groups), :] = drive[:, part]
    for k in range(chans // CB):
        cols = slice(k * CB, (k + 1) * CB)
        pre_gate = (dot(xn[...], wgate[k]) * gate_s[:, cols]).astype(BF16)
        gel[:, cols] = jax.nn.gelu(pre_gate.astype(F32), approximate=True)
    h = jnp.zeros((groups, LANES), F32)
    for t in range(length):
        rows = slice(t * groups, (t + 1) * groups)
        h = a_s[rows, :] * h + b_s[rows, :]
        b_s[rows, :] = h
    for g in range(groups):
        cols = slice(g * LANES, (g + 1) * LANES)
        gated[:, cols] = (b_s[pl.ds(g, length, stride=groups), :] * gel[:, cols]).astype(BF16)


def back_kernel(place, mine, other, s2a, s2b, s3a, s3b, partial, g, w0, w1, acc, outs, sems):
    at = (place[0], place[1], place[2])
    low = place[0]
    loads = [
        pltpu.make_async_copy(mine, g.at[low], sems.at[2]),
        pltpu.make_async_copy(other, g.at[1 - low], sems.at[3]),
    ]
    place_blocks(OUT_ORDERS[0], (s2a, s2b), w0, at, sems.at[0])
    for copy in loads:
        copy.start()
    place_blocks(OUT_ORDERS[1], (s3a, s3b), w1, at, sems.at[1])
    for copy in loads:
        copy.wait()
    wait_for(w0, sems.at[0])
    width = w0.shape[0]
    cols = partial.shape[2]
    piece = cols // 2
    for c in range(width // piece):
        rows = slice(c * piece, (c + 1) * piece)
        acc[:, rows] = dot_t(g[0], w0[rows, :])
    wait_for(w1, sems.at[1])
    sent = []
    for c in range(width // piece):
        rows = slice(c * piece, (c + 1) * piece)
        outs[c] = (acc[:, rows] + dot_t(g[1], w1[rows, :])).astype(BF16)
        copy = pltpu.make_async_copy(
            outs.at[c],
            partial.at[c // 2, :, pl.ds((c % 2) * piece, piece)],
            sems.at[4 + c],
        )
        copy.start()
        sent.append(copy)
    for copy in sent:
        copy.wait()


def norm_kernel(place, mine, other, gain, xn):
    put_halves(
        xn, lambda rows: (mine[rows, :].astype(F32), other[rows, :].astype(F32)), gain, place[3]
    )


def mixed_kernel(place, tok_mine, tok_other, part, got, out_scale, gain, mixed, xn):
    tp = place[3]

    def mix(tok, which, rows):
        total = part[which, rows, :].astype(F32) + got[which, rows, :].astype(F32)
        return (tok[rows, :].astype(F32) + total * out_scale[which]).astype(BF16)

    def halves(rows):
        a = mix(tok_mine, tp, rows)
        mixed[rows, :] = a
        return a.astype(F32), mix(tok_other, 1 - tp, rows).astype(F32)

    put_halves(xn, halves, gain, tp)


def ffn_kernel(
    place, normed, weights, gate_scale, up_scale, own, send, xn, wgate, wup, wdown, hid, outs, sems
):
    length, width = xn.shape
    hidden = gate_scale.shape[1]
    kdown = wdown.shape[2]
    starts = list(FFN_BLOCKS) + [hidden]
    blocks = [(s, e - s) for s, e in zip(starts[:-1], starts[1:])]
    copies = []

    def begin(source, target, sem):
        copy = pltpu.make_async_copy(source, target, sem)
        copy.start()
        return copy

    loaded = begin(normed, xn, sems.at[3, 0])
    for k, (s, n) in enumerate(blocks):
        for r, dst in ((0, wgate), (1, wup)):
            copies.append(
                begin(
                    weights.at[pl.ds(r * width, width), pl.ds(s, n)],
                    dst.at[:, pl.ds(s, n)],
                    sems.at[r, k],
                )
            )
    down_copies = [
        begin(
            weights.at[pl.ds(r * width, width), pl.ds(hidden, kdown)], wdown.at[r], sems.at[2, r]
        )
        for r in range(2)
    ]
    cols = width // 2
    tp = place[3]
    loaded.wait()
    for k, (s, n) in enumerate(blocks):
        part = slice(s, s + n)
        copies[2 * k].wait()
        copies[2 * k + 1].wait()
        gate = dot(xn[...], wgate[:, part]) * gate_scale[:, part]
        up = dot(xn[...], wup[:, part]) * up_scale[:, part]
        hid[:, part] = (gate * sigmoid(gate) * up).astype(BF16)
    for copy in down_copies:
        copy.wait()
    skip = 2 * kdown - hidden
    sent = []
    piece = cols // 2
    for i, (dst, which) in enumerate(((send, 1 - tp), (own, tp))):
        for j in range(2):
            rows = pl.ds(pl.multiple_of(which * cols + j * piece, piece), piece)
            acc = dot_t(hid[:, :kdown], wdown[0, rows, :])
            acc = acc + dot_t(hid[:, kdown:], wdown[1, rows, skip:])
            span = slice(j * piece, (j + 1) * piece)
            outs[i, :, span] = acc.astype(BF16)
            sent.append(begin(outs.at[i, :, span], dst.at[:, span], sems.at[4, 2 * i + j]))
    for copy in sent:
        copy.wait()


def local(
    tokens, mix_gain, lru_input, lru_gate, lru_input_scale, lru_gate_scale, conv_weight,
    recur_gate, input_gate, decay_rate, extra_decay, lru_output, lru_output_scale, ffn_gain,
    ffn_gate, ffn_up, ffn_gate_scale, ffn_up_scale, ffn_down, ffn_down_scale,
):
    length, cols = tokens.shape
    width = 2 * cols
    chans = lru_input.shape[1] // 2
    hidden = ffn_gate.shape[1]
    rep = lax.axis_index("rep")
    tp = lax.axis_index("tp")
    zed = lax.axis_index("fs_0")
    swap = [(0, 1), (1, 0)]
    place = jnp.stack(
        [lax.axis_index(axis) for axis in ("fs_0", "fs_1", "fs_2", "tp")]
    ).astype(jnp.int32)

    down_t = ffn_down.T
    kdown = -(-hidden // (2 * LANES)) * LANES
    skip = hidden - kdown
    first = jnp.concatenate([ffn_gate, down_t[:, :kdown]], axis=1)
    second = jnp.concatenate([ffn_up, down_t[:, skip:]], axis=1)
    mine = jnp.where(rep == 0, first, second).astype(BF16)

    lru = (lru_input, lru_gate)
    low = jnp.concatenate([w[:, :chans] for w in lru], axis=1).astype(BF16)
    high = jnp.concatenate([w[:, chans:] for w in lru], axis=1).astype(BF16)
    home = jnp.where(zed == 0, low, high)
    away = lax.ppermute(jnp.where(zed == 0, high, low), "fs_0", swap)
    out = lru_output.T.astype(BF16)
    away_out = lax.ppermute(out, "fs_0", swap)
    blocks = lambda h, a, k, n: jnp.stack([h[:, k * n : (k + 1) * n], a[:, k * n : (k + 1) * n]])
    streams, ticks = spread_streams([blocks(home, away, k, CB) for k in range(4)], IN_ORDERS)
    late = [blocks(out, away_out, k, chans) for k in range(2)]
    late = list(lax.optimization_barrier((*late, ticks[1][0]))[:2])

    weights = lax.all_gather(mine, REP_FS, axis=0, tiled=True)

    behind, behind_extra, _ = lax.optimization_barrier((tokens, extra_decay, away))
    guest = lax.ppermute(behind, "fs_0", swap)
    guest_extra = lax.ppermute(behind_extra, "fs_0", swap)
    guest_other = lax.ppermute(guest, "tp", swap)
    tokens_other = lax.ppermute(tokens, "tp", swap)
    rate = -RATE * jax.nn.softplus(-decay_rate)

    vmem = pl.BlockSpec(memory_space=pltpu.VMEM)
    hbm = pl.BlockSpec(memory_space=pl.ANY)
    smem = pl.BlockSpec(memory_space=pltpu.SMEM)
    dma = pltpu.SemaphoreType.DMA
    row = lambda v: v.reshape(1, -1)
    groups = chans // LANES
    half_rows = jax.ShapeDtypeStruct((length, cols), BF16)

    blk = 256
    grid = (length // blk,)
    whole = lambda *dims: pl.BlockSpec(dims, lambda i: (0,) * len(dims))
    rows_of = lambda n: pl.BlockSpec((blk, n), lambda i: (i, 0))

    def norm(mine, other):
        return pl.pallas_call(
            norm_kernel,
            grid=grid,
            out_shape=jax.ShapeDtypeStruct((length, width), BF16),
            in_specs=[smem, rows_of(cols), rows_of(cols), whole(1, width)],
            out_specs=rows_of(width),
            name="norm",
        )(place, mine, other, row(mix_gain))

    def mix(normed, extra):
        return pl.pallas_call(
            front_kernel,
            out_shape=jax.ShapeDtypeStruct((length, chans), BF16),
            in_specs=[smem, hbm] + [hbm] * 8 + [vmem] * 7,
            out_specs=vmem,
            scratch_shapes=[
                pltpu.VMEM((length, width), BF16),
                pltpu.VMEM((chans // CB, width, CB), BF16),
                pltpu.VMEM((chans // CB, width, CB), BF16),
                pltpu.VMEM((length + 8, CB), F32),
                pltpu.VMEM((length * groups, LANES), F32),
                pltpu.VMEM((length * groups, LANES), F32),
                pltpu.VMEM((length, chans), F32),
                pltpu.VMEM((chans // CB, CB, 2 * CB), BF16),
                dma((5,)),
            ],
            name="front",
        )(
            place, normed, *streams[0], *streams[1], *streams[2], *streams[3],
            row(lru_input_scale),
            row(lru_gate_scale), conv_weight, recur_gate, input_gate, row(rate),
            extra.reshape(-1, 1),
        )

    normed = norm(tokens, tokens_other)
    guest_normed = norm(guest, guest_other)
    outs, _ = spread_streams(
        late, OUT_ORDERS, (None, None, None, (normed, guest_normed))
    )
    guest_gated = mix(guest_normed, guest_extra)
    normed, guest_gated = lax.optimization_barrier((normed, guest_gated))
    gated_away = lax.ppermute(guest_gated, "fs_0", swap)
    gated = mix(normed, extra_decay)
    partial = pl.pallas_call(
        back_kernel,
        out_shape=jax.ShapeDtypeStruct((2, length, cols), BF16),
        in_specs=[smem] + [hbm] * 6,
        out_specs=hbm,
        scratch_shapes=[
            pltpu.VMEM((2, length, chans), BF16),
            pltpu.VMEM((width, chans), BF16),
            pltpu.VMEM((width, chans), BF16),
            pltpu.VMEM((length, width), F32),
            pltpu.VMEM((4, length, width // 4), BF16),
            dma((8,)),
        ],
        name="back",
    )(place, gated, gated_away, *outs[0], *outs[1])
    got = lax.ppermute(partial, "tp", swap)
    mixed, normed = pl.pallas_call(
        mixed_kernel,
        grid=grid,
        out_shape=[half_rows, jax.ShapeDtypeStruct((length, width), BF16)],
        in_specs=[smem, rows_of(cols), rows_of(cols)]
        + [pl.BlockSpec((2, blk, cols), lambda i: (0, i, 0))] * 2
        + [whole(2, 1, cols), whole(1, width)],
        out_specs=[rows_of(cols), rows_of(width)],
        name="mixed",
    )(
        place, tokens, tokens_other, partial, got, lru_output_scale.reshape(2, 1, cols),
        row(ffn_gain),
    )
    own, send = pl.pallas_call(
        ffn_kernel,
        out_shape=[half_rows] * 2,
        in_specs=[smem, hbm, hbm, vmem, vmem],
        out_specs=[hbm] * 2,
        scratch_shapes=[
            pltpu.VMEM((length, width), BF16),
            pltpu.VMEM((width, hidden), BF16),
            pltpu.VMEM((width, hidden), BF16),
            pltpu.VMEM((2, width, kdown), BF16),
            pltpu.VMEM((length, hidden), BF16),
            pltpu.VMEM((2, length, cols), BF16),
            dma((5, 4)),
        ],
        name="ffn",
    )(place, normed, weights, row(ffn_gate_scale), row(ffn_up_scale))
    got = lax.ppermute(send, "tp", swap)
    scale = lax.dynamic_slice_in_dim(ffn_down_scale, tp * cols, cols)
    total = own.astype(F32) + got.astype(F32)
    return (mixed.astype(F32) + total * scale).astype(BF16)


def solution(mesh):
    split = Mesh(
        mesh.devices.reshape(mesh.shape["rep"], 2, 4, 4, mesh.shape["tp"]),
        ("rep", "fs_0", "fs_1", "fs_2", "tp"),
    )
    in_specs = (
        P(REP_FS, "tp"),
        P(),
        P(FS, "tp"),
        P(FS, "tp"),
        P("tp"),
        P("tp"),
        P(None, "tp"),
        P("tp", None, None),
        P("tp", None, None),
        P("tp"),
        P(REP_FS),
        P("tp", FS),
        P(),
        P(),
        P(FS, "tp"),
        P(FS, "tp"),
        P("tp"),
        P("tp"),
        P("tp", FS),
        P(),
    )
    out_specs = P(REP_FS, "tp")
    return jax.shard_map(local, mesh=split, in_specs=in_specs, out_specs=out_specs, check_vma=False)
```

```python
import jax
import jax.numpy as jnp
from jax import lax
from jax.experimental import pallas as pl
from jax.experimental.pallas import tpu as pltpu
from jax.sharding import Mesh
from jax.sharding import PartitionSpec as P

FS = ("fs_0", "fs_1", "fs_2")
REP_FS = ("rep", "fs_0", "fs_1", "fs_2")

EPS = 1e-06
RATE = 8.0
F32 = jnp.float32
BF16 = jnp.bfloat16
CB = 256
LANES = 128
FFN_BLOCKS = (0, 256, 512, 1024)


def sigmoid(v):
    return 0.5 + 0.5 * jnp.tanh(0.5 * v)


def dot(a, b):
    return jnp.dot(a, b, preferred_element_type=F32)


def dot_t(a, b):
    return lax.dot_general(a, b, (((1,), (1,)), ((), ())), preferred_element_type=F32)


def partner(kind, place):
    z, y, x = place
    if kind == "z":
        return z ^ 1, y, x
    if kind == "ye":
        return z, y ^ 1, x
    if kind == "yo":
        return z, (((y + 1) ^ 1) + 3) % 4, x
    if kind == "xe":
        return z, y, x ^ 1
    return z, y, (((x + 1) ^ 1) + 3) % 4


ODD = [(0, 3), (3, 0), (1, 2), (2, 1)]
EVEN = [(0, 1), (1, 0), (2, 3), (3, 2)]
PAIRS = {
    "z": ("fs_0", [(0, 1), (1, 0)]),
    "ye": ("fs_1", EVEN),
    "yo": ("fs_1", ODD),
    "xe": ("fs_2", EVEN),
    "xo": ("fs_2", ODD),
}
KINDS = ("xe", "ye", "z", "xo", "yo")
OUT_ORDERS = (("z", "ye", "yo", "xe", "xo"), ("yo", "xe", "xo", "ye", "z"))


IN_ORDERS = tuple(KINDS[k:] + KINDS[:k] for k in range(4))


def origin(order, index, place):
    for s in reversed(range(len(order))):
        if (index >> s) & 1:
            place = partner(order[s], place)
    z, y, x = place
    return (z * 4 + y) * 4 + x


def spread_streams(held, orders, after=()):
    got = [None] * len(held)
    ticks = []
    for s in range(len(KINDS)):
        for k in range(len(held)):
            if s > 0:
                joined = jnp.concatenate([held[k], got[k]], axis=0)
                ready = after[s] if s < len(after) and after[s] is not None else ()
                held[k] = lax.optimization_barrier((joined, *ready))[0]
        for k in range(len(held)):
            axis, pairs = PAIRS[orders[k][s]]
            got[k] = lax.ppermute(held[k], axis, pairs)
        ticks.append(list(got))
    return [(h, g) for h, g in zip(held, got)], ticks


def place_blocks(order, halves, target, place, sem):
    count, rows = halves[0].shape[0], halves[0].shape[1]
    for index in range(2 * count):
        at = pl.multiple_of(origin(order, index, place) * rows, rows)
        source = halves[index // count].at[index % count]
        pltpu.make_async_copy(source, target.at[pl.ds(at, rows)], sem).start()


def wait_for(target, sem):
    pltpu.make_async_copy(target, target, sem).wait()


def put_halves(xn, halves, gain, tp):
    length, width = xn.shape
    cols = width // 2
    low, high = gain[:, :cols], gain[:, cols:]
    first = tp == 0
    gain_a, gain_b = jnp.where(first, low, high), jnp.where(first, high, low)
    step = 16
    for r in range(0, length, step):
        rows = slice(r, r + step)
        a, b = halves(rows)
        squares = jnp.sum(a * a + b * b, axis=-1, keepdims=True)
        scale = lax.rsqrt(squares * (1.0 / width) + EPS)
        a = a * scale * gain_a
        b = b * scale * gain_b
        xn[rows, :cols] = jnp.where(first, a, b).astype(BF16)
        xn[rows, cols:] = jnp.where(first, b, a).astype(BF16)


def front_kernel(
    place, normed, s0a, s0b, s1a, s1b, s2a, s2b, s3a, s3b, in_scale, gate_scale, taps, maps_r, maps_i,
    rate, extra, gated, xn, win, wgate, xpad, a_s, b_s, gel, block_maps, sems,
):
    length = xn.shape[0]
    chans = gated.shape[1]
    at = (place[0], place[1], place[2])
    loaded = pltpu.make_async_copy(normed, xn, sems.at[2])
    loaded.start()
    place_blocks(IN_ORDERS[0], (s0a, s0b), win.at[0], at, sems.at[0])
    place_blocks(IN_ORDERS[1], (s1a, s1b), win.at[1], at, sems.at[1])
    place_blocks(IN_ORDERS[2], (s2a, s2b), wgate.at[0], at, sems.at[3])
    place_blocks(IN_ORDERS[3], (s3a, s3b), wgate.at[1], at, sems.at[4])
    low = place[4] == 0

    def half(ref):
        return jnp.where(low, ref[:, :chans], ref[:, chans:])

    bd = maps_r.shape[1]
    per = CB // bd
    block_maps[...] = jnp.zeros(block_maps.shape, BF16)
    for n in range(chans // bd):
        k, i = n // per, n % per
        which = place[4] * (chans // bd) + n
        rows, cols = slice(i * bd, (i + 1) * bd), slice(i * bd, (i + 1) * bd)
        block_maps[k, rows, cols] = maps_r[which].astype(BF16)
        block_maps[k, rows, slice(CB + i * bd, CB + (i + 1) * bd)] = maps_i[which].astype(BF16)

    in_s, gate_s, tap, slope = half(in_scale), half(gate_scale), half(taps), half(rate)
    xpad[0:8, :] = jnp.zeros((8, CB), F32)
    groups = chans // LANES
    loaded.wait()
    wait_for(win.at[0], sems.at[0])
    wait_for(win.at[1], sems.at[1])
    wait_for(wgate.at[0], sems.at[3])
    wait_for(wgate.at[1], sems.at[4])
    for k in range(chans // CB):
        cols = slice(k * CB, (k + 1) * CB)
        pre = dot(xn[...], win[k]) * in_s[:, cols]
        xpad[8 : 8 + length, :] = pre.astype(BF16).astype(F32)
        conv = tap[3:4, cols] * xpad[8 : 8 + length, :]
        for j in range(3):
            conv = conv + tap[j : j + 1, cols] * xpad[5 + j : 5 + j + length, :]
        maps = dot(conv.astype(BF16), block_maps[k])
        recur = sigmoid(maps[:, :CB])
        ingate = sigmoid(maps[:, CB:])
        factor = jnp.exp(slope[:, cols] * recur - extra[...])
        rest = 1.0 - factor * factor
        drive = rest * lax.rsqrt(rest) * (ingate * conv)
        for g in range(CB // LANES):
            row = k * (CB // LANES) + g
            part = slice(g * LANES, (g + 1) * LANES)
            a_s[pl.ds(row, length, stride=groups), :] = factor[:, part]
            b_s[pl.ds(row, length, stride=groups), :] = drive[:, part]
    for k in range(chans // CB):
        cols = slice(k * CB, (k + 1) * CB)
        pre_gate = (dot(xn[...], wgate[k]) * gate_s[:, cols]).astype(BF16)
        gel[:, cols] = jax.nn.gelu(pre_gate.astype(F32), approximate=True)
    step = 64

    def scan(i, h):
        base = pl.multiple_of(i * (step * groups), step * groups)
        for t in range(step):
            rows = pl.ds(base + t * groups, groups)
            h = a_s[rows, :] * h + b_s[rows, :]
            b_s[rows, :] = h
        return h

    lax.fori_loop(0, length // step, scan, jnp.zeros((groups, LANES), F32))
    for g in range(groups):
        cols = slice(g * LANES, (g + 1) * LANES)
        gated[:, cols] = (b_s[pl.ds(g, length, stride=groups), :] * gel[:, cols]).astype(BF16)


def back_kernel(place, mine, other, s2a, s2b, s3a, s3b, partial, g, w0, w1, acc, outs, sems):
    at = (place[0], place[1], place[2])
    low = place[4]
    loads = [
        pltpu.make_async_copy(mine, g.at[low], sems.at[2]),
        pltpu.make_async_copy(other, g.at[1 - low], sems.at[3]),
    ]
    place_blocks(OUT_ORDERS[0], (s2a, s2b), w0, at, sems.at[0])
    for copy in loads:
        copy.start()
    place_blocks(OUT_ORDERS[1], (s3a, s3b), w1, at, sems.at[1])
    for copy in loads:
        copy.wait()
    wait_for(w0, sems.at[0])
    width = w0.shape[0]
    cols = partial.shape[2]
    piece = cols // 2
    for c in range(width // piece):
        rows = slice(c * piece, (c + 1) * piece)
        acc[:, rows] = dot_t(g[0], w0[rows, :])
    wait_for(w1, sems.at[1])
    sent = []
    for c in range(width // piece):
        rows = slice(c * piece, (c + 1) * piece)
        outs[c] = (acc[:, rows] + dot_t(g[1], w1[rows, :])).astype(BF16)
        copy = pltpu.make_async_copy(
            outs.at[c],
            partial.at[c // 2, :, pl.ds((c % 2) * piece, piece)],
            sems.at[4 + c],
        )
        copy.start()
        sent.append(copy)
    for copy in sent:
        copy.wait()


def norm_kernel(place, mine, other, gain, xn):
    put_halves(
        xn, lambda rows: (mine[rows, :].astype(F32), other[rows, :].astype(F32)), gain, place[3]
    )


def mixed_kernel(place, tok_mine, tok_other, part, got, out_scale, gain, mixed, xn):
    tp = place[3]

    def mix(tok, which, rows):
        total = part[which, rows, :].astype(F32) + got[which, rows, :].astype(F32)
        return (tok[rows, :].astype(F32) + total * out_scale[which]).astype(BF16)

    def halves(rows):
        a = mix(tok_mine, tp, rows)
        mixed[rows, :] = a
        return a.astype(F32), mix(tok_other, 1 - tp, rows).astype(F32)

    put_halves(xn, halves, gain, tp)


def ffn_kernel(
    place, normed, weights, gate_scale, up_scale, own, send, xn, wgate, wup, wdown, hid, outs, sems
):
    length, width = xn.shape
    hidden = gate_scale.shape[1]
    kdown = wdown.shape[2]
    starts = list(FFN_BLOCKS) + [hidden]
    blocks = [(s, e - s) for s, e in zip(starts[:-1], starts[1:])]
    copies = []

    def begin(source, target, sem):
        copy = pltpu.make_async_copy(source, target, sem)
        copy.start()
        return copy

    loaded = begin(normed, xn, sems.at[3, 0])
    for k, (s, n) in enumerate(blocks):
        for r, dst in ((0, wgate), (1, wup)):
            copies.append(
                begin(
                    weights.at[pl.ds(r * width, width), pl.ds(s, n)],
                    dst.at[:, pl.ds(s, n)],
                    sems.at[r, k],
                )
            )
    down_copies = [
        begin(
            weights.at[pl.ds(r * width, width), pl.ds(hidden, kdown)], wdown.at[r], sems.at[2, r]
        )
        for r in range(2)
    ]
    cols = width // 2
    tp = place[3]
    loaded.wait()
    for k, (s, n) in enumerate(blocks):
        part = slice(s, s + n)
        copies[2 * k].wait()
        copies[2 * k + 1].wait()
        gate = dot(xn[...], wgate[:, part]) * gate_scale[:, part]
        up = dot(xn[...], wup[:, part]) * up_scale[:, part]
        hid[:, part] = (gate * sigmoid(gate) * up).astype(BF16)
    for copy in down_copies:
        copy.wait()
    skip = 2 * kdown - hidden
    sent = []
    piece = cols // 2
    for i, (dst, which) in enumerate(((send, 1 - tp), (own, tp))):
        for j in range(2):
            rows = pl.ds(pl.multiple_of(which * cols + j * piece, piece), piece)
            acc = dot_t(hid[:, :kdown], wdown[0, rows, :])
            acc = acc + dot_t(hid[:, kdown:], wdown[1, rows, skip:])
            span = slice(j * piece, (j + 1) * piece)
            outs[i, :, span] = acc.astype(BF16)
            sent.append(begin(outs.at[i, :, span], dst.at[:, span], sems.at[4, 2 * i + j]))
    for copy in sent:
        copy.wait()


def local(
    tokens, mix_gain, lru_input, lru_gate, lru_input_scale, lru_gate_scale, conv_weight,
    recur_gate, input_gate, decay_rate, extra_decay, lru_output, lru_output_scale, ffn_gain,
    ffn_gate, ffn_up, ffn_gate_scale, ffn_up_scale, ffn_down, ffn_down_scale,
):
    length, cols = tokens.shape
    width = 2 * cols
    chans = lru_input.shape[1] // 2
    hidden = ffn_gate.shape[1]
    rep = lax.axis_index("rep")
    tp = lax.axis_index("tp")
    swap = [(0, 1), (1, 0)]
    place = jnp.stack(
        [lax.axis_index(axis) for axis in ("fs_0", "fs_1", "fs_2", "tp", "rep")]
    ).astype(jnp.int32)

    down_t = ffn_down.T
    kdown = -(-hidden // (2 * LANES)) * LANES
    skip = hidden - kdown
    first = jnp.concatenate([ffn_gate, down_t[:, :kdown]], axis=1)
    second = jnp.concatenate([ffn_up, down_t[:, skip:]], axis=1)
    mine = jnp.where(rep == 0, first, second).astype(BF16)

    pair = lambda v: lax.ppermute(v, ("rep", "fs_0"), ODD)
    lru = (lru_input, lru_gate)
    low = jnp.concatenate([w[:, :chans] for w in lru], axis=1).astype(BF16)
    high = jnp.concatenate([w[:, chans:] for w in lru], axis=1).astype(BF16)
    home = jnp.where(rep == 0, low, high)
    out = lru_output.T.astype(BF16)
    blocks = lambda h, k, n: h[None, :, k * n : (k + 1) * n]
    streams, ticks = spread_streams([blocks(home, k, CB) for k in range(4)], IN_ORDERS)
    late = [blocks(out, k, chans) for k in range(2)]
    late = list(lax.optimization_barrier((*late, ticks[1][0]))[:2])

    weights = lax.all_gather(mine, REP_FS, axis=0, tiled=True)

    guest = pair(tokens)
    guest_extra = pair(extra_decay)
    guest_other = lax.ppermute(guest, "tp", swap)
    tokens_other = lax.ppermute(tokens, "tp", swap)
    rate = -RATE * jax.nn.softplus(-decay_rate)

    vmem = pl.BlockSpec(memory_space=pltpu.VMEM)
    hbm = pl.BlockSpec(memory_space=pl.ANY)
    smem = pl.BlockSpec(memory_space=pltpu.SMEM)
    dma = pltpu.SemaphoreType.DMA
    row = lambda v: v.reshape(1, -1)
    groups = chans // LANES
    half_rows = jax.ShapeDtypeStruct((length, cols), BF16)

    blk = 256
    grid = (length // blk,)
    whole = lambda *dims: pl.BlockSpec(dims, lambda i: (0,) * len(dims))
    rows_of = lambda n: pl.BlockSpec((blk, n), lambda i: (i, 0))

    def norm(mine, other):
        return pl.pallas_call(
            norm_kernel,
            grid=grid,
            out_shape=jax.ShapeDtypeStruct((length, width), BF16),
            in_specs=[smem, rows_of(cols), rows_of(cols), whole(1, width)],
            out_specs=rows_of(width),
            name="norm",
        )(place, mine, other, row(mix_gain))

    def mix(normed, extra):
        return pl.pallas_call(
            front_kernel,
            out_shape=jax.ShapeDtypeStruct((length, chans), BF16),
            in_specs=[smem, hbm] + [hbm] * 8 + [vmem] * 7,
            out_specs=vmem,
            scratch_shapes=[
                pltpu.VMEM((length, width), BF16),
                pltpu.VMEM((chans // CB, width, CB), BF16),
                pltpu.VMEM((chans // CB, width, CB), BF16),
                pltpu.VMEM((length + 8, CB), F32),
                pltpu.VMEM((length * groups, LANES), F32),
                pltpu.VMEM((length * groups, LANES), F32),
                pltpu.VMEM((length, chans), F32),
                pltpu.VMEM((chans // CB, CB, 2 * CB), BF16),
                dma((5,)),
            ],
            name="front",
        )(
            place, normed, *streams[0], *streams[1], *streams[2], *streams[3],
            row(lru_input_scale),
            row(lru_gate_scale), conv_weight, recur_gate, input_gate, row(rate),
            extra.reshape(-1, 1),
        )

    normed = norm(tokens, tokens_other)
    guest_normed = norm(guest, guest_other)
    outs, _ = spread_streams(
        late, OUT_ORDERS, (None, None, None, None, (normed, guest_normed))
    )
    guest_gated = mix(guest_normed, guest_extra)
    normed, guest_gated = lax.optimization_barrier((normed, guest_gated))
    gated_away = pair(guest_gated)
    gated = mix(normed, extra_decay)
    partial = pl.pallas_call(
        back_kernel,
        out_shape=jax.ShapeDtypeStruct((2, length, cols), BF16),
        in_specs=[smem] + [hbm] * 6,
        out_specs=hbm,
        scratch_shapes=[
            pltpu.VMEM((2, length, chans), BF16),
            pltpu.VMEM((width, chans), BF16),
            pltpu.VMEM((width, chans), BF16),
            pltpu.VMEM((length, width), F32),
            pltpu.VMEM((4, length, width // 4), BF16),
            dma((8,)),
        ],
        name="back",
    )(place, gated, gated_away, *outs[0], *outs[1])
    got = lax.ppermute(partial, "tp", swap)
    mixed, normed = pl.pallas_call(
        mixed_kernel,
        grid=grid,
        out_shape=[half_rows, jax.ShapeDtypeStruct((length, width), BF16)],
        in_specs=[smem, rows_of(cols), rows_of(cols)]
        + [pl.BlockSpec((2, blk, cols), lambda i: (0, i, 0))] * 2
        + [whole(2, 1, cols), whole(1, width)],
        out_specs=[rows_of(cols), rows_of(width)],
        name="mixed",
    )(
        place, tokens, tokens_other, partial, got, lru_output_scale.reshape(2, 1, cols),
        row(ffn_gain),
    )
    own, send = pl.pallas_call(
        ffn_kernel,
        out_shape=[half_rows] * 2,
        in_specs=[smem, hbm, hbm, vmem, vmem],
        out_specs=[hbm] * 2,
        scratch_shapes=[
            pltpu.VMEM((length, width), BF16),
            pltpu.VMEM((width, hidden), BF16),
            pltpu.VMEM((width, hidden), BF16),
            pltpu.VMEM((2, width, kdown), BF16),
            pltpu.VMEM((length, hidden), BF16),
            pltpu.VMEM((2, length, cols), BF16),
            dma((5, 4)),
        ],
        name="ffn",
    )(place, normed, weights, row(ffn_gate_scale), row(ffn_up_scale))
    got = lax.ppermute(send, "tp", swap)
    scale = lax.dynamic_slice_in_dim(ffn_down_scale, tp * cols, cols)
    total = own.astype(F32) + got.astype(F32)
    return (mixed.astype(F32) + total * scale).astype(BF16)


def solution(mesh):
    split = Mesh(
        mesh.devices.reshape(mesh.shape["rep"], 2, 4, 4, mesh.shape["tp"]),
        ("rep", "fs_0", "fs_1", "fs_2", "tp"),
    )
    in_specs = (
        P(REP_FS, "tp"),
        P(),
        P(FS, "tp"),
        P(FS, "tp"),
        P("tp"),
        P("tp"),
        P(None, "tp"),
        P("tp", None, None),
        P("tp", None, None),
        P("tp"),
        P(REP_FS),
        P("tp", FS),
        P(),
        P(),
        P(FS, "tp"),
        P(FS, "tp"),
        P("tp"),
        P("tp"),
        P("tp", FS),
        P(),
    )
    out_specs = P(REP_FS, "tp")
    return jax.shard_map(local, mesh=split, in_specs=in_specs, out_specs=out_specs, check_vma=False)
```

```python
import jax
import jax.numpy as jnp
from jax import lax
from jax.experimental import pallas as pl
from jax.experimental.pallas import tpu as pltpu
from jax.sharding import Mesh
from jax.sharding import PartitionSpec as P

FS = ("fs_0", "fs_1", "fs_2")
REP_FS = ("rep", "fs_0", "fs_1", "fs_2")

EPS = 1e-06
RATE = 8.0
F32 = jnp.float32
BF16 = jnp.bfloat16
CB = 256
LANES = 128
FFN_BLOCKS = (0, 256, 512, 1024)


def sigmoid(v):
    return 0.5 + 0.5 * jnp.tanh(0.5 * v)


def dot(a, b):
    return jnp.dot(a, b, preferred_element_type=F32)


def dot_t(a, b):
    return lax.dot_general(a, b, (((1,), (1,)), ((), ())), preferred_element_type=F32)


def partner(kind, place):
    z, y, x = place
    if kind == "z":
        return z ^ 1, y, x
    if kind == "ye":
        return z, y ^ 1, x
    if kind == "yo":
        return z, (((y + 1) ^ 1) + 3) % 4, x
    if kind == "xe":
        return z, y, x ^ 1
    return z, y, (((x + 1) ^ 1) + 3) % 4


ODD = [(0, 3), (3, 0), (1, 2), (2, 1)]
EVEN = [(0, 1), (1, 0), (2, 3), (3, 2)]
PAIRS = {
    "z": ("fs_0", [(0, 1), (1, 0)]),
    "ye": ("fs_1", EVEN),
    "yo": ("fs_1", ODD),
    "xe": ("fs_2", EVEN),
    "xo": ("fs_2", ODD),
}
KINDS = ("xe", "ye", "z", "xo", "yo")
OUT_ORDERS = (("z", "ye", "yo", "xe", "xo"), ("yo", "xe", "xo", "ye", "z"))


IN_ORDERS = tuple(KINDS[k:] + KINDS[:k] for k in range(4))


def origin(order, index, place):
    for s in reversed(range(len(order))):
        bit = (index >> s) & 1
        place = tuple(a + bit * (b - a) for a, b in zip(place, partner(order[s], place)))
    z, y, x = place
    return (z * 4 + y) * 4 + x


def spread_streams(held, orders, after=()):
    got = [None] * len(held)
    ticks = []
    for s in range(len(KINDS)):
        for k in range(len(held)):
            if s > 0:
                joined = jnp.concatenate([held[k], got[k]], axis=0)
                ready = after[s] if s < len(after) and after[s] is not None else ()
                held[k] = lax.optimization_barrier((joined, *ready))[0]
        for k in range(len(held)):
            axis, pairs = PAIRS[orders[k][s]]
            got[k] = lax.ppermute(held[k], axis, pairs)
        ticks.append(list(got))
    return [(h, g) for h, g in zip(held, got)], ticks


def place_blocks(order, halves, target, place, sem):
    count, rows = halves[0].shape[0], halves[0].shape[1]
    for h, half in enumerate(halves):

        def begin(i, carry, h=h, half=half):
            at = pl.multiple_of(origin(order, h * count + i, place) * rows, rows)
            pltpu.make_async_copy(half.at[i], target.at[pl.ds(at, rows)], sem).start()
            return carry

        lax.fori_loop(0, count, begin, 0)


def wait_for(target, sem):
    pltpu.make_async_copy(target, target, sem).wait()


def put_halves(xn, halves, gain, tp):
    length, width = xn.shape
    cols = width // 2
    low, high = gain[:, :cols], gain[:, cols:]
    first = tp == 0
    gain_a, gain_b = jnp.where(first, low, high), jnp.where(first, high, low)
    step = 16
    for r in range(0, length, step):
        rows = slice(r, r + step)
        a, b = halves(rows)
        squares = jnp.sum(a * a + b * b, axis=-1, keepdims=True)
        scale = lax.rsqrt(squares * (1.0 / width) + EPS)
        a = a * scale * gain_a
        b = b * scale * gain_b
        xn[rows, :cols] = jnp.where(first, a, b).astype(BF16)
        xn[rows, cols:] = jnp.where(first, b, a).astype(BF16)


def front_kernel(
    place, normed, s0a, s0b, s1a, s1b, s2a, s2b, s3a, s3b, in_scale, gate_scale, taps, maps_r, maps_i,
    rate, extra, gated, xn, win, wgate, xpad, a_s, b_s, gel, block_maps, sems,
):
    length = xn.shape[0]
    chans = gated.shape[1]
    at = (place[0], place[1], place[2])
    loaded = pltpu.make_async_copy(normed, xn, sems.at[2])
    loaded.start()
    place_blocks(IN_ORDERS[0], (s0a, s0b), win.at[0], at, sems.at[0])
    place_blocks(IN_ORDERS[1], (s1a, s1b), win.at[1], at, sems.at[1])
    place_blocks(IN_ORDERS[2], (s2a, s2b), wgate.at[0], at, sems.at[3])
    place_blocks(IN_ORDERS[3], (s3a, s3b), wgate.at[1], at, sems.at[4])
    low = place[4] == 0

    def half(ref):
        return jnp.where(low, ref[:, :chans], ref[:, chans:])

    bd = maps_r.shape[1]
    per = CB // bd
    block_maps[...] = jnp.zeros(block_maps.shape, BF16)
    for n in range(chans // bd):
        k, i = n // per, n % per
        which = place[4] * (chans // bd) + n
        rows, cols = slice(i * bd, (i + 1) * bd), slice(i * bd, (i + 1) * bd)
        block_maps[k, rows, cols] = maps_r[which].astype(BF16)
        block_maps[k, rows, slice(CB + i * bd, CB + (i + 1) * bd)] = maps_i[which].astype(BF16)

    in_s, gate_s, tap, slope = half(in_scale), half(gate_scale), half(taps), half(rate)
    xpad[0:8, :] = jnp.zeros((8, CB), F32)
    groups = chans // LANES
    loaded.wait()
    wait_for(win.at[0], sems.at[0])
    wait_for(win.at[1], sems.at[1])
    wait_for(wgate.at[0], sems.at[3])
    wait_for(wgate.at[1], sems.at[4])
    for k in range(chans // CB):
        cols = slice(k * CB, (k + 1) * CB)
        pre = dot(xn[...], win[k]) * in_s[:, cols]
        xpad[8 : 8 + length, :] = pre.astype(BF16).astype(F32)
        conv = tap[3:4, cols] * xpad[8 : 8 + length, :]
        for j in range(3):
            conv = conv + tap[j : j + 1, cols] * xpad[5 + j : 5 + j + length, :]
        maps = dot(conv.astype(BF16), block_maps[k])
        recur = sigmoid(maps[:, :CB])
        ingate = sigmoid(maps[:, CB:])
        factor = jnp.exp(slope[:, cols] * recur - extra[...])
        rest = 1.0 - factor * factor
        drive = rest * lax.rsqrt(rest) * (ingate * conv)
        for g in range(CB // LANES):
            row = k * (CB // LANES) + g
            part = slice(g * LANES, (g + 1) * LANES)
            a_s[pl.ds(row, length, stride=groups), :] = factor[:, part]
            b_s[pl.ds(row, length, stride=groups), :] = drive[:, part]
    for k in range(chans // CB):
        cols = slice(k * CB, (k + 1) * CB)
        pre_gate = (dot(xn[...], wgate[k]) * gate_s[:, cols]).astype(BF16)
        gel[:, cols] = jax.nn.gelu(pre_gate.astype(F32), approximate=True)
    step = 64

    def scan(i, h):
        base = pl.multiple_of(i * (step * groups), step * groups)
        for t in range(step):
            rows = pl.ds(base + t * groups, groups)
            h = a_s[rows, :] * h + b_s[rows, :]
            b_s[rows, :] = h
        return h

    lax.fori_loop(0, length // step, scan, jnp.zeros((groups, LANES), F32))
    for g in range(groups):
        cols = slice(g * LANES, (g + 1) * LANES)
        gated[:, cols] = (b_s[pl.ds(g, length, stride=groups), :] * gel[:, cols]).astype(BF16)


def back_kernel(place, mine, other, s2a, s2b, s3a, s3b, partial, g, w0, w1, acc, outs, sems):
    at = (place[0], place[1], place[2])
    low = place[4]
    loads = [
        pltpu.make_async_copy(mine, g.at[low], sems.at[2]),
        pltpu.make_async_copy(other, g.at[1 - low], sems.at[3]),
    ]
    place_blocks(OUT_ORDERS[0], (s2a, s2b), w0, at, sems.at[0])
    for copy in loads:
        copy.start()
    place_blocks(OUT_ORDERS[1], (s3a, s3b), w1, at, sems.at[1])
    for copy in loads:
        copy.wait()
    wait_for(w0, sems.at[0])
    width = w0.shape[0]
    cols = partial.shape[2]
    piece = cols // 2
    for c in range(width // piece):
        rows = slice(c * piece, (c + 1) * piece)
        acc[:, rows] = dot_t(g[0], w0[rows, :])
    wait_for(w1, sems.at[1])
    sent = []
    for c in range(width // piece):
        rows = slice(c * piece, (c + 1) * piece)
        outs[c] = (acc[:, rows] + dot_t(g[1], w1[rows, :])).astype(BF16)
        copy = pltpu.make_async_copy(
            outs.at[c],
            partial.at[c // 2, :, pl.ds((c % 2) * piece, piece)],
            sems.at[4 + c],
        )
        copy.start()
        sent.append(copy)
    for copy in sent:
        copy.wait()


def norm_kernel(place, mine, other, gain, xn):
    put_halves(
        xn, lambda rows: (mine[rows, :].astype(F32), other[rows, :].astype(F32)), gain, place[3]
    )


def mixed_kernel(place, tok_mine, tok_other, part, got, out_scale, gain, mixed, xn):
    tp = place[3]

    def mix(tok, which, rows):
        total = part[which, rows, :].astype(F32) + got[which, rows, :].astype(F32)
        return (tok[rows, :].astype(F32) + total * out_scale[which]).astype(BF16)

    def halves(rows):
        a = mix(tok_mine, tp, rows)
        mixed[rows, :] = a
        return a.astype(F32), mix(tok_other, 1 - tp, rows).astype(F32)

    put_halves(xn, halves, gain, tp)


def ffn_kernel(
    place, normed, weights, gate_scale, up_scale, own, send, xn, wgate, wup, wdown, hid, outs, sems
):
    length, width = xn.shape
    hidden = gate_scale.shape[1]
    kdown = wdown.shape[2]
    starts = list(FFN_BLOCKS) + [hidden]
    blocks = [(s, e - s) for s, e in zip(starts[:-1], starts[1:])]
    copies = []

    def begin(source, target, sem):
        copy = pltpu.make_async_copy(source, target, sem)
        copy.start()
        return copy

    loaded = begin(normed, xn, sems.at[3, 0])
    for k, (s, n) in enumerate(blocks):
        for r, dst in ((0, wgate), (1, wup)):
            copies.append(
                begin(
                    weights.at[pl.ds(r * width, width), pl.ds(s, n)],
                    dst.at[:, pl.ds(s, n)],
                    sems.at[r, k],
                )
            )
    down_copies = [
        begin(
            weights.at[pl.ds(r * width, width), pl.ds(hidden, kdown)], wdown.at[r], sems.at[2, r]
        )
        for r in range(2)
    ]
    cols = width // 2
    tp = place[3]
    loaded.wait()
    for k, (s, n) in enumerate(blocks):
        part = slice(s, s + n)
        copies[2 * k].wait()
        copies[2 * k + 1].wait()
        gate = dot(xn[...], wgate[:, part]) * gate_scale[:, part]
        up = dot(xn[...], wup[:, part]) * up_scale[:, part]
        hid[:, part] = (gate * sigmoid(gate) * up).astype(BF16)
    for copy in down_copies:
        copy.wait()
    skip = 2 * kdown - hidden
    sent = []
    piece = cols // 2
    for i, (dst, which) in enumerate(((send, 1 - tp), (own, tp))):
        for j in range(2):
            rows = pl.ds(pl.multiple_of(which * cols + j * piece, piece), piece)
            acc = dot_t(hid[:, :kdown], wdown[0, rows, :])
            acc = acc + dot_t(hid[:, kdown:], wdown[1, rows, skip:])
            span = slice(j * piece, (j + 1) * piece)
            outs[i, :, span] = acc.astype(BF16)
            sent.append(begin(outs.at[i, :, span], dst.at[:, span], sems.at[4, 2 * i + j]))
    for copy in sent:
        copy.wait()


def local(
    tokens, mix_gain, lru_input, lru_gate, lru_input_scale, lru_gate_scale, conv_weight,
    recur_gate, input_gate, decay_rate, extra_decay, lru_output, lru_output_scale, ffn_gain,
    ffn_gate, ffn_up, ffn_gate_scale, ffn_up_scale, ffn_down, ffn_down_scale,
):
    length, cols = tokens.shape
    width = 2 * cols
    chans = lru_input.shape[1] // 2
    hidden = ffn_gate.shape[1]
    rep = lax.axis_index("rep")
    tp = lax.axis_index("tp")
    swap = [(0, 1), (1, 0)]
    place = jnp.stack(
        [lax.axis_index(axis) for axis in ("fs_0", "fs_1", "fs_2", "tp", "rep")]
    ).astype(jnp.int32)

    down_t = ffn_down.T
    kdown = -(-hidden // (2 * LANES)) * LANES
    skip = hidden - kdown
    first = jnp.concatenate([ffn_gate, down_t[:, :kdown]], axis=1)
    second = jnp.concatenate([ffn_up, down_t[:, skip:]], axis=1)
    mine = jnp.where(rep == 0, first, second).astype(BF16)

    pair = lambda v: lax.ppermute(v, ("rep", "fs_0"), ODD)
    lru = (lru_input, lru_gate)
    low = jnp.concatenate([w[:, :chans] for w in lru], axis=1).astype(BF16)
    high = jnp.concatenate([w[:, chans:] for w in lru], axis=1).astype(BF16)
    home = jnp.where(rep == 0, low, high)
    out = lru_output.T.astype(BF16)
    blocks = lambda h, k, n: h[None, :, k * n : (k + 1) * n]
    streams, ticks = spread_streams([blocks(home, k, CB) for k in range(4)], IN_ORDERS)
    late = [blocks(out, k, chans) for k in range(2)]
    late = list(lax.optimization_barrier((*late, ticks[0][0]))[:2])

    weights = lax.all_gather(mine, REP_FS, axis=0, tiled=True)

    guest = pair(tokens)
    guest_extra = pair(extra_decay)
    guest_other = lax.ppermute(guest, "tp", swap)
    tokens_other = lax.ppermute(tokens, "tp", swap)
    rate = -RATE * jax.nn.softplus(-decay_rate)

    vmem = pl.BlockSpec(memory_space=pltpu.VMEM)
    hbm = pl.BlockSpec(memory_space=pl.ANY)
    smem = pl.BlockSpec(memory_space=pltpu.SMEM)
    dma = pltpu.SemaphoreType.DMA
    row = lambda v: v.reshape(1, -1)
    groups = chans // LANES
    half_rows = jax.ShapeDtypeStruct((length, cols), BF16)

    blk = 256
    grid = (length // blk,)
    whole = lambda *dims: pl.BlockSpec(dims, lambda i: (0,) * len(dims))
    rows_of = lambda n: pl.BlockSpec((blk, n), lambda i: (i, 0))

    def norm(mine, other):
        return pl.pallas_call(
            norm_kernel,
            grid=grid,
            out_shape=jax.ShapeDtypeStruct((length, width), BF16),
            in_specs=[smem, rows_of(cols), rows_of(cols), whole(1, width)],
            out_specs=rows_of(width),
            name="norm",
        )(place, mine, other, row(mix_gain))

    def mix(normed, extra):
        return pl.pallas_call(
            front_kernel,
            out_shape=jax.ShapeDtypeStruct((length, chans), BF16),
            in_specs=[smem, hbm] + [hbm] * 8 + [vmem] * 7,
            out_specs=vmem,
            scratch_shapes=[
                pltpu.VMEM((length, width), BF16),
                pltpu.VMEM((chans // CB, width, CB), BF16),
                pltpu.VMEM((chans // CB, width, CB), BF16),
                pltpu.VMEM((length + 8, CB), F32),
                pltpu.VMEM((length * groups, LANES), F32),
                pltpu.VMEM((length * groups, LANES), F32),
                pltpu.VMEM((length, chans), F32),
                pltpu.VMEM((chans // CB, CB, 2 * CB), BF16),
                dma((5,)),
            ],
            name="front",
        )(
            place, normed, *streams[0], *streams[1], *streams[2], *streams[3],
            row(lru_input_scale),
            row(lru_gate_scale), conv_weight, recur_gate, input_gate, row(rate),
            extra.reshape(-1, 1),
        )

    normed = norm(tokens, tokens_other)
    guest_normed = norm(guest, guest_other)
    outs, _ = spread_streams(
        late, OUT_ORDERS, (None, None, None, None, (normed, guest_normed))
    )
    guest_gated = mix(guest_normed, guest_extra)
    normed, guest_gated = lax.optimization_barrier((normed, guest_gated))
    gated_away = pair(guest_gated)
    gated = mix(normed, extra_decay)
    partial = pl.pallas_call(
        back_kernel,
        out_shape=jax.ShapeDtypeStruct((2, length, cols), BF16),
        in_specs=[smem] + [hbm] * 6,
        out_specs=hbm,
        scratch_shapes=[
            pltpu.VMEM((2, length, chans), BF16),
            pltpu.VMEM((width, chans), BF16),
            pltpu.VMEM((width, chans), BF16),
            pltpu.VMEM((length, width), F32),
            pltpu.VMEM((4, length, width // 4), BF16),
            dma((8,)),
        ],
        name="back",
    )(place, gated, gated_away, *outs[0], *outs[1])
    got = lax.ppermute(partial, "tp", swap)
    mixed, normed = pl.pallas_call(
        mixed_kernel,
        grid=grid,
        out_shape=[half_rows, jax.ShapeDtypeStruct((length, width), BF16)],
        in_specs=[smem, rows_of(cols), rows_of(cols)]
        + [pl.BlockSpec((2, blk, cols), lambda i: (0, i, 0))] * 2
        + [whole(2, 1, cols), whole(1, width)],
        out_specs=[rows_of(cols), rows_of(width)],
        name="mixed",
    )(
        place, tokens, tokens_other, partial, got, lru_output_scale.reshape(2, 1, cols),
        row(ffn_gain),
    )
    own, send = pl.pallas_call(
        ffn_kernel,
        out_shape=[half_rows] * 2,
        in_specs=[smem, hbm, hbm, vmem, vmem],
        out_specs=[hbm] * 2,
        scratch_shapes=[
            pltpu.VMEM((length, width), BF16),
            pltpu.VMEM((width, hidden), BF16),
            pltpu.VMEM((width, hidden), BF16),
            pltpu.VMEM((2, width, kdown), BF16),
            pltpu.VMEM((length, hidden), BF16),
            pltpu.VMEM((2, length, cols), BF16),
            dma((5, 4)),
        ],
        name="ffn",
    )(place, normed, weights, row(ffn_gate_scale), row(ffn_up_scale))
    got = lax.ppermute(send, "tp", swap)
    scale = lax.dynamic_slice_in_dim(ffn_down_scale, tp * cols, cols)
    total = own.astype(F32) + got.astype(F32)
    return (mixed.astype(F32) + total * scale).astype(BF16)


def solution(mesh):
    split = Mesh(
        mesh.devices.reshape(mesh.shape["rep"], 2, 4, 4, mesh.shape["tp"]),
        ("rep", "fs_0", "fs_1", "fs_2", "tp"),
    )
    in_specs = (
        P(REP_FS, "tp"),
        P(),
        P(FS, "tp"),
        P(FS, "tp"),
        P("tp"),
        P("tp"),
        P(None, "tp"),
        P("tp", None, None),
        P("tp", None, None),
        P("tp"),
        P(REP_FS),
        P("tp", FS),
        P(),
        P(),
        P(FS, "tp"),
        P(FS, "tp"),
        P("tp"),
        P("tp"),
        P("tp", FS),
        P(),
    )
    out_specs = P(REP_FS, "tp")
    return jax.shard_map(local, mesh=split, in_specs=in_specs, out_specs=out_specs, check_vma=False)
```

```python
import jax
import jax.numpy as jnp
from jax import lax
from jax.experimental import pallas as pl
from jax.experimental.pallas import tpu as pltpu
from jax.sharding import Mesh
from jax.sharding import PartitionSpec as P

FS = ("fs_0", "fs_1", "fs_2")
REP_FS = ("rep", "fs_0", "fs_1", "fs_2")

EPS = 1e-06
RATE = 8.0
F32 = jnp.float32
BF16 = jnp.bfloat16
CB = 256
LANES = 128
FFN_BLOCKS = (0, 256, 512, 1024)


def sigmoid(v):
    return 0.5 + 0.5 * jnp.tanh(0.5 * v)


def dot(a, b):
    return jnp.dot(a, b, preferred_element_type=F32)


def dot_t(a, b):
    return lax.dot_general(a, b, (((1,), (1,)), ((), ())), preferred_element_type=F32)


def partner(kind, place):
    z, y, x = place
    if kind == "z":
        return z ^ 1, y, x
    if kind == "ye":
        return z, y ^ 1, x
    if kind == "yo":
        return z, (((y + 1) ^ 1) + 3) % 4, x
    if kind == "xe":
        return z, y, x ^ 1
    return z, y, (((x + 1) ^ 1) + 3) % 4


ODD = [(0, 3), (3, 0), (1, 2), (2, 1)]
EVEN = [(0, 1), (1, 0), (2, 3), (3, 2)]
PAIRS = {
    "z": ("fs_0", [(0, 1), (1, 0)]),
    "ye": ("fs_1", EVEN),
    "yo": ("fs_1", ODD),
    "xe": ("fs_2", EVEN),
    "xo": ("fs_2", ODD),
}
KINDS = ("xe", "ye", "z", "xo", "yo")
OUT_ORDERS = (("z", "ye", "yo", "xe", "xo"), ("yo", "xe", "xo", "ye", "z"))


IN_ORDERS = tuple(KINDS[k:] + KINDS[:k] for k in range(4))


def origin(order, index, place):
    for s in reversed(range(len(order))):
        bit = (index >> s) & 1
        place = tuple(a + bit * (b - a) for a, b in zip(place, partner(order[s], place)))
    z, y, x = place
    return (z * 4 + y) * 4 + x


def spread_streams(held, orders, after=()):
    got = [None] * len(held)
    ticks = []
    for s in range(len(KINDS)):
        for k in range(len(held)):
            if s > 0:
                joined = jnp.concatenate([held[k], got[k]], axis=0)
                ready = after[s] if s < len(after) and after[s] is not None else ()
                held[k] = lax.optimization_barrier((joined, *ready))[0]
        for k in range(len(held)):
            axis, pairs = PAIRS[orders[k][s]]
            got[k] = lax.ppermute(held[k], axis, pairs)
        ticks.append(list(got))
    return [(h, g) for h, g in zip(held, got)], ticks


def place_blocks(order, halves, target, place, sem):
    count, rows = halves[0].shape[0], halves[0].shape[1]
    for h, half in enumerate(halves):

        def begin(i, carry, h=h, half=half):
            at = pl.multiple_of(origin(order, h * count + i, place) * rows, rows)
            pltpu.make_async_copy(half.at[i], target.at[pl.ds(at, rows)], sem).start()
            return carry

        lax.fori_loop(0, count, begin, 0)


def wait_for(target, sem):
    pltpu.make_async_copy(target, target, sem).wait()


def put_halves(xn, halves, gain, tp):
    length, width = xn.shape
    cols = width // 2
    low, high = gain[:, :cols], gain[:, cols:]
    first = tp == 0
    gain_a, gain_b = jnp.where(first, low, high), jnp.where(first, high, low)
    step = 16
    for r in range(0, length, step):
        rows = slice(r, r + step)
        a, b = halves(rows)
        squares = jnp.sum(a * a + b * b, axis=-1, keepdims=True)
        scale = lax.rsqrt(squares * (1.0 / width) + EPS)
        a = a * scale * gain_a
        b = b * scale * gain_b
        xn[rows, :cols] = jnp.where(first, a, b).astype(BF16)
        xn[rows, cols:] = jnp.where(first, b, a).astype(BF16)


def front_kernel(
    place, normed, s0a, s0b, s1a, s1b, s2a, s2b, s3a, s3b, in_scale, gate_scale, taps, maps_r, maps_i,
    rate, extra, gated, xn, win, wgate, xpad, a_s, b_s, gel, block_maps, sems,
):
    length = xn.shape[0]
    chans = gated.shape[1]
    at = (place[0], place[1], place[2])
    loaded = pltpu.make_async_copy(normed, xn, sems.at[2])
    loaded.start()
    place_blocks(IN_ORDERS[0], (s0a, s0b), win.at[0], at, sems.at[0])
    place_blocks(IN_ORDERS[1], (s1a, s1b), win.at[1], at, sems.at[1])
    place_blocks(IN_ORDERS[2], (s2a, s2b), wgate.at[0], at, sems.at[3])
    place_blocks(IN_ORDERS[3], (s3a, s3b), wgate.at[1], at, sems.at[4])
    low = place[4] == 0

    def half(ref):
        return jnp.where(low, ref[:, :chans], ref[:, chans:])

    bd = maps_r.shape[1]
    per = CB // bd
    block_maps[...] = jnp.zeros(block_maps.shape, BF16)
    for n in range(chans // bd):
        k, i = n // per, n % per
        which = place[4] * (chans // bd) + n
        rows, cols = slice(i * bd, (i + 1) * bd), slice(i * bd, (i + 1) * bd)
        block_maps[k, rows, cols] = maps_r[which].astype(BF16)
        block_maps[k, rows, slice(CB + i * bd, CB + (i + 1) * bd)] = maps_i[which].astype(BF16)

    in_s, gate_s, tap, slope = half(in_scale), half(gate_scale), half(taps), half(rate)
    xpad[0:8, :] = jnp.zeros((8, CB), F32)
    groups = chans // LANES
    loaded.wait()
    wait_for(win.at[0], sems.at[0])
    wait_for(win.at[1], sems.at[1])
    wait_for(wgate.at[0], sems.at[3])
    wait_for(wgate.at[1], sems.at[4])
    for k in range(chans // CB):
        cols = slice(k * CB, (k + 1) * CB)
        pre = dot(xn[...], win[k]) * in_s[:, cols]
        xpad[8 : 8 + length, :] = pre.astype(BF16).astype(F32)
        conv = tap[3:4, cols] * xpad[8 : 8 + length, :]
        for j in range(3):
            conv = conv + tap[j : j + 1, cols] * xpad[5 + j : 5 + j + length, :]
        maps = dot(conv.astype(BF16), block_maps[k])
        recur = sigmoid(maps[:, :CB])
        ingate = sigmoid(maps[:, CB:])
        factor = jnp.exp(slope[:, cols] * recur - extra[...])
        rest = 1.0 - factor * factor
        drive = rest * lax.rsqrt(rest) * (ingate * conv)
        for g in range(CB // LANES):
            row = k * (CB // LANES) + g
            part = slice(g * LANES, (g + 1) * LANES)
            a_s[pl.ds(row, length, stride=groups), :] = factor[:, part]
            b_s[pl.ds(row, length, stride=groups), :] = drive[:, part]
    for k in range(chans // CB):
        cols = slice(k * CB, (k + 1) * CB)
        pre_gate = (dot(xn[...], wgate[k]) * gate_s[:, cols]).astype(BF16)
        gel[:, cols] = jax.nn.gelu(pre_gate.astype(F32), approximate=True)
    step = 64

    def scan(i, h):
        base = pl.multiple_of(i * (step * groups), step * groups)
        for t in range(step):
            rows = pl.ds(base + t * groups, groups)
            h = a_s[rows, :] * h + b_s[rows, :]
            b_s[rows, :] = h
        return h

    lax.fori_loop(0, length // step, scan, jnp.zeros((groups, LANES), F32))
    for g in range(groups):
        cols = slice(g * LANES, (g + 1) * LANES)
        gated[:, cols] = (b_s[pl.ds(g, length, stride=groups), :] * gel[:, cols]).astype(BF16)


def back_kernel(place, mine, other, s2a, s2b, s3a, s3b, partial, g, w0, w1, acc, outs, sems):
    at = (place[0], place[1], place[2])
    low = place[4]
    loads = [
        pltpu.make_async_copy(mine, g.at[low], sems.at[2]),
        pltpu.make_async_copy(other, g.at[1 - low], sems.at[3]),
    ]
    place_blocks(OUT_ORDERS[0], (s2a, s2b), w0, at, sems.at[0])
    for copy in loads:
        copy.start()
    place_blocks(OUT_ORDERS[1], (s3a, s3b), w1, at, sems.at[1])
    for copy in loads:
        copy.wait()
    wait_for(w0, sems.at[0])
    width = w0.shape[0]
    cols = partial.shape[2]
    piece = cols // 2
    for c in range(width // piece):
        rows = slice(c * piece, (c + 1) * piece)
        acc[:, rows] = dot_t(g[0], w0[rows, :])
    wait_for(w1, sems.at[1])
    sent = []
    for c in range(width // piece):
        rows = slice(c * piece, (c + 1) * piece)
        outs[c] = (acc[:, rows] + dot_t(g[1], w1[rows, :])).astype(BF16)
        copy = pltpu.make_async_copy(
            outs.at[c],
            partial.at[c // 2, :, pl.ds((c % 2) * piece, piece)],
            sems.at[4 + c],
        )
        copy.start()
        sent.append(copy)
    for copy in sent:
        copy.wait()


def norm_kernel(place, mine, other, gain, xn):
    put_halves(
        xn, lambda rows: (mine[rows, :].astype(F32), other[rows, :].astype(F32)), gain, place[3]
    )


def mixed_kernel(place, tok_mine, tok_other, part, got, out_scale, gain, mixed, xn):
    tp = place[3]

    def mix(tok, which, rows):
        total = part[which, rows, :].astype(F32) + got[which, rows, :].astype(F32)
        return (tok[rows, :].astype(F32) + total * out_scale[which]).astype(BF16)

    def halves(rows):
        a = mix(tok_mine, tp, rows)
        mixed[rows, :] = a
        return a.astype(F32), mix(tok_other, 1 - tp, rows).astype(F32)

    put_halves(xn, halves, gain, tp)


def ffn_kernel(
    place, normed, weights, gate_scale, up_scale, own, send, xn, wgate, wup, wdown, hid, outs, sems
):
    length, width = xn.shape
    hidden = gate_scale.shape[1]
    kdown = wdown.shape[2]
    starts = list(FFN_BLOCKS) + [hidden]
    blocks = [(s, e - s) for s, e in zip(starts[:-1], starts[1:])]
    copies = []

    def begin(source, target, sem):
        copy = pltpu.make_async_copy(source, target, sem)
        copy.start()
        return copy

    loaded = begin(normed, xn, sems.at[3, 0])
    for k, (s, n) in enumerate(blocks):
        for r, dst in ((0, wgate), (1, wup)):
            copies.append(
                begin(
                    weights.at[pl.ds(r * width, width), pl.ds(s, n)],
                    dst.at[:, pl.ds(s, n)],
                    sems.at[r, k],
                )
            )
    down_copies = [
        begin(
            weights.at[pl.ds(r * width, width), pl.ds(hidden, kdown)], wdown.at[r], sems.at[2, r]
        )
        for r in range(2)
    ]
    cols = width // 2
    tp = place[3]
    loaded.wait()
    for k, (s, n) in enumerate(blocks):
        part = slice(s, s + n)
        copies[2 * k].wait()
        copies[2 * k + 1].wait()
        gate = dot(xn[...], wgate[:, part]) * gate_scale[:, part]
        up = dot(xn[...], wup[:, part]) * up_scale[:, part]
        hid[:, part] = (gate * sigmoid(gate) * up).astype(BF16)
    for copy in down_copies:
        copy.wait()
    skip = 2 * kdown - hidden
    sent = []
    piece = cols // 2
    for i, (dst, which) in enumerate(((send, 1 - tp), (own, tp))):
        for j in range(2):
            rows = pl.ds(pl.multiple_of(which * cols + j * piece, piece), piece)
            acc = dot_t(hid[:, :kdown], wdown[0, rows, :])
            acc = acc + dot_t(hid[:, kdown:], wdown[1, rows, skip:])
            span = slice(j * piece, (j + 1) * piece)
            outs[i, :, span] = acc.astype(BF16)
            sent.append(begin(outs.at[i, :, span], dst.at[:, span], sems.at[4, 2 * i + j]))
    for copy in sent:
        copy.wait()


def local(
    tokens, mix_gain, lru_input, lru_gate, lru_input_scale, lru_gate_scale, conv_weight,
    recur_gate, input_gate, decay_rate, extra_decay, lru_output, lru_output_scale, ffn_gain,
    ffn_gate, ffn_up, ffn_gate_scale, ffn_up_scale, ffn_down, ffn_down_scale,
):
    length, cols = tokens.shape
    width = 2 * cols
    chans = lru_input.shape[1] // 2
    hidden = ffn_gate.shape[1]
    rep = lax.axis_index("rep")
    tp = lax.axis_index("tp")
    swap = [(0, 1), (1, 0)]
    place = jnp.stack(
        [lax.axis_index(axis) for axis in ("fs_0", "fs_1", "fs_2", "tp", "rep")]
    ).astype(jnp.int32)

    down_t = ffn_down.T
    kdown = -(-hidden // (2 * LANES)) * LANES
    skip = hidden - kdown
    first = jnp.concatenate([ffn_gate, down_t[:, :kdown]], axis=1)
    second = jnp.concatenate([ffn_up, down_t[:, skip:]], axis=1)
    mine = jnp.where(rep == 0, first, second).astype(BF16)

    pair = lambda v: lax.ppermute(v, ("rep", "fs_0"), ODD)
    lru = (lru_input, lru_gate)
    low = jnp.concatenate([w[:, :chans] for w in lru], axis=1).astype(BF16)
    high = jnp.concatenate([w[:, chans:] for w in lru], axis=1).astype(BF16)
    home = jnp.where(rep == 0, low, high)
    out = lru_output.T.astype(BF16)
    blocks = lambda h, k, n: h[None, :, k * n : (k + 1) * n]
    streams, ticks = spread_streams([blocks(home, k, CB) for k in range(4)], IN_ORDERS)
    late = [blocks(out, k, chans) for k in range(2)]
    late = list(lax.optimization_barrier((*late, ticks[2][0]))[:2])

    weights = lax.all_gather(mine, REP_FS, axis=0, tiled=True)

    guest = pair(tokens)
    guest_extra = pair(extra_decay)
    guest_other = lax.ppermute(guest, "tp", swap)
    tokens_other = lax.ppermute(tokens, "tp", swap)
    rate = -RATE * jax.nn.softplus(-decay_rate)

    vmem = pl.BlockSpec(memory_space=pltpu.VMEM)
    hbm = pl.BlockSpec(memory_space=pl.ANY)
    smem = pl.BlockSpec(memory_space=pltpu.SMEM)
    dma = pltpu.SemaphoreType.DMA
    row = lambda v: v.reshape(1, -1)
    groups = chans // LANES
    half_rows = jax.ShapeDtypeStruct((length, cols), BF16)

    blk = 256
    grid = (length // blk,)
    whole = lambda *dims: pl.BlockSpec(dims, lambda i: (0,) * len(dims))
    rows_of = lambda n: pl.BlockSpec((blk, n), lambda i: (i, 0))

    def norm(mine, other):
        return pl.pallas_call(
            norm_kernel,
            grid=grid,
            out_shape=jax.ShapeDtypeStruct((length, width), BF16),
            in_specs=[smem, rows_of(cols), rows_of(cols), whole(1, width)],
            out_specs=rows_of(width),
            name="norm",
        )(place, mine, other, row(mix_gain))

    def mix(normed, extra):
        return pl.pallas_call(
            front_kernel,
            out_shape=jax.ShapeDtypeStruct((length, chans), BF16),
            in_specs=[smem, hbm] + [hbm] * 8 + [vmem] * 7,
            out_specs=vmem,
            scratch_shapes=[
                pltpu.VMEM((length, width), BF16),
                pltpu.VMEM((chans // CB, width, CB), BF16),
                pltpu.VMEM((chans // CB, width, CB), BF16),
                pltpu.VMEM((length + 8, CB), F32),
                pltpu.VMEM((length * groups, LANES), F32),
                pltpu.VMEM((length * groups, LANES), F32),
                pltpu.VMEM((length, chans), F32),
                pltpu.VMEM((chans // CB, CB, 2 * CB), BF16),
                dma((5,)),
            ],
            name="front",
        )(
            place, normed, *streams[0], *streams[1], *streams[2], *streams[3],
            row(lru_input_scale),
            row(lru_gate_scale), conv_weight, recur_gate, input_gate, row(rate),
            extra.reshape(-1, 1),
        )

    normed = norm(tokens, tokens_other)
    guest_normed = norm(guest, guest_other)
    outs, _ = spread_streams(
        late, OUT_ORDERS, (None, None, None, None, (normed, guest_normed))
    )
    guest_gated = mix(guest_normed, guest_extra)
    normed, guest_gated = lax.optimization_barrier((normed, guest_gated))
    gated_away = pair(guest_gated)
    gated = mix(normed, extra_decay)
    partial = pl.pallas_call(
        back_kernel,
        out_shape=jax.ShapeDtypeStruct((2, length, cols), BF16),
        in_specs=[smem] + [hbm] * 6,
        out_specs=hbm,
        scratch_shapes=[
            pltpu.VMEM((2, length, chans), BF16),
            pltpu.VMEM((width, chans), BF16),
            pltpu.VMEM((width, chans), BF16),
            pltpu.VMEM((length, width), F32),
            pltpu.VMEM((4, length, width // 4), BF16),
            dma((8,)),
        ],
        name="back",
    )(place, gated, gated_away, *outs[0], *outs[1])
    got = lax.ppermute(partial, "tp", swap)
    mixed, normed = pl.pallas_call(
        mixed_kernel,
        grid=grid,
        out_shape=[half_rows, jax.ShapeDtypeStruct((length, width), BF16)],
        in_specs=[smem, rows_of(cols), rows_of(cols)]
        + [pl.BlockSpec((2, blk, cols), lambda i: (0, i, 0))] * 2
        + [whole(2, 1, cols), whole(1, width)],
        out_specs=[rows_of(cols), rows_of(width)],
        name="mixed",
    )(
        place, tokens, tokens_other, partial, got, lru_output_scale.reshape(2, 1, cols),
        row(ffn_gain),
    )
    own, send = pl.pallas_call(
        ffn_kernel,
        out_shape=[half_rows] * 2,
        in_specs=[smem, hbm, hbm, vmem, vmem],
        out_specs=[hbm] * 2,
        scratch_shapes=[
            pltpu.VMEM((length, width), BF16),
            pltpu.VMEM((width, hidden), BF16),
            pltpu.VMEM((width, hidden), BF16),
            pltpu.VMEM((2, width, kdown), BF16),
            pltpu.VMEM((length, hidden), BF16),
            pltpu.VMEM((2, length, cols), BF16),
            dma((5, 4)),
        ],
        name="ffn",
    )(place, normed, weights, row(ffn_gate_scale), row(ffn_up_scale))
    got = lax.ppermute(send, "tp", swap)
    scale = lax.dynamic_slice_in_dim(ffn_down_scale, tp * cols, cols)
    total = own.astype(F32) + got.astype(F32)
    return (mixed.astype(F32) + total * scale).astype(BF16)


def solution(mesh):
    split = Mesh(
        mesh.devices.reshape(mesh.shape["rep"], 2, 4, 4, mesh.shape["tp"]),
        ("rep", "fs_0", "fs_1", "fs_2", "tp"),
    )
    in_specs = (
        P(REP_FS, "tp"),
        P(),
        P(FS, "tp"),
        P(FS, "tp"),
        P("tp"),
        P("tp"),
        P(None, "tp"),
        P("tp", None, None),
        P("tp", None, None),
        P("tp"),
        P(REP_FS),
        P("tp", FS),
        P(),
        P(),
        P(FS, "tp"),
        P(FS, "tp"),
        P("tp"),
        P("tp"),
        P("tp", FS),
        P(),
    )
    out_specs = P(REP_FS, "tp")
    return jax.shard_map(local, mesh=split, in_specs=in_specs, out_specs=out_specs, check_vma=False)
```

```python
import jax
import jax.numpy as jnp
from jax import lax
from jax.experimental import pallas as pl
from jax.experimental.pallas import tpu as pltpu
from jax.sharding import Mesh
from jax.sharding import PartitionSpec as P

FS = ("fs_0", "fs_1", "fs_2")
REP_FS = ("rep", "fs_0", "fs_1", "fs_2")

EPS = 1e-06
RATE = 8.0
F32 = jnp.float32
BF16 = jnp.bfloat16
CB = 256
LANES = 128
FFN_BLOCKS = (0, 256, 512, 1024)


def sigmoid(v):
    return 0.5 + 0.5 * jnp.tanh(0.5 * v)


def dot(a, b):
    return jnp.dot(a, b, preferred_element_type=F32)


def dot_t(a, b):
    return lax.dot_general(a, b, (((1,), (1,)), ((), ())), preferred_element_type=F32)


def partner(kind, place):
    z, y, x = place
    if kind == "z":
        return z ^ 1, y, x
    if kind == "ye":
        return z, y ^ 1, x
    if kind == "yo":
        return z, (((y + 1) ^ 1) + 3) % 4, x
    if kind == "xe":
        return z, y, x ^ 1
    return z, y, (((x + 1) ^ 1) + 3) % 4


ODD = [(0, 3), (3, 0), (1, 2), (2, 1)]
EVEN = [(0, 1), (1, 0), (2, 3), (3, 2)]
PAIRS = {
    "z": ("fs_0", [(0, 1), (1, 0)]),
    "ye": ("fs_1", EVEN),
    "yo": ("fs_1", ODD),
    "xe": ("fs_2", EVEN),
    "xo": ("fs_2", ODD),
}
KINDS = ("xe", "ye", "xo", "yo")
OUT_ORDERS = (("xe", "ye", "xo", "yo"), ("yo", "xo", "ye", "xe"))


IN_ORDERS = tuple(KINDS[k:] + KINDS[:k] for k in range(len(KINDS)))


def origin(order, index, place):
    order = ("z",) + order
    for s in reversed(range(len(order))):
        if (index >> s) & 1:
            place = partner(order[s], place)
    z, y, x = place
    return (z * 4 + y) * 4 + x


def spread_streams(held, orders, after=()):
    got = [None] * len(held)
    ticks = []
    for s in range(len(KINDS)):
        for k in range(len(held)):
            if s > 0:
                joined = jnp.concatenate([held[k], got[k]], axis=0)
                ready = after[s] if s < len(after) and after[s] is not None else ()
                held[k] = lax.optimization_barrier((joined, *ready))[0]
        for k in range(len(held)):
            axis, pairs = PAIRS[orders[k][s]]
            got[k] = lax.ppermute(held[k], axis, pairs)
        ticks.append(list(got))
    return [(h, g) for h, g in zip(held, got)], ticks


def place_blocks(order, halves, target, place, sem):
    count, rows = halves[0].shape[0], halves[0].shape[1]
    for index in range(2 * count):
        at = pl.multiple_of(origin(order, index, place) * rows, rows)
        source = halves[index // count].at[index % count]
        pltpu.make_async_copy(source, target.at[pl.ds(at, rows)], sem).start()


def wait_for(target, sem):
    pltpu.make_async_copy(target, target, sem).wait()


def put_halves(xn, halves, gain, tp):
    length, width = xn.shape
    cols = width // 2
    low, high = gain[:, :cols], gain[:, cols:]
    first = tp == 0
    gain_a, gain_b = jnp.where(first, low, high), jnp.where(first, high, low)
    step = 16
    for r in range(0, length, step):
        rows = slice(r, r + step)
        a, b = halves(rows)
        squares = jnp.sum(a * a + b * b, axis=-1, keepdims=True)
        scale = lax.rsqrt(squares * (1.0 / width) + EPS)
        a = a * scale * gain_a
        b = b * scale * gain_b
        xn[rows, :cols] = jnp.where(first, a, b).astype(BF16)
        xn[rows, cols:] = jnp.where(first, b, a).astype(BF16)


def front_kernel(
    place, normed, s0a, s0b, s1a, s1b, s2a, s2b, s3a, s3b, in_scale, gate_scale, taps, maps_r, maps_i,
    rate, extra, gated, xn, win, wgate, xpad, a_s, b_s, gel, block_maps, sems,
):
    length = xn.shape[0]
    chans = gated.shape[1]
    at = (place[0], place[1], place[2])
    loaded = pltpu.make_async_copy(normed, xn, sems.at[2])
    loaded.start()
    place_blocks(IN_ORDERS[0], (s0a, s0b), win.at[0], at, sems.at[0])
    place_blocks(IN_ORDERS[1], (s1a, s1b), win.at[1], at, sems.at[1])
    place_blocks(IN_ORDERS[2], (s2a, s2b), wgate.at[0], at, sems.at[3])
    place_blocks(IN_ORDERS[3], (s3a, s3b), wgate.at[1], at, sems.at[4])
    low = place[0] == 0

    def half(ref):
        return jnp.where(low, ref[:, :chans], ref[:, chans:])

    bd = maps_r.shape[1]
    per = CB // bd
    block_maps[...] = jnp.zeros(block_maps.shape, BF16)
    for n in range(chans // bd):
        k, i = n // per, n % per
        which = place[0] * (chans // bd) + n
        rows, cols = slice(i * bd, (i + 1) * bd), slice(i * bd, (i + 1) * bd)
        block_maps[k, rows, cols] = maps_r[which].astype(BF16)
        block_maps[k, rows, slice(CB + i * bd, CB + (i + 1) * bd)] = maps_i[which].astype(BF16)

    in_s, gate_s, tap, slope = half(in_scale), half(gate_scale), half(taps), half(rate)
    xpad[0:8, :] = jnp.zeros((8, CB), F32)
    groups = chans // LANES
    loaded.wait()
    wait_for(win.at[0], sems.at[0])
    wait_for(win.at[1], sems.at[1])
    wait_for(wgate.at[0], sems.at[3])
    wait_for(wgate.at[1], sems.at[4])
    for k in range(chans // CB):
        cols = slice(k * CB, (k + 1) * CB)
        pre = dot(xn[...], win[k]) * in_s[:, cols]
        xpad[8 : 8 + length, :] = pre.astype(BF16).astype(F32)
        conv = tap[3:4, cols] * xpad[8 : 8 + length, :]
        for j in range(3):
            conv = conv + tap[j : j + 1, cols] * xpad[5 + j : 5 + j + length, :]
        maps = dot(conv.astype(BF16), block_maps[k])
        recur = sigmoid(maps[:, :CB])
        ingate = sigmoid(maps[:, CB:])
        factor = jnp.exp(slope[:, cols] * recur - extra[...])
        rest = 1.0 - factor * factor
        drive = rest * lax.rsqrt(rest) * (ingate * conv)
        for g in range(CB // LANES):
            row = k * (CB // LANES) + g
            part = slice(g * LANES, (g + 1) * LANES)
            a_s[pl.ds(row, length, stride=groups), :] = factor[:, part]
            b_s[pl.ds(row, length, stride=groups), :] = drive[:, part]
    for k in range(chans // CB):
        cols = slice(k * CB, (k + 1) * CB)
        pre_gate = (dot(xn[...], wgate[k]) * gate_s[:, cols]).astype(BF16)
        gel[:, cols] = jax.nn.gelu(pre_gate.astype(F32), approximate=True)
    h = jnp.zeros((groups, LANES), F32)
    for t in range(length):
        rows = slice(t * groups, (t + 1) * groups)
        h = a_s[rows, :] * h + b_s[rows, :]
        b_s[rows, :] = h
    for g in range(groups):
        cols = slice(g * LANES, (g + 1) * LANES)
        gated[:, cols] = (b_s[pl.ds(g, length, stride=groups), :] * gel[:, cols]).astype(BF16)


def back_kernel(place, mine, other, s2a, s2b, s3a, s3b, partial, g, w0, w1, acc, outs, sems):
    at = (place[0], place[1], place[2])
    low = place[0]
    loads = [
        pltpu.make_async_copy(mine, g.at[low], sems.at[2]),
        pltpu.make_async_copy(other, g.at[1 - low], sems.at[3]),
    ]
    place_blocks(OUT_ORDERS[0], (s2a, s2b), w0, at, sems.at[0])
    for copy in loads:
        copy.start()
    place_blocks(OUT_ORDERS[1], (s3a, s3b), w1, at, sems.at[1])
    for copy in loads:
        copy.wait()
    wait_for(w0, sems.at[0])
    width = w0.shape[0]
    cols = partial.shape[2]
    piece = cols // 2
    for c in range(width // piece):
        rows = slice(c * piece, (c + 1) * piece)
        acc[:, rows] = dot_t(g[0], w0[rows, :])
    wait_for(w1, sems.at[1])
    sent = []
    for c in range(width // piece):
        rows = slice(c * piece, (c + 1) * piece)
        outs[c] = (acc[:, rows] + dot_t(g[1], w1[rows, :])).astype(BF16)
        copy = pltpu.make_async_copy(
            outs.at[c],
            partial.at[c // 2, :, pl.ds((c % 2) * piece, piece)],
            sems.at[4 + c],
        )
        copy.start()
        sent.append(copy)
    for copy in sent:
        copy.wait()


def norm_kernel(place, mine, other, gain, xn):
    put_halves(
        xn, lambda rows: (mine[rows, :].astype(F32), other[rows, :].astype(F32)), gain, place[3]
    )


def mixed_kernel(place, tok_mine, tok_other, part, got, out_scale, gain, mixed, xn):
    tp = place[3]

    def mix(tok, which, rows):
        total = part[which, rows, :].astype(F32) + got[which, rows, :].astype(F32)
        return (tok[rows, :].astype(F32) + total * out_scale[which]).astype(BF16)

    def halves(rows):
        a = mix(tok_mine, tp, rows)
        mixed[rows, :] = a
        return a.astype(F32), mix(tok_other, 1 - tp, rows).astype(F32)

    put_halves(xn, halves, gain, tp)


def ffn_kernel(
    place, normed, weights, gate_scale, up_scale, own, send, xn, wgate, wup, wdown, hid, outs, sems
):
    length, width = xn.shape
    hidden = gate_scale.shape[1]
    kdown = wdown.shape[2]
    starts = list(FFN_BLOCKS) + [hidden]
    blocks = [(s, e - s) for s, e in zip(starts[:-1], starts[1:])]
    copies = []

    def begin(source, target, sem):
        copy = pltpu.make_async_copy(source, target, sem)
        copy.start()
        return copy

    loaded = begin(normed, xn, sems.at[3, 0])
    for k, (s, n) in enumerate(blocks):
        for r, dst in ((0, wgate), (1, wup)):
            copies.append(
                begin(
                    weights.at[pl.ds(r * width, width), pl.ds(s, n)],
                    dst.at[:, pl.ds(s, n)],
                    sems.at[r, k],
                )
            )
    down_copies = [
        begin(
            weights.at[pl.ds(r * width, width), pl.ds(hidden, kdown)], wdown.at[r], sems.at[2, r]
        )
        for r in range(2)
    ]
    cols = width // 2
    tp = place[3]
    loaded.wait()
    held = None

    def activate(part, gate, up):
        hid[:, part] = (gate * sigmoid(gate) * up).astype(BF16)

    for k, (s, n) in enumerate(blocks):
        part = slice(s, s + n)
        copies[2 * k].wait()
        copies[2 * k + 1].wait()
        gate = dot(xn[...], wgate[:, part]) * gate_scale[:, part]
        up = dot(xn[...], wup[:, part]) * up_scale[:, part]
        if held is not None:
            activate(*held)
        held = (part, gate, up)
    for copy in down_copies:
        copy.wait()
    activate(*held)
    skip = 2 * kdown - hidden
    sent = []
    piece = cols // 2
    for i, (dst, which) in enumerate(((send, 1 - tp), (own, tp))):
        for j in range(2):
            rows = pl.ds(pl.multiple_of(which * cols + j * piece, piece), piece)
            acc = dot_t(hid[:, :kdown], wdown[0, rows, :])
            acc = acc + dot_t(hid[:, kdown:], wdown[1, rows, skip:])
            span = slice(j * piece, (j + 1) * piece)
            outs[i, :, span] = acc.astype(BF16)
            sent.append(begin(outs.at[i, :, span], dst.at[:, span], sems.at[4, 2 * i + j]))
    for copy in sent:
        copy.wait()


def local(
    tokens, mix_gain, lru_input, lru_gate, lru_input_scale, lru_gate_scale, conv_weight,
    recur_gate, input_gate, decay_rate, extra_decay, lru_output, lru_output_scale, ffn_gain,
    ffn_gate, ffn_up, ffn_gate_scale, ffn_up_scale, ffn_down, ffn_down_scale,
):
    length, cols = tokens.shape
    width = 2 * cols
    chans = lru_input.shape[1] // 2
    hidden = ffn_gate.shape[1]
    rep = lax.axis_index("rep")
    tp = lax.axis_index("tp")
    zed = lax.axis_index("fs_0")
    swap = [(0, 1), (1, 0)]
    place = jnp.stack(
        [lax.axis_index(axis) for axis in ("fs_0", "fs_1", "fs_2", "tp")]
    ).astype(jnp.int32)

    down_t = ffn_down.T
    kdown = -(-hidden // (2 * LANES)) * LANES
    skip = hidden - kdown
    first = jnp.concatenate([ffn_gate, down_t[:, :kdown]], axis=1)
    second = jnp.concatenate([ffn_up, down_t[:, skip:]], axis=1)
    mine = jnp.where(rep == 0, first, second).astype(BF16)

    lru = (lru_input, lru_gate)
    low = jnp.concatenate([w[:, :chans] for w in lru], axis=1).astype(BF16)
    high = jnp.concatenate([w[:, chans:] for w in lru], axis=1).astype(BF16)
    home = jnp.where(zed == 0, low, high)
    away = lax.ppermute(jnp.where(zed == 0, high, low), "fs_0", swap)
    out = lru_output.T.astype(BF16)
    away_out = lax.ppermute(out, "fs_0", swap)
    blocks = lambda h, a, k, n: jnp.stack([h[:, k * n : (k + 1) * n], a[:, k * n : (k + 1) * n]])
    streams, ticks = spread_streams([blocks(home, away, k, CB) for k in range(4)], IN_ORDERS)
    late = [blocks(out, away_out, k, chans) for k in range(2)]
    late = list(lax.optimization_barrier((*late, ticks[1][0]))[:2])

    weights = lax.all_gather(mine, REP_FS, axis=0, tiled=True)

    behind, behind_extra, _ = lax.optimization_barrier((tokens, extra_decay, away))
    guest = lax.ppermute(behind, "fs_0", swap)
    guest_extra = lax.ppermute(behind_extra, "fs_0", swap)
    guest_other = lax.ppermute(guest, "tp", swap)
    tokens_other = lax.ppermute(tokens, "tp", swap)
    rate = -RATE * jax.nn.softplus(-decay_rate)

    vmem = pl.BlockSpec(memory_space=pltpu.VMEM)
    hbm = pl.BlockSpec(memory_space=pl.ANY)
    smem = pl.BlockSpec(memory_space=pltpu.SMEM)
    dma = pltpu.SemaphoreType.DMA
    row = lambda v: v.reshape(1, -1)
    groups = chans // LANES
    half_rows = jax.ShapeDtypeStruct((length, cols), BF16)

    blk = 256
    grid = (length // blk,)
    whole = lambda *dims: pl.BlockSpec(dims, lambda i: (0,) * len(dims))
    rows_of = lambda n: pl.BlockSpec((blk, n), lambda i: (i, 0))

    def norm(mine, other):
        return pl.pallas_call(
            norm_kernel,
            grid=grid,
            out_shape=jax.ShapeDtypeStruct((length, width), BF16),
            in_specs=[smem, rows_of(cols), rows_of(cols), whole(1, width)],
            out_specs=rows_of(width),
            name="norm",
        )(place, mine, other, row(mix_gain))

    def mix(normed, extra):
        return pl.pallas_call(
            front_kernel,
            out_shape=jax.ShapeDtypeStruct((length, chans), BF16),
            in_specs=[smem, hbm] + [hbm] * 8 + [vmem] * 7,
            out_specs=vmem,
            scratch_shapes=[
                pltpu.VMEM((length, width), BF16),
                pltpu.VMEM((chans // CB, width, CB), BF16),
                pltpu.VMEM((chans // CB, width, CB), BF16),
                pltpu.VMEM((length + 8, CB), F32),
                pltpu.VMEM((length * groups, LANES), F32),
                pltpu.VMEM((length * groups, LANES), F32),
                pltpu.VMEM((length, chans), F32),
                pltpu.VMEM((chans // CB, CB, 2 * CB), BF16),
                dma((5,)),
            ],
            name="front",
        )(
            place, normed, *streams[0], *streams[1], *streams[2], *streams[3],
            row(lru_input_scale),
            row(lru_gate_scale), conv_weight, recur_gate, input_gate, row(rate),
            extra.reshape(-1, 1),
        )

    normed = norm(tokens, tokens_other)
    guest_normed = norm(guest, guest_other)
    outs, _ = spread_streams(
        late, OUT_ORDERS, (None, None, None, (normed, guest_normed))
    )
    guest_gated = mix(guest_normed, guest_extra)
    normed, guest_gated = lax.optimization_barrier((normed, guest_gated))
    gated_away = lax.ppermute(guest_gated, "fs_0", swap)
    gated = mix(normed, extra_decay)
    partial = pl.pallas_call(
        back_kernel,
        out_shape=jax.ShapeDtypeStruct((2, length, cols), BF16),
        in_specs=[smem] + [hbm] * 6,
        out_specs=hbm,
        scratch_shapes=[
            pltpu.VMEM((2, length, chans), BF16),
            pltpu.VMEM((width, chans), BF16),
            pltpu.VMEM((width, chans), BF16),
            pltpu.VMEM((length, width), F32),
            pltpu.VMEM((4, length, width // 4), BF16),
            dma((8,)),
        ],
        name="back",
    )(place, gated, gated_away, *outs[0], *outs[1])
    got = lax.ppermute(partial, "tp", swap)
    mixed, normed = pl.pallas_call(
        mixed_kernel,
        grid=grid,
        out_shape=[half_rows, jax.ShapeDtypeStruct((length, width), BF16)],
        in_specs=[smem, rows_of(cols), rows_of(cols)]
        + [pl.BlockSpec((2, blk, cols), lambda i: (0, i, 0))] * 2
        + [whole(2, 1, cols), whole(1, width)],
        out_specs=[rows_of(cols), rows_of(width)],
        name="mixed",
    )(
        place, tokens, tokens_other, partial, got, lru_output_scale.reshape(2, 1, cols),
        row(ffn_gain),
    )
    own, send = pl.pallas_call(
        ffn_kernel,
        out_shape=[half_rows] * 2,
        in_specs=[smem, hbm, hbm, vmem, vmem],
        out_specs=[hbm] * 2,
        scratch_shapes=[
            pltpu.VMEM((length, width), BF16),
            pltpu.VMEM((width, hidden), BF16),
            pltpu.VMEM((width, hidden), BF16),
            pltpu.VMEM((2, width, kdown), BF16),
            pltpu.VMEM((length, hidden), BF16),
            pltpu.VMEM((2, length, cols), BF16),
            dma((5, 4)),
        ],
        name="ffn",
    )(place, normed, weights, row(ffn_gate_scale), row(ffn_up_scale))
    got = lax.ppermute(send, "tp", swap)
    scale = lax.dynamic_slice_in_dim(ffn_down_scale, tp * cols, cols)
    total = own.astype(F32) + got.astype(F32)
    return (mixed.astype(F32) + total * scale).astype(BF16)


def solution(mesh):
    split = Mesh(
        mesh.devices.reshape(mesh.shape["rep"], 2, 4, 4, mesh.shape["tp"]),
        ("rep", "fs_0", "fs_1", "fs_2", "tp"),
    )
    in_specs = (
        P(REP_FS, "tp"),
        P(),
        P(FS, "tp"),
        P(FS, "tp"),
        P("tp"),
        P("tp"),
        P(None, "tp"),
        P("tp", None, None),
        P("tp", None, None),
        P("tp"),
        P(REP_FS),
        P("tp", FS),
        P(),
        P(),
        P(FS, "tp"),
        P(FS, "tp"),
        P("tp"),
        P("tp"),
        P("tp", FS),
        P(),
    )
    out_specs = P(REP_FS, "tp")
    return jax.shard_map(local, mesh=split, in_specs=in_specs, out_specs=out_specs, check_vma=False)
```
